32 devices in a mesh: rep: 2 (over x), fs: 4 (over z), tp: 4 (over y, core).
Axes of the slice: x: 2, y: 2, z: 4, core: 2. Of those that a mesh axis runs over, the one named last changes fastest.
Arguments:
- residual: bfloat16 [8, 768, 4, 512], P(('rep', 'fs'), None, None, 'tp'), may hold values from -6 to 6
- mixer_gain: float32 [4, 512], P(None, 'tp'), may hold values from 0.1 to 1.9
- pool_weight: float32 [4, 512, 512], P(None, 'fs', 'tp'), may hold values from -0.25 to 0.25
- pool_scale: float32 [4, 512], P(None, 'tp'), may hold values from 0.5 to 2
- channel_gain: float32 [4, 512], P(None, 'tp'), may hold values from 0.1 to 1.9
- gate_weight: float32 [2048, 6144], P('fs', 'tp'), may hold values from -0.125 to 0.125
- up_weight: float32 [2048, 6144], P('fs', 'tp'), may hold values from -0.125 to 0.125
- gate_scale: float32 [4, 1536], P('fs', 'tp'), may hold values from 0.5 to 2
- up_scale: float32 [4, 1536], P('fs', 'tp'), may hold values from 0.5 to 2
- gate_taps: float32 [3, 6144], P(None, 'tp'), may hold values from -3.5 to 3.5
- up_taps: float32 [3, 6144], P(None, 'tp'), may hold values from -3.5 to 3.5
- down_weight: float32 [6144, 2048], P('tp', 'fs'), may hold values from -0.078125 to 0.078125
- down_scale: float32 [4, 512], P(None, 'tp'), may hold values from 0.5 to 2
Outputs:
- layer_out: bfloat16 [8, 768, 4, 512], P(('rep', 'fs'), None, None, 'tp')
The draws below stay inside these ranges and needn't reach their ends.
All inputs are finite; a program needn't handle non-finite values.
Results may differ from the reference program's by a relative error of at most 0.018.
Values may be sent and summed in bfloat16 or wider, within the bound.
A program may use at most 128 MiB of HBM per device.

```python
import math
import jax
import jax.numpy as jnp
from jax import lax

D = 2048
G = 4
C = 512
FF = 6144
SEQ_LEN = 768
SEQS = 8
N_FS = 4
N_TP = 4


def level_of(own_key, shape, shards, least, largest):
    level = 1.0
    for position, parts in shards:
        draws = jax.random.uniform(jax.random.fold_in(jax.random.fold_in(own_key, 6), position), (parts,), jnp.float32, least / len(shards), largest / len(shards))
        level = level * jnp.repeat(jnp.exp(draws), shape[position] // parts).reshape((-1,) + (1,) * (len(shape) - 1 - position))
    return level


def gaussian(rng, shape, scale, reach, shards=(), kind=jnp.bfloat16):
    level = level_of(rng, shape, shards, -0.22, 0.18) if shards else 1.0
    values = jax.random.normal(rng, shape, jnp.float32) * scale * level
    return jnp.minimum(jnp.maximum(values, -reach), reach).astype(kind)


def setup_inputs(seed: int = 0) -> dict:
    key_list = jax.random.split(jax.random.key(seed), 14)
    residual = gaussian(key_list[0], (SEQS, SEQ_LEN, G, C), 1.0, 6.0, ((0, 8), (3, 4)))
    mixer_gain = jnp.clip(1.0 + 0.18 * jax.random.normal(key_list[1], (G, C), jnp.float32), 0.1, 1.9)
    pool_weight = gaussian(key_list[2], (G, C, C), C ** -0.5, 0.25, ((1, 4), (2, 4)), jnp.float32)
    pool_scale = jnp.clip(jnp.exp(math.log(2.0) - 1.3862944 * jax.random.uniform(key_list[3], (G, C), jnp.float32) ** level_of(key_list[3], (G, C), ((1, 4),), -0.2, 0.2)), 0.5, 2.0)
    channel_gain = jnp.clip(1.0 + 0.18 * jax.random.normal(key_list[4], (G, C), jnp.float32), 0.1, 1.9)
    gate_weight = gaussian(key_list[5], (D, FF), D ** -0.5, 0.125, ((0, 4), (1, 4)), jnp.float32)
    up_weight = gaussian(key_list[6], (D, FF), D ** -0.5, 0.125, ((0, 4), (1, 4)), jnp.float32)
    gate_scale = jnp.clip(jnp.exp(math.log(2.0) - 1.3862944 * jax.random.uniform(key_list[7], (N_FS, FF // N_FS), jnp.float32) ** level_of(key_list[7], (N_FS, FF // N_FS), ((0, 4), (1, 4)), -0.2, 0.2)), 0.5, 2.0)
    up_scale = jnp.clip(jnp.exp(math.log(2.0) - 1.3862944 * jax.random.uniform(key_list[8], (N_FS, FF // N_FS), jnp.float32) ** level_of(key_list[8], (N_FS, FF // N_FS), ((0, 4), (1, 4)), -0.2, 0.2)), 0.5, 2.0)
    gate_taps = gaussian(key_list[9], (3, FF), 3 ** -0.5, 3.5, ((1, 4),), jnp.float32)
    up_taps = gaussian(key_list[10], (3, FF), 3 ** -0.5, 3.5, ((1, 4),), jnp.float32)
    down_weight = gaussian(key_list[11], (FF, D), FF ** -0.5, 0.078125, ((0, 4), (1, 4)), jnp.float32)
    down_scale = jnp.clip(jnp.exp(math.log(2.0) - 1.3862944 * jax.random.uniform(key_list[12], (G, C), jnp.float32) ** level_of(key_list[12], (G, C), ((1, 4),), -0.2, 0.2)), 0.5, 2.0)
    return dict(residual=residual, mixer_gain=mixer_gain, pool_weight=pool_weight, pool_scale=pool_scale, channel_gain=channel_gain, gate_weight=gate_weight, up_weight=up_weight, gate_scale=gate_scale, up_scale=up_scale, gate_taps=gate_taps, up_taps=up_taps, down_weight=down_weight, down_scale=down_scale)


WINDOWS = (2, 4, 8, 16)
EPSILON = 1e-05

def shifted(values, steps):
    padding = jnp.zeros((steps,) + values.shape[1:], values.dtype)
    return jnp.concatenate([padding, values[:-steps]], axis=0)

def pooled_groups(normed):
    values = normed.astype(jnp.float32)
    totals = values
    reach_now = 1
    columns = []
    positions = jnp.arange(1, values.shape[0] + 1).astype(jnp.float32)
    for group_idx in range(len(WINDOWS)):
        while reach_now < WINDOWS[group_idx]:
            totals = totals + shifted(totals, reach_now)
            reach_now = reach_now * 2
        divisor = jnp.minimum(positions, float(WINDOWS[group_idx]))
        columns.append(totals[:, group_idx] / divisor[:, None] - values[:, group_idx])
    return jnp.stack(columns, axis=1).astype(jnp.bfloat16)

def normalized(residual, gain):
    values = residual.astype(jnp.float32)
    mean_square = lax.optimization_barrier(jnp.mean(values * values, axis=(1, 2), keepdims=True))
    return (values * lax.rsqrt(mean_square + EPSILON) * gain).astype(jnp.bfloat16)

def causal_taps(stored, taps):
    values = stored.astype(jnp.float32)
    return taps[2] * values + taps[1] * shifted(values, 1) + taps[0] * shifted(values, 2)

def shard_order(scale):
    return jnp.transpose(scale.reshape(N_FS, N_TP, -1), (1, 0, 2)).reshape(-1)

def one_sequence(residual, mixer_gain, pool_half, pool_scale, channel_gain, gate_half, up_half, gate_columns, up_columns, gate_taps, up_taps, down_half, down_scale):
    normed = normalized(residual, mixer_gain)
    pooled = pooled_groups(normed)
    mixed = jnp.einsum('lgc,gce->lge', pooled.astype(jnp.float32), pool_half.astype(jnp.float32))
    middle = (mixed * pool_scale + residual.astype(jnp.float32)).astype(jnp.bfloat16)
    length = middle.shape[0]
    inputs = normalized(middle, channel_gain).reshape(length, -1)
    gate_pre = (jnp.dot(inputs, gate_half, preferred_element_type=jnp.float32) * gate_columns).astype(jnp.bfloat16)
    up_pre = (jnp.dot(inputs, up_half, preferred_element_type=jnp.float32) * up_columns).astype(jnp.bfloat16)
    hidden = (jax.nn.silu(causal_taps(gate_pre, gate_taps)) * causal_taps(up_pre, up_taps)).astype(jnp.bfloat16)
    block_rows = hidden.shape[1] // N_TP
    summed = jnp.zeros((length, down_half.shape[1]), jnp.float32)
    for shard_idx in range(N_TP):
        lower = shard_idx * block_rows
        partial_sum = jnp.dot(hidden[:, lower:lower + block_rows], down_half[lower:lower + block_rows], preferred_element_type=jnp.float32).astype(jnp.bfloat16)
        summed = summed + lax.optimization_barrier(partial_sum).astype(jnp.float32)
    summed = summed.reshape(middle.shape)
    return (summed * down_scale + middle.astype(jnp.float32)).astype(jnp.bfloat16)

def reference(residual, mixer_gain, pool_weight, pool_scale, channel_gain, gate_weight, up_weight, gate_scale, up_scale, gate_taps, up_taps, down_weight, down_scale):
    pool_half = pool_weight.astype(jnp.bfloat16)
    gate_half = gate_weight.astype(jnp.bfloat16)
    up_half = up_weight.astype(jnp.bfloat16)
    down_half = down_weight.astype(jnp.bfloat16)
    gate_columns = shard_order(gate_scale)
    up_columns = shard_order(up_scale)

    def per_sequence(sequence):
        return one_sequence(sequence, mixer_gain, pool_half, pool_scale, channel_gain, gate_half, up_half, gate_columns, up_columns, gate_taps, up_taps, down_half, down_scale)
    return lax.map(per_sequence, residual)
```

```python
import functools

import jax
import jax.numpy as jnp
from jax import lax
from jax.experimental import pallas as pl
from jax.experimental.pallas import tpu as pltpu
from jax.sharding import PartitionSpec as P

WINDOWS = (2, 4, 8, 16)
EPSILON = 1e-05
SUBS = 2
COLUMNS = 256
VMEM_BYTES = 62 * 1024 * 1024
F32 = jnp.float32
BF16 = jnp.bfloat16


def delayed(values, steps):
    rows = lax.broadcasted_iota(jnp.int32, values.shape, 0)
    return jnp.where(rows >= steps, pltpu.roll(values, steps, 0), 0.0)


def causal_taps(values, taps):
    return taps[2:3] * values + taps[1:2] * delayed(values, 1) + taps[0:1] * delayed(values, 2)


def block_kernel(
    sizes,
    residual,
    gains,
    pool_scale,
    down_scale,
    scale_pair,
    gate_taps,
    up_taps,
    pool_own,
    gate_own,
    up_own,
    down_own,
    out,
    pool_full,
    gate_full,
    up_full,
    down_full,
    gathered,
    middle_all,
    gains_all,
    scales_all,
    scale_row,
    pooled,
    middle,
    inputs,
    gate_pre,
    hidden,
    partials,
    arrived,
    ring_send,
    ring_recv,
    rep_send,
    rep_recv,
    pool_send,
    pool_recv,
    pool_rep_send,
    pool_rep_recv,
    scale_send,
    scale_recv,
    tp_send,
    tp_recv,
    part_send,
    part_recv,
    local_sem,
):
    n_rep, n_fs, n_tp = sizes
    rep, fs, tp = (lax.axis_index(name) for name in ("rep", "fs", "tp"))
    length = residual.shape[0]
    groups = pool_full.shape[0]
    channels = pool_full.shape[1]
    local = residual.shape[1] // groups
    width = groups * channels

    def other(axis, offset):
        me, count = {"rep": (rep, n_rep), "fs": (fs, n_fs), "tp": (tp, n_tp)}[axis]
        return lax.rem(me + offset, count)

    def remote(src, dst, send, recv, axis, offset):
        return pltpu.make_async_remote_copy(
            src_ref=src,
            dst_ref=dst,
            send_sem=send,
            recv_sem=recv,
            device_id={axis: other(axis, offset)},
            device_id_type=pl.DeviceIdType.MESH,
        )

    barrier = pltpu.get_barrier_semaphore()
    for axis, count in (("rep", n_rep), ("fs", n_fs), ("tp", n_tp)):
        for offset in range(1, count):
            pl.semaphore_signal(
                barrier,
                inc=1,
                device_id={axis: other(axis, offset)},
                device_id_type=pl.DeviceIdType.MESH,
            )
    pl.semaphore_wait(barrier, n_rep + n_fs + n_tp - 3)

    sent = []

    def start(copy, valid=None):
        sent.append((copy, valid))
        if valid is None:
            copy.start()
        else:
            pl.when(valid)(copy.start)

    weights = ((gate_own, gate_full), (up_own, up_full), (down_own, down_full))

    def piece(w, shard, half, sub, own=False):
        rows = weights[w][0].shape[0] // (n_rep * SUBS)
        part = pl.ds(pl.multiple_of((half * SUBS + sub) * rows, rows), rows)
        return weights[w][0].at[part] if own else weights[w][1].at[shard, part]

    def shard_sent(step, way):
        shard = fs + step if way else fs - step
        return jnp.clip(shard, 0, n_fs - 1), (shard <= n_fs - 1 if way else shard >= 0)

    def line(w, sub, step):
        for way in range(2):
            shard, valid = shard_sent(step, way)
            start(
                remote(
                    piece(w, shard, rep, sub, own=step == 0),
                    piece(w, shard, rep, sub),
                    ring_send.at[w, sub, 2 * step + way],
                    ring_recv.at[w, sub, 2 * step + way],
                    "fs",
                    n_fs - 1 if way else 1,
                ),
                valid & (fs > 0 if way else fs < n_fs - 1),
            )

    def serve(w, sub, step):
        for way in range(2):
            shard, valid = shard_sent(step + 1, way)
            mine = piece(w, shard, rep, sub)
            sems = (w, sub, 2 * step + way)
            pl.when(valid)(
                remote(
                    mine, mine, ring_send.at[sems], ring_recv.at[sems], "fs", 1
                ).wait_recv
            )
            if step < n_fs - 2:
                onward = (w, sub, 2 * step + 2 + way)
                start(
                    remote(
                        mine,
                        mine,
                        ring_send.at[onward],
                        ring_recv.at[onward],
                        "fs",
                        n_fs - 1 if way else 1,
                    ),
                    valid & (fs > 0 if way else fs < n_fs - 1),
                )
            for d in range(1, n_rep):
                start(
                    remote(
                        mine,
                        mine,
                        rep_send.at[sems + (d - 1,)],
                        rep_recv.at[sems + (d - 1,)],
                        "rep",
                        d,
                    ),
                    valid,
                )

    def settle(w, step, ways=(0, 1)):
        for way in ways:
            shard, valid = shard_sent(step + 1, way)

            @pl.when(valid)
            def _():
                for sub in range(SUBS):
                    for d in range(1, n_rep):
                        got = piece(w, shard, other("rep", n_rep - d), sub)
                        sems = (w, sub, 2 * step + way, d - 1)
                        remote(
                            got, got, rep_send.at[sems], rep_recv.at[sems], "rep", d
                        ).wait_recv()

    def local_copy(src, dst, idx):
        copy = pltpu.make_async_copy(src, dst, local_sem.at[idx])
        copy.start()
        return copy

    own_copies = [
        local_copy(residual, gathered.at[tp], 0),
        local_copy(gains, gains_all.at[tp], 1),
        local_copy(scale_pair, scales_all.at[fs], 2),
        local_copy(gate_own, gate_full.at[fs], 3),
        local_copy(up_own, up_full.at[fs], 4),
        local_copy(down_own, down_full.at[fs], 5),
    ]

    pool_rows = pool_own.shape[1]
    rep_groups = groups // n_rep

    def pool_part(shard, half):
        return pool_full.at[
            pl.ds(half * rep_groups, rep_groups),
            pl.ds(pl.multiple_of(shard * pool_rows, pool_rows), pool_rows),
        ]

    pool_copy = local_copy(
        pool_own, pool_full.at[:, pl.ds(pl.multiple_of(fs * pool_rows, pool_rows), pool_rows)], 6
    )

    for d in range(1, n_fs):
        start(
            remote(
                pool_own.at[pl.ds(rep * rep_groups, rep_groups)],
                pool_part(fs, rep),
                pool_send.at[d - 1],
                pool_recv.at[d - 1],
                "fs",
                d,
            )
        )
    for w in (0, 1):
        for sub in range(SUBS):
            if n_fs > 1:
                line(w, sub, 0)
    for d in range(1, n_tp):
        start(remote(gains, gains_all.at[tp], tp_send.at[0, d - 1], tp_recv.at[0, d - 1], "tp", d))
    for d in range(1, n_tp):
        start(
            remote(residual, gathered.at[tp], tp_send.at[1, d - 1], tp_recv.at[1, d - 1], "tp", d)
        )
    for d in range(1, n_fs):
        start(
            remote(
                scale_pair, scales_all.at[fs], scale_send.at[d - 1], scale_recv.at[d - 1], "fs", d
            )
        )

    for d in range(1, n_fs):
        shard = other("fs", n_fs - d)
        mine = pool_part(shard, rep)
        remote(mine, mine, pool_send.at[d - 1], pool_recv.at[d - 1], "fs", d).wait_recv()
        for e in range(1, n_rep):
            start(
                remote(
                    mine,
                    mine,
                    pool_rep_send.at[d - 1, e - 1],
                    pool_rep_recv.at[d - 1, e - 1],
                    "rep",
                    e,
                )
            )
    for d in range(1, n_fs):
        shard = other("fs", n_fs - d)
        for e in range(1, n_rep):
            got = pool_part(shard, other("rep", n_rep - e))
            remote(
                got,
                got,
                pool_rep_send.at[d - 1, e - 1],
                pool_rep_recv.at[d - 1, e - 1],
                "rep",
                e,
            ).wait_recv()
    pool_copy.wait()
    for copy in own_copies:
        copy.wait()

    def tp_arrivals(idx, buffer):
        for d in range(1, n_tp):
            got = buffer.at[other("tp", n_tp - d)]
            remote(got, got, tp_send.at[idx, d - 1], tp_recv.at[idx, d - 1], "tp", d).wait_recv()

    for sub in range(SUBS):
        serve(0, sub, 0)
    tp_arrivals(0, gains_all)
    tp_arrivals(1, gathered)
    for sub in range(SUBS):
        serve(1, sub, 0)

    def mean_square_root(buffer):
        total = jnp.zeros((length, 1), F32)
        for t in range(n_tp):
            values = buffer[t].astype(F32)
            total = total + jnp.sum(values * values, axis=1, keepdims=True)
        return lax.rsqrt(total / width + EPSILON)

    factor = mean_square_root(gathered)
    positions = lax.broadcasted_iota(jnp.int32, (length, 1), 0).astype(F32) + 1.0
    for g in range(groups):
        part = slice(g * local, (g + 1) * local)
        share = 1.0 / jnp.minimum(positions, float(WINDOWS[g]))
        for t in range(n_tp):
            values = gathered[t, :, part].astype(F32)
            normed = (values * factor * gains_all[t, 0:1, part]).astype(BF16).astype(F32)
            totals = normed
            reach = 1
            while reach < WINDOWS[g]:
                totals = totals + delayed(totals, reach)
                reach = reach * 2
            pooled[:, t * local : (t + 1) * local] = (totals * share - normed).astype(BF16)
        mixed = jnp.dot(pooled[...], pool_full[g], preferred_element_type=F32)
        middle[:, part] = (
            mixed * pool_scale[:, part] + residual[:, part].astype(F32)
        ).astype(BF16)

    middle_copy = local_copy(middle, middle_all.at[tp], 0)
    for d in range(1, n_tp):
        start(
            remote(middle, middle_all.at[tp], tp_send.at[2, d - 1], tp_recv.at[2, d - 1], "tp", d)
        )
    for step in range(1, n_fs - 1):
        for w in (0, 1):
            if step == n_fs - 2 and n_fs > 2:
                break
            for sub in range(SUBS):
                serve(w, sub, step)
    for sub in range(SUBS):
        if n_fs > 1:
            line(2, sub, 0)
    for d in range(1, n_fs):
        got = scales_all.at[other("fs", n_fs - d)]
        remote(got, got, scale_send.at[d - 1], scale_recv.at[d - 1], "fs", d).wait_recv()
    shard_columns = scale_pair.shape[1]
    for f in range(n_fs):
        scale_row[:, f * shard_columns : (f + 1) * shard_columns] = scales_all[f]

    middle_copy.wait()
    tp_arrivals(2, middle_all)
    factor = mean_square_root(middle_all)
    for t in range(n_tp):
        for g in range(groups):
            part = slice(g * local, (g + 1) * local)
            start_column = g * channels + t * local
            inputs[:, start_column : start_column + local] = (
                middle_all[t, :, part].astype(F32) * factor * gains_all[t, 1:2, part]
            ).astype(BF16)

    def finish(w):
        if n_fs > 2:
            for sub in range(SUBS):
                serve(w, sub, n_fs - 2)
        for step in range(n_fs - 1):
            settle(w, step)

    def product(full, columns, row):
        block = full[:, :, columns].reshape(width, COLUMNS)
        made = jnp.dot(inputs[...], block, preferred_element_type=F32)
        return (made * scale_row[row : row + 1, columns]).astype(BF16)

    chunks = gate_full.shape[2] // COLUMNS

    finish(0)

    @pl.loop(0, chunks)
    def _(j):
        columns = pl.ds(pl.multiple_of(j * COLUMNS, COLUMNS), COLUMNS)
        gate_pre[:, columns] = product(gate_full, columns, 0)

    finish(1)
    for sub in range(SUBS):
        if n_fs > 1:
            serve(2, sub, 0)

    @pl.loop(0, chunks)
    def _(j):
        columns = pl.ds(pl.multiple_of(j * COLUMNS, COLUMNS), COLUMNS)
        up_values = product(up_full, columns, 1).astype(F32)
        conv_gate = causal_taps(gate_pre[:, columns].astype(F32), gate_taps[:, columns])
        conv_up = causal_taps(up_values, up_taps[:, columns])
        silu = conv_gate / (1.0 + jnp.exp(-conv_gate))
        hidden[:, columns] = (silu * conv_up).astype(BF16)

    shard_width = down_own.shape[1]

    def to_peers(idx, src, dst):
        for d in range(1, n_tp):
            start(
                remote(
                    src(other("tp", d)),
                    dst(tp),
                    part_send.at[idx, d - 1],
                    part_recv.at[idx, d - 1],
                    "tp",
                    d,
                )
            )

    def from_peers(idx, dst):
        for d in range(1, n_tp):
            got = dst(other("tp", n_tp - d))
            remote(
                got, got, part_send.at[idx, d - 1], part_recv.at[idx, d - 1], "tp", d
            ).wait_recv()

    def conclude(g, columns):
        total = partials[tp, g].astype(F32)
        for d in range(1, n_tp):
            total = total + arrived[other("tp", d), g].astype(F32)
        out[:, columns] = (
            total * down_scale[:, columns] + middle[:, columns].astype(F32)
        ).astype(BF16)

    if shard_width == channels and local % 128 == 0:
        def share(shard):
            made = jnp.dot(hidden[...], down_full[shard], preferred_element_type=F32)
            for t in range(n_tp):
                partials[t, shard] = made[:, t * local : (t + 1) * local].astype(BF16)
            for d in range(1, n_tp):
                peer = other("tp", d)
                remote(
                    partials.at[peer, shard],
                    arrived.at[tp, shard],
                    part_send.at[shard, d - 1],
                    part_recv.at[shard, d - 1],
                    "tp",
                    d,
                ).start()

        share(fs)
        for step in range(n_fs - 1):
            if step >= 1:
                for sub in range(SUBS):
                    serve(2, sub, step)
            for way in range(2):
                settle(2, step, (way,))
                shard, valid = shard_sent(step + 1, way)
                pl.when(valid)(functools.partial(share, shard))
        for shard in range(n_fs):
            from_peers(shard, lambda t: arrived.at[t, shard])
            conclude(shard, slice(shard * local, (shard + 1) * local))
            for d in range(1, n_tp):
                mine = partials.at[other("tp", d), shard]
                remote(
                    mine, mine, part_send.at[shard, d - 1], part_recv.at[shard, d - 1], "tp", d
                ).wait_send()
    else:
        for step in range(n_fs - 1):
            if step >= 1:
                for sub in range(SUBS):
                    serve(2, sub, step)
            settle(2, step)
        for f in range(n_fs):
            made = jnp.dot(hidden[...], down_full[f], preferred_element_type=F32).astype(BF16)
            span = min(local, shard_width)
            for at in range(0, shard_width, span):
                g, channel = divmod(f * shard_width + at, channels)
                t, low = divmod(channel, local)
                partials[t, g, :, low : low + span] = made[:, at : at + span]
        to_peers(0, lambda t: partials.at[t], lambda t: arrived.at[t])
        from_peers(0, lambda t: arrived.at[t])
        for g in range(groups):
            conclude(g, slice(g * local, (g + 1) * local))

    for copy, valid in sent:
        if valid is None:
            copy.wait_send()
        else:
            pl.when(valid)(copy.wait_send)


BAND = 256
PIECES = 4
TOKEN_PARTS = 2


def pair_kernel(
    residual,
    mixer_gain,
    pool_scale,
    channel_gain,
    down_scale,
    gate_scale,
    up_scale,
    gate_taps,
    up_taps,
    pool_own,
    gate_own,
    up_own,
    down_own,
    out,
    stage_own,
    stage_other,
    stage_down,
    stage_down_other,
    stage_pool,
    tokens,
    small_all,
    scales_all,
    pool_near,
    pool_full,
    weights,
    other,
    down_full,
    down_other,
    normed,
    pooled,
    inputs,
    middle,
    hidden,
    keep,
    give,
    got,
    y_out,
    y_in,
    z_out,
    z_in,
    small_send,
    small_recv,
    scale_send,
    scale_recv,
    pz_send,
    pz_recv,
    px_send,
    px_recv,
    pt_send,
    pt_recv,
    rz_send,
    rz_recv,
    ry_send,
    ry_recv,
    rs_send,
    rs_recv,
    gz_send,
    gz_recv,
    gx_send,
    gx_recv,
    dz_send,
    dz_recv,
    dx_send,
    dx_recv,
    core_send,
    core_recv,
    y_send,
    y_recv,
    z_send,
    z_recv,
    local_sem,
):
    rep, fs, tp = (lax.axis_index(name) for name in ("rep", "fs", "tp"))
    length = residual.shape[0]
    groups, pool_rows, local = pool_own.shape
    channels = pool_full.shape[1]
    width = groups * channels
    rows = gate_own.shape[0]
    half_rows = rows // 2
    half_hidden = gate_own.shape[1] // 2
    chunks = half_hidden // 128
    half_columns = down_own.shape[1] // 2
    member = lax.rem(fs, 2)
    side = tp // 2
    core = lax.rem(tp, 2)
    sibling = {"tp": tp + 1 - 2 * core}
    across = {"tp": lax.rem(tp + 2, 4)}
    diagonal = {"tp": 3 - tp}
    mirror = {"rep": 1 - rep}
    same, far, partner = lax.rem(fs + 2, 4), 3 - fs, fs + 1 - 2 * member
    sources = (same, far, partner)
    outer = (fs == 0) | (fs == 3)

    sent = []

    def remote(src, dst, send, recv, device):
        return pltpu.make_async_remote_copy(
            src_ref=src,
            dst_ref=dst,
            send_sem=send,
            recv_sem=recv,
            device_id=device,
            device_id_type=pl.DeviceIdType.MESH,
        )

    def start(*parts):
        copy = remote(*parts)
        sent.append(copy)
        copy.start()

    def aligned(at, size):
        return pl.ds(pl.multiple_of(at, size), size)

    def local_copy(src, dst, idx):
        copy = pltpu.make_async_copy(src, dst, local_sem.at[idx])
        copy.start()
        return copy

    mine = aligned(member * half_hidden, half_hidden)
    theirs = aligned((1 - member) * half_hidden, half_hidden)
    rep_rows = aligned(rep * half_rows, half_rows)
    rep_columns = aligned(rep * half_columns, half_columns)
    load_tokens = local_copy(residual, tokens.at[0, tp], 0)
    load_pool = local_copy(pool_own, stage_pool, 1)
    loads = [
        local_copy(gate_own.at[:, mine], stage_own.at[0], 2),
        local_copy(up_own.at[:, mine], stage_own.at[1], 3),
        local_copy(gate_own.at[rep_rows, theirs], stage_other.at[0], 4),
        local_copy(up_own.at[rep_rows, theirs], stage_other.at[1], 5),
    ]
    load_down = [
        local_copy(down_own.at[mine], stage_down, 6),
        local_copy(down_own.at[theirs, rep_columns], stage_down_other, 7),
    ]

    barrier = pltpu.get_barrier_semaphore()
    peers = (mirror, sibling, across, diagonal) + tuple({"fs": f} for f in sources)
    for device in peers:
        pl.semaphore_signal(
            barrier, inc=1, device_id=device, device_id_type=pl.DeviceIdType.MESH
        )
    small_all[tp, 0] = mixer_gain[...]
    small_all[tp, 1] = pool_scale[...]
    small_all[tp, 2] = channel_gain[...]
    scales_all[fs, 0] = gate_scale[...]
    scales_all[fs, 1] = up_scale[...]
    load_pool.wait()
    pool_near[...] = stage_pool[...].astype(BF16)
    load_tokens.wait()
    pl.semaphore_wait(barrier, len(peers))

    def token_part(slot, t, part):
        span = length // TOKEN_PARTS
        return tokens.at[slot, t, pl.ds(part * span, span)]

    def pool_part(shard, half):
        span = groups // 2
        return pool_full.at[
            pl.ds(half * span, span),
            aligned(shard * pool_rows, pool_rows),
            aligned(tp * local, local),
        ]

    for q, f in enumerate(sources):
        start(
            pool_near.at[pl.ds(rep * (groups // 2), groups // 2)],
            pool_part(fs, rep),
            pz_send.at[q],
            pz_recv.at[q],
            {"fs": f},
        )
    for part in range(TOKEN_PARTS):
        piece = token_part(0, tp, part)
        start(piece, piece, ry_send.at[0, part], ry_recv.at[0, part], across)
        start(piece, piece, rs_send.at[0, part], rs_recv.at[0, part], sibling)
    for at, values in enumerate((mixer_gain, pool_scale, channel_gain)):
        for q, device in enumerate((sibling, across, diagonal)):
            start(values, small_all.at[tp, at], small_send.at[at, q], small_recv.at[at, q], device)
    for at, values in enumerate((gate_scale, up_scale)):
        for q, f in enumerate(sources):
            start(
                values, scales_all.at[fs, at], scale_send.at[at, q], scale_recv.at[at, q], {"fs": f}
            )
    pool_copy = local_copy(
        pool_near,
        pool_full.at[:, aligned(fs * pool_rows, pool_rows), aligned(tp * local, local)],
        8,
    )

    def chunk_target(j, shard, half):
        return weights.at[j, shard, aligned(half * half_rows, half_rows)]

    def chunk_copies(j):
        target = chunk_target(j, fs, rep)
        return [
            remote(source, target, gz_send.at[j, q], gz_recv.at[j, q], {"fs": f})
            for q, (source, f) in enumerate(
                ((target, same), (other.at[j], far), (other.at[j], partner))
            )
        ]

    for load in loads:
        load.wait()

    @pl.loop(0, chunks)
    def _(j):
        columns = aligned(j * 128, 128)
        for at in range(2):
            lanes = slice(at * 128, (at + 1) * 128)
            weights[j, fs, :, lanes] = stage_own[at, :, columns].astype(BF16)
            other[j, :, lanes] = stage_other[at, :, columns].astype(BF16)
        for copy in chunk_copies(j):
            copy.start()

        @pl.when(j == 0)
        def _():
            for part in range(TOKEN_PARTS):
                remote(
                    token_part(0, tp, part),
                    token_part(1, tp, part),
                    rz_send.at[part],
                    rz_recv.at[part],
                    {"fs": partner},
                ).start()

    for load in load_down:
        load.wait()
    for half in range(2):
        down_full[fs, half] = stage_down[
            :, half * half_columns : (half + 1) * half_columns
        ].astype(BF16)
    down_other[...] = stage_down_other[...].astype(BF16)

    def down_part(shard, half, sub):
        span = half_hidden // PIECES
        return down_full.at[shard, half, pl.ds(sub * span, span)]

    for q, f in enumerate(sources):
        for sub in range(PIECES):
            span = half_hidden // PIECES
            source = (
                down_part(fs, rep, sub) if q == 0 else down_other.at[pl.ds(sub * span, span)]
            )
            start(
                source,
                down_part(fs, rep, sub),
                dz_send.at[q, sub],
                dz_recv.at[q, sub],
                {"fs": f},
            )

    def landed(ref, send, recv):
        remote(ref, ref, send, recv, mirror).wait_recv()

    for q, f in enumerate(sources):
        piece = pool_part(f, rep)
        landed(piece, pz_send.at[q], pz_recv.at[q])
        start(piece, piece, px_send.at[q], px_recv.at[q], mirror)
    for q, f in enumerate(sources):
        landed(pool_part(f, 1 - rep), px_send.at[q], px_recv.at[q])
    pool_copy.wait()

    def pool_slab(t):
        return pool_full.at[:, :, aligned(t * local, local)]

    slab = pool_slab(tp)
    start(slab, slab, pt_send.at[1], pt_recv.at[1], across)
    start(slab, slab, pt_send.at[0], pt_recv.at[0], sibling)

    def forward_chunk(j, do_start):
        for q, f in enumerate(sources):
            piece = chunk_target(j, f, rep)
            landed(piece, gz_send.at[j, q], gz_recv.at[j, q])
            do_start(piece, piece, gx_send.at[j, q], gx_recv.at[j, q], mirror)

    t_sibling, t_across, t_diagonal = sibling["tp"], across["tp"], diagonal["tp"]
    for part in range(TOKEN_PARTS):
        piece = token_part(0, t_across, part)
        landed(piece, ry_send.at[0, part], ry_recv.at[0, part])
        start(piece, piece, rs_send.at[1, part], rs_recv.at[1, part], sibling)
    forward_chunk(0, start)
    for part in range(TOKEN_PARTS):
        piece = token_part(1, tp, part)
        landed(piece, rz_send.at[part], rz_recv.at[part])
        start(piece, piece, ry_send.at[1, part], ry_recv.at[1, part], across)
        start(piece, piece, rs_send.at[2, part], rs_recv.at[2, part], sibling)
    slab = pool_slab(t_across)
    landed(slab, pt_send.at[1], pt_recv.at[1])
    start(slab, slab, pt_send.at[2], pt_recv.at[2], sibling)
    for part in range(TOKEN_PARTS):
        landed(token_part(0, t_sibling, part), rs_send.at[0, part], rs_recv.at[0, part])
        landed(token_part(0, t_diagonal, part), rs_send.at[1, part], rs_recv.at[1, part])
    for at in range(3):
        for q, t in enumerate((t_sibling, t_across, t_diagonal)):
            landed(small_all.at[t, at], small_send.at[at, q], small_recv.at[at, q])
    landed(pool_slab(t_sibling), pt_send.at[0], pt_recv.at[0])
    landed(pool_slab(t_diagonal), pt_send.at[2], pt_recv.at[2])

    positions = lax.broadcasted_iota(jnp.int32, (BAND, 1), 0).astype(F32) + 1.0
    distance = (
        lax.broadcasted_iota(jnp.int32, (BAND, 2 * BAND), 0)
        + BAND
        - lax.broadcasted_iota(jnp.int32, (BAND, 2 * BAND), 1)
    )

    def mix(slot):
        span = slice(slot * length, (slot + 1) * length)
        square = jnp.zeros((length, local), F32)
        for t in range(4):
            for g in range(groups):
                values = tokens[slot, t, :, g * local : (g + 1) * local].astype(F32)
                square = square + values * values
        factor = lax.rsqrt(jnp.sum(square, axis=1, keepdims=True) / width + EPSILON)
        square = jnp.zeros((length, local), F32)
        for g in range(groups):
            part = slice(g * local, (g + 1) * local)
            for t in range(4):
                values = tokens[slot, t, :, part].astype(F32)
                normed[:, t * local : (t + 1) * local] = (
                    values * factor * small_all[t, 0, g : g + 1]
                ).astype(BF16)
            band = jnp.where((distance >= 0) & (distance < WINDOWS[g]), 1.0, 0.0).astype(BF16)
            for b in range(length // BAND):
                here = slice(b * BAND, (b + 1) * BAND)
                if b == 0:
                    totals = jnp.dot(band[:, BAND:], normed[here], preferred_element_type=F32)
                    totals = totals / jnp.minimum(positions, float(WINDOWS[g]))
                else:
                    totals = jnp.dot(
                        band,
                        normed[(b - 1) * BAND : (b + 1) * BAND],
                        preferred_element_type=F32,
                    ) * (1.0 / WINDOWS[g])
                pooled[here] = (totals - normed[here].astype(F32)).astype(BF16)
            mixed = jnp.dot(pooled[...], pool_full[g], preferred_element_type=F32)
            for t in range(4):
                made = (
                    mixed[:, t * local : (t + 1) * local] * small_all[t, 1, g : g + 1]
                    + tokens[slot, t, :, part].astype(F32)
                ).astype(BF16)
                inputs[span, g * channels + t * local : g * channels + (t + 1) * local] = made
                values = made.astype(F32)
                square = square + values * values
        factor = lax.rsqrt(jnp.sum(square, axis=1, keepdims=True) / width + EPSILON)
        if slot == 0:
            for g in range(groups):
                middle[:, g * local : (g + 1) * local] = inputs[
                    span, aligned(g * channels + tp * local, local)
                ]
        for g in range(groups):
            for t in range(4):
                columns = slice(g * channels + t * local, g * channels + (t + 1) * local)
                inputs[span, columns] = (
                    inputs[span, columns].astype(F32) * factor * small_all[t, 2, g : g + 1]
                ).astype(BF16)

    mix(0)
    forward_chunk(1, start)
    for part in range(TOKEN_PARTS):
        piece = token_part(1, t_across, part)
        landed(piece, ry_send.at[1, part], ry_recv.at[1, part])
        start(piece, piece, rs_send.at[3, part], rs_recv.at[3, part], sibling)
    for part in range(TOKEN_PARTS):
        landed(token_part(1, t_sibling, part), rs_send.at[2, part], rs_recv.at[2, part])
        landed(token_part(1, t_diagonal, part), rs_send.at[3, part], rs_recv.at[3, part])
    forward_chunk(2, start)
    mix(1)
    forward_chunk(3, start)
    for at in range(2):
        for q, f in enumerate(sources):
            landed(scales_all.at[f, at], scale_send.at[at, q], scale_recv.at[at, q])

    ahead = 4
    thirds = scales_all.shape[3] // 128

    def start_only(*parts):
        remote(*parts).start()

    @pl.loop(0, chunks)
    def _(j):
        for q, f in enumerate(sources):
            landed(chunk_target(j, f, 1 - rep), gx_send.at[j, q], gx_recv.at[j, q])
        here = aligned(member * half_hidden + j * 128, 128)
        unit = member * chunks + j
        scale_at = aligned(lax.rem(unit, thirds) * 128, 128)
        taps = [
            table[:, here] * scales_all[unit // thirds, at, :, scale_at]
            for at, table in enumerate((gate_taps, up_taps))
        ]
        block = weights[j].reshape(width, 256)
        for slot in range(2):
            span = slice(slot * length, (slot + 1) * length)
            made = jnp.dot(inputs[span], block, preferred_element_type=F32)
            conv_gate = causal_taps(made[:, :128], taps[0])
            conv_up = causal_taps(made[:, 128:], taps[1])
            silu = conv_gate / (1.0 + jnp.exp(-conv_gate))
            hidden[span, aligned(j * 128, 128)] = (silu * conv_up).astype(BF16)

        @pl.when(j + ahead < chunks)
        def _():
            forward_chunk(j + ahead, start_only)

    kinds = (jnp.where(outer, 2, 1), jnp.int32(0), jnp.where(outer, 1, 2))
    shard_order = (
        fs,
        jnp.where(outer, partner, far),
        same,
        jnp.where(outer, far, partner),
    )

    def product(shard, half):
        for slot in (1, 0):
            span = slice(slot * length, (slot + 1) * length)
            made = jnp.dot(hidden[span], down_full[shard, half], preferred_element_type=F32)
            low, high = made[:, :local], made[:, local:]
            keep[shard, half, span] = jnp.where(core == 0, low, high)
            give[shard, half, span] = jnp.where(core == 0, high, low).astype(BF16)
        start(
            give.at[shard, half],
            got.at[shard, half],
            core_send.at[shard, half],
            core_recv.at[shard, half],
            sibling,
        )

    def y_copy(shard):
        return remote(y_out.at[shard], y_in.at[shard], y_send.at[shard], y_recv.at[shard], across)

    def join_cores(shard, half):
        landed(got.at[shard, half], core_send.at[shard, half], core_recv.at[shard, half])
        total = keep[shard, half] + got[shard, half].astype(F32)

        @pl.when(half == side)
        def _():
            keep[shard, half] = total

        @pl.when(half != side)
        def _():
            y_out[shard] = total.astype(BF16)
            y_copy(shard).start()

    def join_sides(shard):
        landed(y_in.at[shard], y_send.at[shard], y_recv.at[shard])
        total = keep[shard, side] + y_in[shard].astype(F32)
        z_out[shard] = total[length:].astype(BF16)
        start(
            z_out.at[shard],
            z_in.at[shard],
            z_send.at[shard],
            z_recv.at[shard],
            {"fs": partner},
        )
        keep[shard, side, :length] = total[:length]

    def conclude(shard):
        landed(z_in.at[shard], z_send.at[shard], z_recv.at[shard])
        columns = aligned(shard * local, local)
        total = keep[shard, side, :length] + z_in[shard].astype(F32)
        out[:, columns] = (
            total * down_scale[pl.ds(shard, 1), :] + middle[:, columns].astype(F32)
        ).astype(BF16)

    product(fs, rep)
    product(fs, 1 - rep)
    join_cores(fs, rep)
    for k in range(1, 4):
        shard, q = shard_order[k], kinds[k - 1]
        before = shard_order[k - 1]
        for sub in range(PIECES):
            piece = down_part(shard, rep, sub)
            landed(piece, dz_send.at[q, sub], dz_recv.at[q, sub])
            start(piece, piece, dx_send.at[q, sub], dx_recv.at[q, sub], mirror)
        product(shard, rep)
        join_cores(before, 1 - rep)
        for sub in range(PIECES):
            landed(
                down_part(shard, 1 - rep, sub), dx_send.at[q, sub], dx_recv.at[q, sub]
            )
        product(shard, 1 - rep)
        join_cores(shard, rep)
        join_sides(before)
    last = shard_order[3]
    join_cores(last, 1 - rep)
    join_sides(last)
    conclude(partner)
    conclude(jnp.where(outer, same, fs))
    conclude(far)
    conclude(jnp.where(outer, fs, same))

    for copy in sent:
        copy.wait_send()
    for part in range(TOKEN_PARTS):
        piece = token_part(0, tp, part)
        remote(piece, piece, rz_send.at[part], rz_recv.at[part], {"fs": partner}).wait_send()
    for shard in range(4):
        y_copy(shard).wait_send()

    @pl.loop(0, chunks)
    def _(j):
        for copy in chunk_copies(j):
            copy.wait_send()

        @pl.when(j >= ahead)
        def _():
            for q, f in enumerate(sources):
                piece = chunk_target(j, f, rep)
                remote(piece, piece, gx_send.at[j, q], gx_recv.at[j, q], mirror).wait_send()


def pair_shards(
    residual,
    mixer_gain,
    pool_weight,
    pool_scale,
    channel_gain,
    gate_weight,
    up_weight,
    gate_scale,
    up_scale,
    gate_taps,
    up_taps,
    down_weight,
    down_scale,
):
    _, length, groups, local = residual.shape
    channels = local * 4
    width = groups * channels
    rows, hidden_width = gate_weight.shape
    half = hidden_width // 2
    chunks = half // 128
    half_columns = down_weight.shape[1] // 2
    vmem = pl.BlockSpec(memory_space=pltpu.VMEM)
    anywhere = pl.BlockSpec(memory_space=pl.ANY)
    dma = pltpu.SemaphoreType.DMA
    pairs = [
        (3, 3),
        (2, 3),
        (3,),
        (3,),
        (3,),
        (TOKEN_PARTS,),
        (2, TOKEN_PARTS),
        (4, TOKEN_PARTS),
        (chunks, 3),
        (chunks, 3),
        (3, PIECES),
        (3, PIECES),
        (4, 2),
        (4,),
        (4,),
    ]
    out = pl.pallas_call(
        pair_kernel,
        out_shape=jax.ShapeDtypeStruct((length, groups * local), BF16),
        in_specs=[anywhere] + [vmem] * 8 + [anywhere] * 4,
        out_specs=vmem,
        scratch_shapes=[
            pltpu.VMEM((2, rows, half), F32),
            pltpu.VMEM((2, rows // 2, half), F32),
            pltpu.VMEM((half, 2 * half_columns), F32),
            pltpu.VMEM((half, half_columns), F32),
            pltpu.VMEM(pool_weight.shape, F32),
            pltpu.VMEM((2, 4, length, groups * local), BF16),
            pltpu.VMEM((4, 3, groups, local), F32),
            pltpu.VMEM((4, 2) + gate_scale.shape, F32),
            pltpu.VMEM(pool_weight.shape, BF16),
            pltpu.VMEM((groups, channels, channels), BF16),
            pltpu.VMEM((chunks, 4, rows, 256), BF16),
            pltpu.VMEM((chunks, rows // 2, 256), BF16),
            pltpu.VMEM((4, 2, half, half_columns), BF16),
            pltpu.VMEM((half, half_columns), BF16),
            pltpu.VMEM((length, channels), BF16),
            pltpu.VMEM((length, channels), BF16),
            pltpu.VMEM((2 * length, width), BF16),
            pltpu.VMEM((length, groups * local), BF16),
            pltpu.VMEM((2 * length, half), BF16),
            pltpu.VMEM((4, 2, 2 * length, local), F32),
            pltpu.VMEM((4, 2, 2 * length, local), BF16),
            pltpu.VMEM((4, 2, 2 * length, local), BF16),
            pltpu.VMEM((4, 2 * length, local), BF16),
            pltpu.VMEM((4, 2 * length, local), BF16),
            pltpu.VMEM((4, length, local), BF16),
            pltpu.VMEM((4, length, local), BF16),
        ]
        + [dma(shape) for shape in pairs for _ in range(2)]
        + [dma((9,))],
        compiler_params=pltpu.CompilerParams(
            collective_id=0, has_side_effects=True, vmem_limit_bytes=VMEM_BYTES
        ),
    )(
        residual.reshape(length, groups * local),
        mixer_gain,
        pool_scale,
        channel_gain,
        down_scale,
        gate_scale,
        up_scale,
        gate_taps,
        up_taps,
        pool_weight,
        gate_weight,
        up_weight,
        down_weight,
    )
    return out.reshape(1, length, groups, local)


def paired(sizes, residual, gate_weight, down_weight):
    _, length, groups, local = residual
    return (
        sizes == (2, 4, 4)
        and residual[0] == 1
        and local == 128
        and length % BAND == 0
        and groups == len(WINDOWS)
        and down_weight[1] == 4 * local
        and gate_weight[0] * 4 == groups * local * 4
        and gate_weight[1] % 512 == 0
    )


def shards(
    sizes,
    residual,
    mixer_gain,
    pool_weight,
    pool_scale,
    channel_gain,
    gate_weight,
    up_weight,
    gate_scale,
    up_scale,
    gate_taps,
    up_taps,
    down_weight,
    down_scale,
):
    if paired(sizes, residual.shape, gate_weight.shape, down_weight.shape):
        return pair_shards(
            residual,
            mixer_gain,
            pool_weight,
            pool_scale,
            channel_gain,
            gate_weight,
            up_weight,
            gate_scale,
            up_scale,
            gate_taps,
            up_taps,
            down_weight,
            down_scale,
        )
    n_rep, n_fs, n_tp = sizes
    _, length, groups, local = residual.shape
    channels = local * n_tp
    width = groups * channels
    own_width = groups * local
    hidden_width = gate_weight.shape[1]
    vmem = pl.BlockSpec(memory_space=pltpu.VMEM)
    anywhere = pl.BlockSpec(memory_space=pl.ANY)
    dma = pltpu.SemaphoreType.DMA
    hops = max(n_fs - 1, 1)
    reps = max(n_rep - 1, 1)
    peers = max(n_tp - 1, 1)
    out = pl.pallas_call(
        functools.partial(block_kernel, sizes),
        out_shape=jax.ShapeDtypeStruct((length, own_width), BF16),
        in_specs=[vmem] * 8 + [anywhere] * 3,
        out_specs=vmem,
        scratch_shapes=[
            pltpu.VMEM((groups, channels, local), BF16),
            pltpu.VMEM((n_fs,) + gate_weight.shape, BF16),
            pltpu.VMEM((n_fs,) + up_weight.shape, BF16),
            pltpu.VMEM((n_fs,) + down_weight.shape, BF16),
            pltpu.VMEM((n_tp, length, own_width), BF16),
            pltpu.VMEM((n_tp, length, own_width), BF16),
            pltpu.VMEM((n_tp, 2, own_width), F32),
            pltpu.VMEM((n_fs, 2, gate_scale.shape[1]), F32),
            pltpu.VMEM((2, hidden_width), F32),
            pltpu.VMEM((length, channels), BF16),
            pltpu.VMEM((length, own_width), BF16),
            pltpu.VMEM((length, width), BF16),
            pltpu.VMEM((length, hidden_width), BF16),
            pltpu.VMEM((length, hidden_width), BF16),
            pltpu.VMEM((n_tp, groups, length, local), BF16),
            pltpu.VMEM((n_tp, groups, length, local), BF16),
            dma((3, SUBS, 2 * hops)),
            dma((3, SUBS, 2 * hops)),
            dma((3, SUBS, 2 * hops, reps)),
            dma((3, SUBS, 2 * hops, reps)),
            dma((hops,)),
            dma((hops,)),
            dma((hops, reps)),
            dma((hops, reps)),
            dma((hops,)),
            dma((hops,)),
            dma((3, peers)),
            dma((3, peers)),
            dma((n_fs, peers)),
            dma((n_fs, peers)),
            dma((7,)),
        ],
        compiler_params=pltpu.CompilerParams(
            collective_id=0, has_side_effects=True, vmem_limit_bytes=60 * 1024 * 1024
        ),
    )(
        residual.reshape(length, own_width),
        jnp.stack([mixer_gain.reshape(-1), channel_gain.reshape(-1)]),
        pool_scale.reshape(1, -1),
        down_scale.reshape(1, -1),
        jnp.concatenate([gate_scale, up_scale], axis=0),
        gate_taps,
        up_taps,
        pool_weight.astype(BF16),
        gate_weight.astype(BF16),
        up_weight.astype(BF16),
        down_weight.astype(BF16),
    )
    return out.reshape(1, length, groups, local)


def solution(mesh):
    placed = (
        P(("rep", "fs"), None, None, "tp"),
        P(None, "tp"),
        P(None, "fs", "tp"),
        P(None, "tp"),
        P(None, "tp"),
        P("fs", "tp"),
        P("fs", "tp"),
        P("fs", "tp"),
        P("fs", "tp"),
        P(None, "tp"),
        P(None, "tp"),
        P("tp", "fs"),
        P(None, "tp"),
    )
    sizes = tuple(mesh.shape[name] for name in ("rep", "fs", "tp"))
    return jax.shard_map(
        functools.partial(shards, sizes),
        mesh=mesh,
        in_specs=placed,
        out_specs=P(("rep", "fs"), None, None, "tp"),
        check_vma=False,
    )
```

```python
import functools

import jax
import jax.numpy as jnp
from jax import lax
from jax.experimental import pallas as pl
from jax.experimental.pallas import tpu as pltpu
from jax.sharding import PartitionSpec as P

WINDOWS = (2, 4, 8, 16)
EPSILON = 1e-05
SUBS = 2
COLUMNS = 256
VMEM_BYTES = 62 * 1024 * 1024
F32 = jnp.float32
BF16 = jnp.bfloat16


def delayed(values, steps):
    rows = lax.broadcasted_iota(jnp.int32, values.shape, 0)
    return jnp.where(rows >= steps, pltpu.roll(values, steps, 0), 0.0)


def causal_taps(values, taps):
    return taps[2:3] * values + taps[1:2] * delayed(values, 1) + taps[0:1] * delayed(values, 2)


def block_kernel(
    sizes,
    residual,
    gains,
    pool_scale,
    down_scale,
    scale_pair,
    gate_taps,
    up_taps,
    pool_own,
    gate_own,
    up_own,
    down_own,
    out,
    pool_full,
    gate_full,
    up_full,
    down_full,
    gathered,
    middle_all,
    gains_all,
    scales_all,
    scale_row,
    pooled,
    middle,
    inputs,
    gate_pre,
    hidden,
    partials,
    arrived,
    ring_send,
    ring_recv,
    rep_send,
    rep_recv,
    pool_send,
    pool_recv,
    pool_rep_send,
    pool_rep_recv,
    scale_send,
    scale_recv,
    tp_send,
    tp_recv,
    part_send,
    part_recv,
    local_sem,
):
    n_rep, n_fs, n_tp = sizes
    rep, fs, tp = (lax.axis_index(name) for name in ("rep", "fs", "tp"))
    length = residual.shape[0]
    groups = pool_full.shape[0]
    channels = pool_full.shape[1]
    local = residual.shape[1] // groups
    width = groups * channels

    def other(axis, offset):
        me, count = {"rep": (rep, n_rep), "fs": (fs, n_fs), "tp": (tp, n_tp)}[axis]
        return lax.rem(me + offset, count)

    def remote(src, dst, send, recv, axis, offset):
        return pltpu.make_async_remote_copy(
            src_ref=src,
            dst_ref=dst,
            send_sem=send,
            recv_sem=recv,
            device_id={axis: other(axis, offset)},
            device_id_type=pl.DeviceIdType.MESH,
        )

    barrier = pltpu.get_barrier_semaphore()
    for axis, count in (("rep", n_rep), ("fs", n_fs), ("tp", n_tp)):
        for offset in range(1, count):
            pl.semaphore_signal(
                barrier,
                inc=1,
                device_id={axis: other(axis, offset)},
                device_id_type=pl.DeviceIdType.MESH,
            )
    pl.semaphore_wait(barrier, n_rep + n_fs + n_tp - 3)

    sent = []

    def start(copy, valid=None):
        sent.append((copy, valid))
        if valid is None:
            copy.start()
        else:
            pl.when(valid)(copy.start)

    weights = ((gate_own, gate_full), (up_own, up_full), (down_own, down_full))

    def piece(w, shard, half, sub, own=False):
        rows = weights[w][0].shape[0] // (n_rep * SUBS)
        part = pl.ds(pl.multiple_of((half * SUBS + sub) * rows, rows), rows)
        return weights[w][0].at[part] if own else weights[w][1].at[shard, part]

    def shard_sent(step, way):
        shard = fs + step if way else fs - step
        return jnp.clip(shard, 0, n_fs - 1), (shard <= n_fs - 1 if way else shard >= 0)

    def line(w, sub, step):
        for way in range(2):
            shard, valid = shard_sent(step, way)
            start(
                remote(
                    piece(w, shard, rep, sub, own=step == 0),
                    piece(w, shard, rep, sub),
                    ring_send.at[w, sub, 2 * step + way],
                    ring_recv.at[w, sub, 2 * step + way],
                    "fs",
                    n_fs - 1 if way else 1,
                ),
                valid & (fs > 0 if way else fs < n_fs - 1),
            )

    def serve(w, sub, step):
        for way in range(2):
            shard, valid = shard_sent(step + 1, way)
            mine = piece(w, shard, rep, sub)
            sems = (w, sub, 2 * step + way)
            pl.when(valid)(
                remote(
                    mine, mine, ring_send.at[sems], ring_recv.at[sems], "fs", 1
                ).wait_recv
            )
            if step < n_fs - 2:
                onward = (w, sub, 2 * step + 2 + way)
                start(
                    remote(
                        mine,
                        mine,
                        ring_send.at[onward],
                        ring_recv.at[onward],
                        "fs",
                        n_fs - 1 if way else 1,
                    ),
                    valid & (fs > 0 if way else fs < n_fs - 1),
                )
            for d in range(1, n_rep):
                start(
                    remote(
                        mine,
                        mine,
                        rep_send.at[sems + (d - 1,)],
                        rep_recv.at[sems + (d - 1,)],
                        "rep",
                        d,
                    ),
                    valid,
                )

    def settle(w, step, ways=(0, 1)):
        for way in ways:
            shard, valid = shard_sent(step + 1, way)

            @pl.when(valid)
            def _():
                for sub in range(SUBS):
                    for d in range(1, n_rep):
                        got = piece(w, shard, other("rep", n_rep - d), sub)
                        sems = (w, sub, 2 * step + way, d - 1)
                        remote(
                            got, got, rep_send.at[sems], rep_recv.at[sems], "rep", d
                        ).wait_recv()

    def local_copy(src, dst, idx):
        copy = pltpu.make_async_copy(src, dst, local_sem.at[idx])
        copy.start()
        return copy

    own_copies = [
        local_copy(residual, gathered.at[tp], 0),
        local_copy(gains, gains_all.at[tp], 1),
        local_copy(scale_pair, scales_all.at[fs], 2),
        local_copy(gate_own, gate_full.at[fs], 3),
        local_copy(up_own, up_full.at[fs], 4),
        local_copy(down_own, down_full.at[fs], 5),
    ]

    pool_rows = pool_own.shape[1]
    rep_groups = groups // n_rep

    def pool_part(shard, half):
        return pool_full.at[
            pl.ds(half * rep_groups, rep_groups),
            pl.ds(pl.multiple_of(shard * pool_rows, pool_rows), pool_rows),
        ]

    pool_copy = local_copy(
        pool_own, pool_full.at[:, pl.ds(pl.multiple_of(fs * pool_rows, pool_rows), pool_rows)], 6
    )

    for d in range(1, n_fs):
        start(
            remote(
                pool_own.at[pl.ds(rep * rep_groups, rep_groups)],
                pool_part(fs, rep),
                pool_send.at[d - 1],
                pool_recv.at[d - 1],
                "fs",
                d,
            )
        )
    for w in (0, 1):
        for sub in range(SUBS):
            if n_fs > 1:
                line(w, sub, 0)
    for d in range(1, n_tp):
        start(remote(gains, gains_all.at[tp], tp_send.at[0, d - 1], tp_recv.at[0, d - 1], "tp", d))
    for d in range(1, n_tp):
        start(
            remote(residual, gathered.at[tp], tp_send.at[1, d - 1], tp_recv.at[1, d - 1], "tp", d)
        )
    for d in range(1, n_fs):
        start(
            remote(
                scale_pair, scales_all.at[fs], scale_send.at[d - 1], scale_recv.at[d - 1], "fs", d
            )
        )

    for d in range(1, n_fs):
        shard = other("fs", n_fs - d)
        mine = pool_part(shard, rep)
        remote(mine, mine, pool_send.at[d - 1], pool_recv.at[d - 1], "fs", d).wait_recv()
        for e in range(1, n_rep):
            start(
                remote(
                    mine,
                    mine,
                    pool_rep_send.at[d - 1, e - 1],
                    pool_rep_recv.at[d - 1, e - 1],
                    "rep",
                    e,
                )
            )
    for d in range(1, n_fs):
        shard = other("fs", n_fs - d)
        for e in range(1, n_rep):
            got = pool_part(shard, other("rep", n_rep - e))
            remote(
                got,
                got,
                pool_rep_send.at[d - 1, e - 1],
                pool_rep_recv.at[d - 1, e - 1],
                "rep",
                e,
            ).wait_recv()
    pool_copy.wait()
    for copy in own_copies:
        copy.wait()

    def tp_arrivals(idx, buffer):
        for d in range(1, n_tp):
            got = buffer.at[other("tp", n_tp - d)]
            remote(got, got, tp_send.at[idx, d - 1], tp_recv.at[idx, d - 1], "tp", d).wait_recv()

    for sub in range(SUBS):
        serve(0, sub, 0)
    tp_arrivals(0, gains_all)
    tp_arrivals(1, gathered)
    for sub in range(SUBS):
        serve(1, sub, 0)

    def mean_square_root(buffer):
        total = jnp.zeros((length, 1), F32)
        for t in range(n_tp):
            values = buffer[t].astype(F32)
            total = total + jnp.sum(values * values, axis=1, keepdims=True)
        return lax.rsqrt(total / width + EPSILON)

    factor = mean_square_root(gathered)
    positions = lax.broadcasted_iota(jnp.int32, (length, 1), 0).astype(F32) + 1.0
    for g in range(groups):
        part = slice(g * local, (g + 1) * local)
        share = 1.0 / jnp.minimum(positions, float(WINDOWS[g]))
        for t in range(n_tp):
            values = gathered[t, :, part].astype(F32)
            normed = (values * factor * gains_all[t, 0:1, part]).astype(BF16).astype(F32)
            totals = normed
            reach = 1
            while reach < WINDOWS[g]:
                totals = totals + delayed(totals, reach)
                reach = reach * 2
            pooled[:, t * local : (t + 1) * local] = (totals * share - normed).astype(BF16)
        mixed = jnp.dot(pooled[...], pool_full[g], preferred_element_type=F32)
        middle[:, part] = (
            mixed * pool_scale[:, part] + residual[:, part].astype(F32)
        ).astype(BF16)

    middle_copy = local_copy(middle, middle_all.at[tp], 0)
    for d in range(1, n_tp):
        start(
            remote(middle, middle_all.at[tp], tp_send.at[2, d - 1], tp_recv.at[2, d - 1], "tp", d)
        )
    for step in range(1, n_fs - 1):
        for w in (0, 1):
            if step == n_fs - 2 and n_fs > 2:
                break
            for sub in range(SUBS):
                serve(w, sub, step)
    for sub in range(SUBS):
        if n_fs > 1:
            line(2, sub, 0)
    for d in range(1, n_fs):
        got = scales_all.at[other("fs", n_fs - d)]
        remote(got, got, scale_send.at[d - 1], scale_recv.at[d - 1], "fs", d).wait_recv()
    shard_columns = scale_pair.shape[1]
    for f in range(n_fs):
        scale_row[:, f * shard_columns : (f + 1) * shard_columns] = scales_all[f]

    middle_copy.wait()
    tp_arrivals(2, middle_all)
    factor = mean_square_root(middle_all)
    for t in range(n_tp):
        for g in range(groups):
            part = slice(g * local, (g + 1) * local)
            start_column = g * channels + t * local
            inputs[:, start_column : start_column + local] = (
                middle_all[t, :, part].astype(F32) * factor * gains_all[t, 1:2, part]
            ).astype(BF16)

    def finish(w):
        if n_fs > 2:
            for sub in range(SUBS):
                serve(w, sub, n_fs - 2)
        for step in range(n_fs - 1):
            settle(w, step)

    def product(full, columns, row):
        block = full[:, :, columns].reshape(width, COLUMNS)
        made = jnp.dot(inputs[...], block, preferred_element_type=F32)
        return (made * scale_row[row : row + 1, columns]).astype(BF16)

    chunks = gate_full.shape[2] // COLUMNS

    finish(0)

    @pl.loop(0, chunks)
    def _(j):
        columns = pl.ds(pl.multiple_of(j * COLUMNS, COLUMNS), COLUMNS)
        gate_pre[:, columns] = product(gate_full, columns, 0)

    finish(1)
    for sub in range(SUBS):
        if n_fs > 1:
            serve(2, sub, 0)

    @pl.loop(0, chunks)
    def _(j):
        columns = pl.ds(pl.multiple_of(j * COLUMNS, COLUMNS), COLUMNS)
        up_values = product(up_full, columns, 1).astype(F32)
        conv_gate = causal_taps(gate_pre[:, columns].astype(F32), gate_taps[:, columns])
        conv_up = causal_taps(up_values, up_taps[:, columns])
        silu = conv_gate / (1.0 + jnp.exp(-conv_gate))
        hidden[:, columns] = (silu * conv_up).astype(BF16)

    shard_width = down_own.shape[1]

    def to_peers(idx, src, dst):
        for d in range(1, n_tp):
            start(
                remote(
                    src(other("tp", d)),
                    dst(tp),
                    part_send.at[idx, d - 1],
                    part_recv.at[idx, d - 1],
                    "tp",
                    d,
                )
            )

    def from_peers(idx, dst):
        for d in range(1, n_tp):
            got = dst(other("tp", n_tp - d))
            remote(
                got, got, part_send.at[idx, d - 1], part_recv.at[idx, d - 1], "tp", d
            ).wait_recv()

    def conclude(g, columns):
        total = partials[tp, g].astype(F32)
        for d in range(1, n_tp):
            total = total + arrived[other("tp", d), g].astype(F32)
        out[:, columns] = (
            total * down_scale[:, columns] + middle[:, columns].astype(F32)
        ).astype(BF16)

    if shard_width == channels and local % 128 == 0:
        def share(shard):
            made = jnp.dot(hidden[...], down_full[shard], preferred_element_type=F32)
            for t in range(n_tp):
                partials[t, shard] = made[:, t * local : (t + 1) * local].astype(BF16)
            for d in range(1, n_tp):
                peer = other("tp", d)
                remote(
                    partials.at[peer, shard],
                    arrived.at[tp, shard],
                    part_send.at[shard, d - 1],
                    part_recv.at[shard, d - 1],
                    "tp",
                    d,
                ).start()

        share(fs)
        for step in range(n_fs - 1):
            if step >= 1:
                for sub in range(SUBS):
                    serve(2, sub, step)
            for way in range(2):
                settle(2, step, (way,))
                shard, valid = shard_sent(step + 1, way)
                pl.when(valid)(functools.partial(share, shard))
        for shard in range(n_fs):
            from_peers(shard, lambda t: arrived.at[t, shard])
            conclude(shard, slice(shard * local, (shard + 1) * local))
            for d in range(1, n_tp):
                mine = partials.at[other("tp", d), shard]
                remote(
                    mine, mine, part_send.at[shard, d - 1], part_recv.at[shard, d - 1], "tp", d
                ).wait_send()
    else:
        for step in range(n_fs - 1):
            if step >= 1:
                for sub in range(SUBS):
                    serve(2, sub, step)
            settle(2, step)
        for f in range(n_fs):
            made = jnp.dot(hidden[...], down_full[f], preferred_element_type=F32).astype(BF16)
            span = min(local, shard_width)
            for at in range(0, shard_width, span):
                g, channel = divmod(f * shard_width + at, channels)
                t, low = divmod(channel, local)
                partials[t, g, :, low : low + span] = made[:, at : at + span]
        to_peers(0, lambda t: partials.at[t], lambda t: arrived.at[t])
        from_peers(0, lambda t: arrived.at[t])
        for g in range(groups):
            conclude(g, slice(g * local, (g + 1) * local))

    for copy, valid in sent:
        if valid is None:
            copy.wait_send()
        else:
            pl.when(valid)(copy.wait_send)


BAND = 256
PIECES = 4
TOKEN_PARTS = 2


def pair_kernel(
    residual,
    mixer_gain,
    pool_scale,
    channel_gain,
    down_scale,
    gate_scale,
    up_scale,
    gate_taps,
    up_taps,
    pool_own,
    gate_own,
    up_own,
    down_own,
    out,
    stage_own,
    stage_other,
    stage_down,
    stage_down_other,
    stage_pool,
    tokens,
    small_all,
    scales_all,
    pool_near,
    pool_full,
    weights,
    other,
    down_full,
    down_other,
    normed,
    pooled,
    inputs,
    middle,
    hidden,
    keep,
    give,
    got,
    y_out,
    y_in,
    z_out,
    z_in,
    small_send,
    small_recv,
    scale_send,
    scale_recv,
    pz_send,
    pz_recv,
    px_send,
    px_recv,
    pt_send,
    pt_recv,
    rz_send,
    rz_recv,
    ry_send,
    ry_recv,
    rs_send,
    rs_recv,
    gz_send,
    gz_recv,
    gx_send,
    gx_recv,
    dz_send,
    dz_recv,
    dx_send,
    dx_recv,
    core_send,
    core_recv,
    y_send,
    y_recv,
    z_send,
    z_recv,
    local_sem,
):
    rep, fs, tp = (lax.axis_index(name) for name in ("rep", "fs", "tp"))
    length = residual.shape[0]
    groups, pool_rows, local = pool_own.shape
    channels = pool_full.shape[1]
    width = groups * channels
    rows = gate_own.shape[0]
    half_rows = rows // 2
    half_hidden = gate_own.shape[1] // 2
    chunks = half_hidden // 128
    half_columns = down_own.shape[1] // 2
    member = lax.rem(fs, 2)
    side = tp // 2
    core = lax.rem(tp, 2)
    sibling = {"tp": tp + 1 - 2 * core}
    across = {"tp": lax.rem(tp + 2, 4)}
    diagonal = {"tp": 3 - tp}
    mirror = {"rep": 1 - rep}
    same, far, partner = lax.rem(fs + 2, 4), 3 - fs, fs + 1 - 2 * member
    sources = (same, far, partner)
    outer = (fs == 0) | (fs == 3)
    inner = jnp.logical_not(outer)

    sent = []

    def remote(src, dst, send, recv, device):
        return pltpu.make_async_remote_copy(
            src_ref=src,
            dst_ref=dst,
            send_sem=send,
            recv_sem=recv,
            device_id=device,
            device_id_type=pl.DeviceIdType.MESH,
        )

    def start(*parts):
        copy = remote(*parts)
        sent.append(copy)
        copy.start()

    def aligned(at, size):
        return pl.ds(pl.multiple_of(at, size), size)

    def local_copy(src, dst, idx):
        copy = pltpu.make_async_copy(src, dst, local_sem.at[idx])
        copy.start()
        return copy

    mine = aligned(member * half_hidden, half_hidden)
    theirs = aligned((1 - member) * half_hidden, half_hidden)
    rep_rows = aligned(rep * half_rows, half_rows)
    rep_columns = aligned(rep * half_columns, half_columns)
    load_tokens = local_copy(residual, tokens.at[0, tp], 0)
    load_pool = local_copy(pool_own, stage_pool, 1)
    loads = [
        local_copy(gate_own.at[:, mine], stage_own.at[0], 2),
        local_copy(up_own.at[:, mine], stage_own.at[1], 3),
        local_copy(gate_own.at[rep_rows, theirs], stage_other.at[0], 4),
        local_copy(up_own.at[rep_rows, theirs], stage_other.at[1], 5),
    ]
    load_down = [
        local_copy(down_own.at[mine], stage_down, 6),
        local_copy(down_own.at[theirs, rep_columns], stage_down_other, 7),
    ]

    barrier = pltpu.get_barrier_semaphore()
    peers = (mirror, sibling, across, diagonal) + tuple({"fs": f} for f in sources)
    for device in peers:
        pl.semaphore_signal(
            barrier, inc=1, device_id=device, device_id_type=pl.DeviceIdType.MESH
        )
    small_all[tp, 0] = mixer_gain[...]
    small_all[tp, 1] = pool_scale[...]
    small_all[tp, 2] = channel_gain[...]
    scales_all[fs, 0] = gate_scale[...]
    scales_all[fs, 1] = up_scale[...]
    load_pool.wait()
    pool_near[...] = stage_pool[...].astype(BF16)
    load_tokens.wait()
    pl.semaphore_wait(barrier, len(peers))

    def token_part(slot, t, part):
        span = length // TOKEN_PARTS
        return tokens.at[slot, t, pl.ds(part * span, span)]

    def pool_part(shard, half):
        span = groups // 2
        return pool_full.at[
            pl.ds(half * span, span),
            aligned(shard * pool_rows, pool_rows),
            aligned(tp * local, local),
        ]

    def pool_copy_to(q):
        return remote(
            pool_near.at[pl.ds(rep * (groups // 2), groups // 2)],
            pool_part(fs, rep),
            pz_send.at[q],
            pz_recv.at[q],
            {"fs": sources[q]},
        )

    for q in (2, 1, 0):
        pool_copy_to(q).start()
    for part in range(TOKEN_PARTS):
        piece = token_part(0, tp, part)
        start(piece, piece, ry_send.at[0, part], ry_recv.at[0, part], across)
        start(piece, piece, rs_send.at[0, part], rs_recv.at[0, part], sibling)
    for at, values in enumerate((mixer_gain, pool_scale, channel_gain)):
        for q, device in enumerate((sibling, across, diagonal)):
            start(values, small_all.at[tp, at], small_send.at[at, q], small_recv.at[at, q], device)
    for at, values in enumerate((gate_scale, up_scale)):
        for q, f in enumerate(sources):
            start(
                values, scales_all.at[fs, at], scale_send.at[at, q], scale_recv.at[at, q], {"fs": f}
            )
    pool_copy = local_copy(
        pool_near,
        pool_full.at[:, aligned(fs * pool_rows, pool_rows), aligned(tp * local, local)],
        8,
    )

    late, late_kind = jnp.where(outer, far, same), jnp.where(outer, 1, 0)

    def chunk_target(j, shard, half):
        return weights.at[j, shard, aligned(half * half_rows, half_rows)]

    def chunk_copy(j, q):
        target = chunk_target(j, fs, rep)
        source = target if q == 0 else other.at[j]
        return remote(source, target, gz_send.at[j, q], gz_recv.at[j, q], {"fs": sources[q]})

    def down_part(shard, half, sub):
        span = half_hidden // PIECES
        return down_full.at[shard, half, pl.ds(sub * span, span)]

    def down_copy(q, sub):
        span = half_hidden // PIECES
        target = down_part(fs, rep, sub)
        source = target if q == 0 else down_other.at[pl.ds(sub * span, span)]
        return remote(source, target, dz_send.at[q, sub], dz_recv.at[q, sub], {"fs": sources[q]})

    def token_copy(part):
        return remote(
            token_part(0, tp, part),
            token_part(1, tp, part),
            rz_send.at[part],
            rz_recv.at[part],
            {"fs": partner},
        )

    before_tokens = 2
    for load in loads:
        load.wait()

    @pl.loop(0, chunks)
    def _(j):
        columns = aligned(j * 128, 128)
        for at in range(2):
            lanes = slice(at * 128, (at + 1) * 128)
            weights[j, fs, :, lanes] = stage_own[at, :, columns].astype(BF16)
            other[j, :, lanes] = stage_other[at, :, columns].astype(BF16)
        chunk_copy(j, 2).start()
        pl.when(inner)(chunk_copy(j, 1).start)

        @pl.when(j == before_tokens - 1)
        def _():
            for part in range(TOKEN_PARTS):
                token_copy(part).start()

    for load in load_down:
        load.wait()
    for half in range(2):
        down_full[fs, half] = stage_down[
            :, half * half_columns : (half + 1) * half_columns
        ].astype(BF16)
    down_other[...] = stage_down_other[...].astype(BF16)
    for sub in range(PIECES):
        down_copy(2, sub).start()

    @pl.when(inner)
    def _():
        for sub in range(PIECES):
            down_copy(1, sub).start()

        @pl.loop(0, chunks)
        def _(j):
            chunk_copy(j, 0).start()

        for sub in range(PIECES):
            down_copy(0, sub).start()

    def landed(ref, send, recv):
        remote(ref, ref, send, recv, mirror).wait_recv()

    def chunk_onward(j, q, shard):
        piece = chunk_target(j, shard, rep)
        return remote(piece, piece, gx_send.at[j, q], gx_recv.at[j, q], mirror)

    def forward_chunk(j, q, shard):
        piece = chunk_target(j, shard, rep)
        landed(piece, gz_send.at[j, q], gz_recv.at[j, q])
        chunk_onward(j, q, shard).start()

    def down_onward(q, shard, sub):
        piece = down_part(shard, rep, sub)
        return remote(piece, piece, dx_send.at[q, sub], dx_recv.at[q, sub], mirror)

    def forward_down(q, shard, subs=range(PIECES)):
        for sub in subs:
            landed(down_part(shard, rep, sub), dz_send.at[q, sub], dz_recv.at[q, sub])
            down_onward(q, shard, sub).start()

    for q, f in ((2, partner), (1, far), (0, same)):
        piece = pool_part(f, rep)
        landed(piece, pz_send.at[q], pz_recv.at[q])
        start(piece, piece, px_send.at[q], px_recv.at[q], mirror)
    for q, f in enumerate(sources):
        landed(pool_part(f, 1 - rep), px_send.at[q], px_recv.at[q])
    pool_copy.wait()

    def pool_slab(t):
        return pool_full.at[:, :, aligned(t * local, local)]

    slab = pool_slab(tp)
    start(slab, slab, pt_send.at[1], pt_recv.at[1], across)
    start(slab, slab, pt_send.at[0], pt_recv.at[0], sibling)

    t_sibling, t_across, t_diagonal = sibling["tp"], across["tp"], diagonal["tp"]

    def own_onward(part):
        piece = token_part(0, t_across, part)
        landed(piece, ry_send.at[0, part], ry_recv.at[0, part])
        start(piece, piece, rs_send.at[1, part], rs_recv.at[1, part], sibling)

    def partner_onward(part):
        piece = token_part(1, tp, part)
        landed(piece, rz_send.at[part], rz_recv.at[part])
        start(piece, piece, ry_send.at[1, part], ry_recv.at[1, part], across)
        start(piece, piece, rs_send.at[2, part], rs_recv.at[2, part], sibling)

    for j in range(before_tokens):
        forward_chunk(j, 2, partner)
        pl.when(inner)(functools.partial(forward_chunk, j, 1, far))
    own_onward(0)

    @pl.when(inner)
    def _():
        for j in range(before_tokens, chunks - 2):
            forward_chunk(j, 1, far)

    own_onward(1)
    partner_onward(0)

    @pl.when(inner)
    def _():
        for j in range(chunks - 2, chunks):
            forward_chunk(j, 1, far)

    partner_onward(1)
    pl.when(inner)(functools.partial(forward_down, 1, far))
    slab = pool_slab(t_across)
    landed(slab, pt_send.at[1], pt_recv.at[1])
    start(slab, slab, pt_send.at[2], pt_recv.at[2], sibling)
    pl.when(outer)(functools.partial(forward_chunk, 0, 0, same))
    for part in range(TOKEN_PARTS):
        landed(token_part(0, t_sibling, part), rs_send.at[0, part], rs_recv.at[0, part])
        landed(token_part(0, t_diagonal, part), rs_send.at[1, part], rs_recv.at[1, part])
    for at in range(3):
        for q, t in enumerate((t_sibling, t_across, t_diagonal)):
            landed(small_all.at[t, at], small_send.at[at, q], small_recv.at[at, q])
    landed(pool_slab(t_sibling), pt_send.at[0], pt_recv.at[0])
    landed(pool_slab(t_diagonal), pt_send.at[2], pt_recv.at[2])

    positions = lax.broadcasted_iota(jnp.int32, (BAND, 1), 0).astype(F32) + 1.0
    distance = (
        lax.broadcasted_iota(jnp.int32, (BAND, 2 * BAND), 0)
        + BAND
        - lax.broadcasted_iota(jnp.int32, (BAND, 2 * BAND), 1)
    )

    def mix(slot):
        span = slice(slot * length, (slot + 1) * length)
        square = jnp.zeros((length, local), F32)
        for t in range(4):
            for g in range(groups):
                values = tokens[slot, t, :, g * local : (g + 1) * local].astype(F32)
                square = square + values * values
        factor = lax.rsqrt(jnp.sum(square, axis=1, keepdims=True) / width + EPSILON)
        square = jnp.zeros((length, local), F32)
        for g in range(groups):
            part = slice(g * local, (g + 1) * local)
            for t in range(4):
                values = tokens[slot, t, :, part].astype(F32)
                normed[:, t * local : (t + 1) * local] = (
                    values * factor * small_all[t, 0, g : g + 1]
                ).astype(BF16)
            band = jnp.where((distance >= 0) & (distance < WINDOWS[g]), 1.0, 0.0).astype(BF16)
            for b in range(length // BAND):
                here = slice(b * BAND, (b + 1) * BAND)
                if b == 0:
                    totals = jnp.dot(band[:, BAND:], normed[here], preferred_element_type=F32)
                    totals = totals / jnp.minimum(positions, float(WINDOWS[g]))
                else:
                    totals = jnp.dot(
                        band,
                        normed[(b - 1) * BAND : (b + 1) * BAND],
                        preferred_element_type=F32,
                    ) * (1.0 / WINDOWS[g])
                pooled[here] = (totals - normed[here].astype(F32)).astype(BF16)
            mixed = jnp.dot(pooled[...], pool_full[g], preferred_element_type=F32)
            for t in range(4):
                made = (
                    mixed[:, t * local : (t + 1) * local] * small_all[t, 1, g : g + 1]
                    + tokens[slot, t, :, part].astype(F32)
                ).astype(BF16)
                inputs[span, g * channels + t * local : g * channels + (t + 1) * local] = made
                values = made.astype(F32)
                square = square + values * values
        factor = lax.rsqrt(jnp.sum(square, axis=1, keepdims=True) / width + EPSILON)
        if slot == 0:
            for g in range(groups):
                middle[:, g * local : (g + 1) * local] = inputs[
                    span, aligned(g * channels + tp * local, local)
                ]
        for g in range(groups):
            for t in range(4):
                columns = slice(g * channels + t * local, g * channels + (t + 1) * local)
                inputs[span, columns] = (
                    inputs[span, columns].astype(F32) * factor * small_all[t, 2, g : g + 1]
                ).astype(BF16)

    mix(0)

    @pl.when(outer)
    def _():
        for j in range(1, chunks):
            forward_chunk(j, 0, same)

        @pl.loop(0, chunks)
        def _(j):
            chunk_copy(j, 0).start()
            chunk_copy(j, 1).start()

        for sub in range(PIECES):
            down_copy(0, sub).start()
            down_copy(1, sub).start()

    @pl.when(inner)
    def _():
        for j in range(before_tokens, chunks):
            forward_chunk(j, 2, partner)
        forward_down(2, partner)

    for part in range(TOKEN_PARTS):
        piece = token_part(1, t_across, part)
        landed(piece, ry_send.at[1, part], ry_recv.at[1, part])
        start(piece, piece, rs_send.at[3, part], rs_recv.at[3, part], sibling)
    for part in range(TOKEN_PARTS):
        landed(token_part(1, t_sibling, part), rs_send.at[2, part], rs_recv.at[2, part])
        landed(token_part(1, t_diagonal, part), rs_send.at[3, part], rs_recv.at[3, part])
    mix(1)
    for at in range(2):
        for q, f in enumerate(sources):
            landed(scales_all.at[f, at], scale_send.at[at, q], scale_recv.at[at, q])

    thirds = scales_all.shape[3] // 128

    def expand(j):
        for q, f in enumerate(sources):
            landed(chunk_target(j, f, 1 - rep), gx_send.at[j, q], gx_recv.at[j, q])
        here = aligned(member * half_hidden + j * 128, 128)
        unit = member * chunks + j
        scale_at = aligned(lax.rem(unit, thirds) * 128, 128)
        taps = [
            table[:, here] * scales_all[unit // thirds, at, :, scale_at]
            for at, table in enumerate((gate_taps, up_taps))
        ]
        block = weights[j].reshape(width, 256)
        for slot in range(2):
            span = slice(slot * length, (slot + 1) * length)
            made = jnp.dot(inputs[span], block, preferred_element_type=F32)
            conv_gate = causal_taps(made[:, :128], taps[0])
            conv_up = causal_taps(made[:, 128:], taps[1])
            silu = conv_gate / (1.0 + jnp.exp(-conv_gate))
            hidden[span, aligned(j * 128, 128)] = (silu * conv_up).astype(BF16)

    @pl.loop(0, chunks + 2)
    def _(j):
        @pl.when(outer & (j < chunks - before_tokens))
        def _():
            forward_chunk(j + before_tokens, 2, partner)

        @pl.when(j < chunks)
        def _():
            forward_chunk(j, late_kind, late)

        @pl.when(outer & (j == chunks))
        def _():
            forward_down(2, partner)

        @pl.when(j > 1)
        def _():
            expand(j - 2)

    def core_copy(shard, half, slot):
        return remote(
            give.at[shard, half, slot],
            got.at[shard, half, slot],
            core_send.at[shard, half, slot],
            core_recv.at[shard, half, slot],
            sibling,
        )

    def product(shard, half):
        for slot in (1, 0):
            span = slice(slot * length, (slot + 1) * length)
            made = jnp.dot(hidden[span], down_full[shard, half], preferred_element_type=F32)
            low, high = made[:, :local], made[:, local:]
            keep[shard, half, slot] = jnp.where(core == 0, low, high)
            give[shard, half, slot] = jnp.where(core == 0, high, low).astype(BF16)
            core_copy(shard, half, slot).start()

    def y_copy(shard, slot):
        return remote(
            y_out.at[shard, slot],
            y_in.at[shard, slot],
            y_send.at[shard, slot],
            y_recv.at[shard, slot],
            across,
        )

    def arrived_x(q, shard):
        for sub in range(PIECES):
            landed(down_part(shard, 1 - rep, sub), dx_send.at[q, sub], dx_recv.at[q, sub])

    def join_cores(shard, half):
        for slot in (1, 0):
            core_copy(shard, half, slot).wait_recv()
            total = keep[shard, half, slot] + got[shard, half, slot].astype(F32)

            @pl.when(half == side)
            def _():
                keep[shard, half, slot] = total

            @pl.when(half != side)
            def _():
                y_out[shard, slot] = total.astype(BF16)
                y_copy(shard, slot).start()

    def join_sides(shard):
        y_copy(shard, 1).wait_recv()
        total = keep[shard, side, 1] + y_in[shard, 1].astype(F32)
        z_out[shard] = total.astype(BF16)
        start(
            z_out.at[shard],
            z_in.at[shard],
            z_send.at[shard],
            z_recv.at[shard],
            {"fs": partner},
        )

    def conclude(shard):
        y_copy(shard, 0).wait_recv()
        total = keep[shard, side, 0] + y_in[shard, 0].astype(F32)
        landed(z_in.at[shard], z_send.at[shard], z_recv.at[shard])
        columns = aligned(shard * local, local)
        total = total + z_in[shard].astype(F32)
        out[:, columns] = (
            total * down_scale[pl.ds(shard, 1), :] + middle[:, columns].astype(F32)
        ).astype(BF16)

    early, early_kind = jnp.where(outer, partner, far), jnp.where(outer, 2, 1)
    later, later_kind = jnp.where(outer, far, partner), jnp.where(outer, 1, 2)

    def later_products():
        product(later, rep)
        arrived_x(later_kind, later)
        product(later, 1 - rep)

    product(fs, rep)
    product(fs, 1 - rep)
    join_cores(fs, rep)
    forward_down(late_kind, late, (0,))
    product(early, rep)
    join_cores(fs, 1 - rep)
    forward_down(late_kind, late, (1,))
    arrived_x(early_kind, early)
    product(early, 1 - rep)
    join_cores(early, rep)
    forward_down(late_kind, late, (2,))
    pl.when(inner)(later_products)
    join_cores(early, 1 - rep)
    forward_down(late_kind, late, (3,))
    join_sides(fs)
    pl.when(outer)(functools.partial(forward_down, 0, same, (0, 1)))
    pl.when(outer)(later_products)
    join_cores(later, rep)
    join_cores(later, 1 - rep)
    pl.when(outer)(functools.partial(forward_down, 0, same, (2, 3)))
    product(same, rep)
    join_sides(early)
    arrived_x(0, same)
    product(same, 1 - rep)
    join_cores(same, rep)
    join_cores(same, 1 - rep)
    join_sides(later)
    join_sides(same)
    conclude(partner)
    conclude(jnp.where(outer, same, fs))
    conclude(jnp.where(outer, fs, same))
    conclude(far)

    for copy in sent:
        copy.wait_send()
    for q in range(3):
        pool_copy_to(q).wait_send()
    for part in range(TOKEN_PARTS):
        token_copy(part).wait_send()
    for shard in range(4):
        for slot in range(2):
            y_copy(shard, slot).wait_send()
            for half in range(2):
                core_copy(shard, half, slot).wait_send()
    for q, f in enumerate(sources):
        for sub in range(PIECES):
            down_copy(q, sub).wait_send()
            down_onward(q, f, sub).wait_send()

    @pl.loop(0, chunks)
    def _(j):
        for q, f in enumerate(sources):
            chunk_copy(j, q).wait_send()
            chunk_onward(j, q, f).wait_send()


def pair_shards(
    residual,
    mixer_gain,
    pool_weight,
    pool_scale,
    channel_gain,
    gate_weight,
    up_weight,
    gate_scale,
    up_scale,
    gate_taps,
    up_taps,
    down_weight,
    down_scale,
):
    _, length, groups, local = residual.shape
    channels = local * 4
    width = groups * channels
    rows, hidden_width = gate_weight.shape
    half = hidden_width // 2
    chunks = half // 128
    half_columns = down_weight.shape[1] // 2
    vmem = pl.BlockSpec(memory_space=pltpu.VMEM)
    anywhere = pl.BlockSpec(memory_space=pl.ANY)
    dma = pltpu.SemaphoreType.DMA
    pairs = [
        (3, 3),
        (2, 3),
        (3,),
        (3,),
        (3,),
        (TOKEN_PARTS,),
        (2, TOKEN_PARTS),
        (4, TOKEN_PARTS),
        (chunks, 3),
        (chunks, 3),
        (3, PIECES),
        (3, PIECES),
        (4, 2, 2),
        (4, 2),
        (4,),
    ]
    out = pl.pallas_call(
        pair_kernel,
        out_shape=jax.ShapeDtypeStruct((length, groups * local), BF16),
        in_specs=[anywhere] + [vmem] * 8 + [anywhere] * 4,
        out_specs=vmem,
        scratch_shapes=[
            pltpu.VMEM((2, rows, half), F32),
            pltpu.VMEM((2, rows // 2, half), F32),
            pltpu.VMEM((half, 2 * half_columns), F32),
            pltpu.VMEM((half, half_columns), F32),
            pltpu.VMEM(pool_weight.shape, F32),
            pltpu.VMEM((2, 4, length, groups * local), BF16),
            pltpu.VMEM((4, 3, groups, local), F32),
            pltpu.VMEM((4, 2) + gate_scale.shape, F32),
            pltpu.VMEM(pool_weight.shape, BF16),
            pltpu.VMEM((groups, channels, channels), BF16),
            pltpu.VMEM((chunks, 4, rows, 256), BF16),
            pltpu.VMEM((chunks, rows // 2, 256), BF16),
            pltpu.VMEM((4, 2, half, half_columns), BF16),
            pltpu.VMEM((half, half_columns), BF16),
            pltpu.VMEM((length, channels), BF16),
            pltpu.VMEM((length, channels), BF16),
            pltpu.VMEM((2 * length, width), BF16),
            pltpu.VMEM((length, groups * local), BF16),
            pltpu.VMEM((2 * length, half), BF16),
            pltpu.VMEM((4, 2, 2, length, local), F32),
            pltpu.VMEM((4, 2, 2, length, local), BF16),
            pltpu.VMEM((4, 2, 2, length, local), BF16),
            pltpu.VMEM((4, 2, length, local), BF16),
            pltpu.VMEM((4, 2, length, local), BF16),
            pltpu.VMEM((4, length, local), BF16),
            pltpu.VMEM((4, length, local), BF16),
        ]
        + [dma(shape) for shape in pairs for _ in range(2)]
        + [dma((9,))],
        compiler_params=pltpu.CompilerParams(
            collective_id=0, has_side_effects=True, vmem_limit_bytes=VMEM_BYTES
        ),
    )(
        residual.reshape(length, groups * local),
        mixer_gain,
        pool_scale,
        channel_gain,
        down_scale,
        gate_scale,
        up_scale,
        gate_taps,
        up_taps,
        pool_weight,
        gate_weight,
        up_weight,
        down_weight,
    )
    return out.reshape(1, length, groups, local)


def paired(sizes, residual, gate_weight, down_weight):
    _, length, groups, local = residual
    return (
        sizes == (2, 4, 4)
        and residual[0] == 1
        and local == 128
        and length % BAND == 0
        and groups == len(WINDOWS)
        and down_weight[1] == 4 * local
        and gate_weight[0] * 4 == groups * local * 4
        and gate_weight[1] % 512 == 0
    )


def shards(
    sizes,
    residual,
    mixer_gain,
    pool_weight,
    pool_scale,
    channel_gain,
    gate_weight,
    up_weight,
    gate_scale,
    up_scale,
    gate_taps,
    up_taps,
    down_weight,
    down_scale,
):
    if paired(sizes, residual.shape, gate_weight.shape, down_weight.shape):
        return pair_shards(
            residual,
            mixer_gain,
            pool_weight,
            pool_scale,
            channel_gain,
            gate_weight,
            up_weight,
            gate_scale,
            up_scale,
            gate_taps,
            up_taps,
            down_weight,
            down_scale,
        )
    n_rep, n_fs, n_tp = sizes
    _, length, groups, local = residual.shape
    channels = local * n_tp
    width = groups * channels
    own_width = groups * local
    hidden_width = gate_weight.shape[1]
    vmem = pl.BlockSpec(memory_space=pltpu.VMEM)
    anywhere = pl.BlockSpec(memory_space=pl.ANY)
    dma = pltpu.SemaphoreType.DMA
    hops = max(n_fs - 1, 1)
    reps = max(n_rep - 1, 1)
    peers = max(n_tp - 1, 1)
    out = pl.pallas_call(
        functools.partial(block_kernel, sizes),
        out_shape=jax.ShapeDtypeStruct((length, own_width), BF16),
        in_specs=[vmem] * 8 + [anywhere] * 3,
        out_specs=vmem,
        scratch_shapes=[
            pltpu.VMEM((groups, channels, local), BF16),
            pltpu.VMEM((n_fs,) + gate_weight.shape, BF16),
            pltpu.VMEM((n_fs,) + up_weight.shape, BF16),
            pltpu.VMEM((n_fs,) + down_weight.shape, BF16),
            pltpu.VMEM((n_tp, length, own_width), BF16),
            pltpu.VMEM((n_tp, length, own_width), BF16),
            pltpu.VMEM((n_tp, 2, own_width), F32),
            pltpu.VMEM((n_fs, 2, gate_scale.shape[1]), F32),
            pltpu.VMEM((2, hidden_width), F32),
            pltpu.VMEM((length, channels), BF16),
            pltpu.VMEM((length, own_width), BF16),
            pltpu.VMEM((length, width), BF16),
            pltpu.VMEM((length, hidden_width), BF16),
            pltpu.VMEM((length, hidden_width), BF16),
            pltpu.VMEM((n_tp, groups, length, local), BF16),
            pltpu.VMEM((n_tp, groups, length, local), BF16),
            dma((3, SUBS, 2 * hops)),
            dma((3, SUBS, 2 * hops)),
            dma((3, SUBS, 2 * hops, reps)),
            dma((3, SUBS, 2 * hops, reps)),
            dma((hops,)),
            dma((hops,)),
            dma((hops, reps)),
            dma((hops, reps)),
            dma((hops,)),
            dma((hops,)),
            dma((3, peers)),
            dma((3, peers)),
            dma((n_fs, peers)),
            dma((n_fs, peers)),
            dma((7,)),
        ],
        compiler_params=pltpu.CompilerParams(
            collective_id=0, has_side_effects=True, vmem_limit_bytes=60 * 1024 * 1024
        ),
    )(
        residual.reshape(length, own_width),
        jnp.stack([mixer_gain.reshape(-1), channel_gain.reshape(-1)]),
        pool_scale.reshape(1, -1),
        down_scale.reshape(1, -1),
        jnp.concatenate([gate_scale, up_scale], axis=0),
        gate_taps,
        up_taps,
        pool_weight.astype(BF16),
        gate_weight.astype(BF16),
        up_weight.astype(BF16),
        down_weight.astype(BF16),
    )
    return out.reshape(1, length, groups, local)


def solution(mesh):
    placed = (
        P(("rep", "fs"), None, None, "tp"),
        P(None, "tp"),
        P(None, "fs", "tp"),
        P(None, "tp"),
        P(None, "tp"),
        P("fs", "tp"),
        P("fs", "tp"),
        P("fs", "tp"),
        P("fs", "tp"),
        P(None, "tp"),
        P(None, "tp"),
        P("tp", "fs"),
        P(None, "tp"),
    )
    sizes = tuple(mesh.shape[name] for name in ("rep", "fs", "tp"))
    return jax.shard_map(
        functools.partial(shards, sizes),
        mesh=mesh,
        in_specs=placed,
        out_specs=P(("rep", "fs"), None, None, "tp"),
        check_vma=False,
    )
```

```python
import functools

import jax
import jax.numpy as jnp
from jax import lax
from jax.experimental import pallas as pl
from jax.experimental.pallas import tpu as pltpu
from jax.sharding import PartitionSpec as P

WINDOWS = (2, 4, 8, 16)
EPSILON = 1e-05
SUBS = 2
COLUMNS = 256
VMEM_BYTES = 62 * 1024 * 1024
F32 = jnp.float32
BF16 = jnp.bfloat16


def delayed(values, steps):
    rows = lax.broadcasted_iota(jnp.int32, values.shape, 0)
    return jnp.where(rows >= steps, pltpu.roll(values, steps, 0), 0.0)


def causal_taps(values, taps):
    return taps[2:3] * values + taps[1:2] * delayed(values, 1) + taps[0:1] * delayed(values, 2)


def block_kernel(
    sizes,
    residual,
    gains,
    pool_scale,
    down_scale,
    scale_pair,
    gate_taps,
    up_taps,
    pool_own,
    gate_own,
    up_own,
    down_own,
    out,
    pool_full,
    gate_full,
    up_full,
    down_full,
    gathered,
    middle_all,
    gains_all,
    scales_all,
    scale_row,
    pooled,
    middle,
    inputs,
    gate_pre,
    hidden,
    partials,
    arrived,
    ring_send,
    ring_recv,
    rep_send,
    rep_recv,
    pool_send,
    pool_recv,
    pool_rep_send,
    pool_rep_recv,
    scale_send,
    scale_recv,
    tp_send,
    tp_recv,
    part_send,
    part_recv,
    local_sem,
):
    n_rep, n_fs, n_tp = sizes
    rep, fs, tp = (lax.axis_index(name) for name in ("rep", "fs", "tp"))
    length = residual.shape[0]
    groups = pool_full.shape[0]
    channels = pool_full.shape[1]
    local = residual.shape[1] // groups
    width = groups * channels

    def other(axis, offset):
        me, count = {"rep": (rep, n_rep), "fs": (fs, n_fs), "tp": (tp, n_tp)}[axis]
        return lax.rem(me + offset, count)

    def remote(src, dst, send, recv, axis, offset):
        return pltpu.make_async_remote_copy(
            src_ref=src,
            dst_ref=dst,
            send_sem=send,
            recv_sem=recv,
            device_id={axis: other(axis, offset)},
            device_id_type=pl.DeviceIdType.MESH,
        )

    barrier = pltpu.get_barrier_semaphore()
    for axis, count in (("rep", n_rep), ("fs", n_fs), ("tp", n_tp)):
        for offset in range(1, count):
            pl.semaphore_signal(
                barrier,
                inc=1,
                device_id={axis: other(axis, offset)},
                device_id_type=pl.DeviceIdType.MESH,
            )
    pl.semaphore_wait(barrier, n_rep + n_fs + n_tp - 3)

    sent = []

    def start(copy, valid=None):
        sent.append((copy, valid))
        if valid is None:
            copy.start()
        else:
            pl.when(valid)(copy.start)

    weights = ((gate_own, gate_full), (up_own, up_full), (down_own, down_full))

    def piece(w, shard, half, sub, own=False):
        rows = weights[w][0].shape[0] // (n_rep * SUBS)
        part = pl.ds(pl.multiple_of((half * SUBS + sub) * rows, rows), rows)
        return weights[w][0].at[part] if own else weights[w][1].at[shard, part]

    def shard_sent(step, way):
        shard = fs + step if way else fs - step
        return jnp.clip(shard, 0, n_fs - 1), (shard <= n_fs - 1 if way else shard >= 0)

    def line(w, sub, step):
        for way in range(2):
            shard, valid = shard_sent(step, way)
            start(
                remote(
                    piece(w, shard, rep, sub, own=step == 0),
                    piece(w, shard, rep, sub),
                    ring_send.at[w, sub, 2 * step + way],
                    ring_recv.at[w, sub, 2 * step + way],
                    "fs",
                    n_fs - 1 if way else 1,
                ),
                valid & (fs > 0 if way else fs < n_fs - 1),
            )

    def serve(w, sub, step):
        for way in range(2):
            shard, valid = shard_sent(step + 1, way)
            mine = piece(w, shard, rep, sub)
            sems = (w, sub, 2 * step + way)
            pl.when(valid)(
                remote(
                    mine, mine, ring_send.at[sems], ring_recv.at[sems], "fs", 1
                ).wait_recv
            )
            if step < n_fs - 2:
                onward = (w, sub, 2 * step + 2 + way)
                start(
                    remote(
                        mine,
                        mine,
                        ring_send.at[onward],
                        ring_recv.at[onward],
                        "fs",
                        n_fs - 1 if way else 1,
                    ),
                    valid & (fs > 0 if way else fs < n_fs - 1),
                )
            for d in range(1, n_rep):
                start(
                    remote(
                        mine,
                        mine,
                        rep_send.at[sems + (d - 1,)],
                        rep_recv.at[sems + (d - 1,)],
                        "rep",
                        d,
                    ),
                    valid,
                )

    def settle(w, step, ways=(0, 1)):
        for way in ways:
            shard, valid = shard_sent(step + 1, way)

            @pl.when(valid)
            def _():
                for sub in range(SUBS):
                    for d in range(1, n_rep):
                        got = piece(w, shard, other("rep", n_rep - d), sub)
                        sems = (w, sub, 2 * step + way, d - 1)
                        remote(
                            got, got, rep_send.at[sems], rep_recv.at[sems], "rep", d
                        ).wait_recv()

    def local_copy(src, dst, idx):
        copy = pltpu.make_async_copy(src, dst, local_sem.at[idx])
        copy.start()
        return copy

    own_copies = [
        local_copy(residual, gathered.at[tp], 0),
        local_copy(gains, gains_all.at[tp], 1),
        local_copy(scale_pair, scales_all.at[fs], 2),
        local_copy(gate_own, gate_full.at[fs], 3),
        local_copy(up_own, up_full.at[fs], 4),
        local_copy(down_own, down_full.at[fs], 5),
    ]

    pool_rows = pool_own.shape[1]
    rep_groups = groups // n_rep

    def pool_part(shard, half):
        return pool_full.at[
            pl.ds(half * rep_groups, rep_groups),
            pl.ds(pl.multiple_of(shard * pool_rows, pool_rows), pool_rows),
        ]

    pool_copy = local_copy(
        pool_own, pool_full.at[:, pl.ds(pl.multiple_of(fs * pool_rows, pool_rows), pool_rows)], 6
    )

    for d in range(1, n_fs):
        start(
            remote(
                pool_own.at[pl.ds(rep * rep_groups, rep_groups)],
                pool_part(fs, rep),
                pool_send.at[d - 1],
                pool_recv.at[d - 1],
                "fs",
                d,
            )
        )
    for w in (0, 1):
        for sub in range(SUBS):
            if n_fs > 1:
                line(w, sub, 0)
    for d in range(1, n_tp):
        start(remote(gains, gains_all.at[tp], tp_send.at[0, d - 1], tp_recv.at[0, d - 1], "tp", d))
    for d in range(1, n_tp):
        start(
            remote(residual, gathered.at[tp], tp_send.at[1, d - 1], tp_recv.at[1, d - 1], "tp", d)
        )
    for d in range(1, n_fs):
        start(
            remote(
                scale_pair, scales_all.at[fs], scale_send.at[d - 1], scale_recv.at[d - 1], "fs", d
            )
        )

    for d in range(1, n_fs):
        shard = other("fs", n_fs - d)
        mine = pool_part(shard, rep)
        remote(mine, mine, pool_send.at[d - 1], pool_recv.at[d - 1], "fs", d).wait_recv()
        for e in range(1, n_rep):
            start(
                remote(
                    mine,
                    mine,
                    pool_rep_send.at[d - 1, e - 1],
                    pool_rep_recv.at[d - 1, e - 1],
                    "rep",
                    e,
                )
            )
    for d in range(1, n_fs):
        shard = other("fs", n_fs - d)
        for e in range(1, n_rep):
            got = pool_part(shard, other("rep", n_rep - e))
            remote(
                got,
                got,
                pool_rep_send.at[d - 1, e - 1],
                pool_rep_recv.at[d - 1, e - 1],
                "rep",
                e,
            ).wait_recv()
    pool_copy.wait()
    for copy in own_copies:
        copy.wait()

    def tp_arrivals(idx, buffer):
        for d in range(1, n_tp):
            got = buffer.at[other("tp", n_tp - d)]
            remote(got, got, tp_send.at[idx, d - 1], tp_recv.at[idx, d - 1], "tp", d).wait_recv()

    for sub in range(SUBS):
        serve(0, sub, 0)
    tp_arrivals(0, gains_all)
    tp_arrivals(1, gathered)
    for sub in range(SUBS):
        serve(1, sub, 0)

    def mean_square_root(buffer):
        total = jnp.zeros((length, 1), F32)
        for t in range(n_tp):
            values = buffer[t].astype(F32)
            total = total + jnp.sum(values * values, axis=1, keepdims=True)
        return lax.rsqrt(total / width + EPSILON)

    factor = mean_square_root(gathered)
    positions = lax.broadcasted_iota(jnp.int32, (length, 1), 0).astype(F32) + 1.0
    for g in range(groups):
        part = slice(g * local, (g + 1) * local)
        share = 1.0 / jnp.minimum(positions, float(WINDOWS[g]))
        for t in range(n_tp):
            values = gathered[t, :, part].astype(F32)
            normed = (values * factor * gains_all[t, 0:1, part]).astype(BF16).astype(F32)
            totals = normed
            reach = 1
            while reach < WINDOWS[g]:
                totals = totals + delayed(totals, reach)
                reach = reach * 2
            pooled[:, t * local : (t + 1) * local] = (totals * share - normed).astype(BF16)
        mixed = jnp.dot(pooled[...], pool_full[g], preferred_element_type=F32)
        middle[:, part] = (
            mixed * pool_scale[:, part] + residual[:, part].astype(F32)
        ).astype(BF16)

    middle_copy = local_copy(middle, middle_all.at[tp], 0)
    for d in range(1, n_tp):
        start(
            remote(middle, middle_all.at[tp], tp_send.at[2, d - 1], tp_recv.at[2, d - 1], "tp", d)
        )
    for step in range(1, n_fs - 1):
        for w in (0, 1):
            if step == n_fs - 2 and n_fs > 2:
                break
            for sub in range(SUBS):
                serve(w, sub, step)
    for sub in range(SUBS):
        if n_fs > 1:
            line(2, sub, 0)
    for d in range(1, n_fs):
        got = scales_all.at[other("fs", n_fs - d)]
        remote(got, got, scale_send.at[d - 1], scale_recv.at[d - 1], "fs", d).wait_recv()
    shard_columns = scale_pair.shape[1]
    for f in range(n_fs):
        scale_row[:, f * shard_columns : (f + 1) * shard_columns] = scales_all[f]

    middle_copy.wait()
    tp_arrivals(2, middle_all)
    factor = mean_square_root(middle_all)
    for t in range(n_tp):
        for g in range(groups):
            part = slice(g * local, (g + 1) * local)
            start_column = g * channels + t * local
            inputs[:, start_column : start_column + local] = (
                middle_all[t, :, part].astype(F32) * factor * gains_all[t, 1:2, part]
            ).astype(BF16)

    def finish(w):
        if n_fs > 2:
            for sub in range(SUBS):
                serve(w, sub, n_fs - 2)
        for step in range(n_fs - 1):
            settle(w, step)

    def product(full, columns, row):
        block = full[:, :, columns].reshape(width, COLUMNS)
        made = jnp.dot(inputs[...], block, preferred_element_type=F32)
        return (made * scale_row[row : row + 1, columns]).astype(BF16)

    chunks = gate_full.shape[2] // COLUMNS

    finish(0)

    @pl.loop(0, chunks)
    def _(j):
        columns = pl.ds(pl.multiple_of(j * COLUMNS, COLUMNS), COLUMNS)
        gate_pre[:, columns] = product(gate_full, columns, 0)

    finish(1)
    for sub in range(SUBS):
        if n_fs > 1:
            serve(2, sub, 0)

    @pl.loop(0, chunks)
    def _(j):
        columns = pl.ds(pl.multiple_of(j * COLUMNS, COLUMNS), COLUMNS)
        up_values = product(up_full, columns, 1).astype(F32)
        conv_gate = causal_taps(gate_pre[:, columns].astype(F32), gate_taps[:, columns])
        conv_up = causal_taps(up_values, up_taps[:, columns])
        silu = conv_gate / (1.0 + jnp.exp(-conv_gate))
        hidden[:, columns] = (silu * conv_up).astype(BF16)

    shard_width = down_own.shape[1]

    def to_peers(idx, src, dst):
        for d in range(1, n_tp):
            start(
                remote(
                    src(other("tp", d)),
                    dst(tp),
                    part_send.at[idx, d - 1],
                    part_recv.at[idx, d - 1],
                    "tp",
                    d,
                )
            )

    def from_peers(idx, dst):
        for d in range(1, n_tp):
            got = dst(other("tp", n_tp - d))
            remote(
                got, got, part_send.at[idx, d - 1], part_recv.at[idx, d - 1], "tp", d
            ).wait_recv()

    def conclude(g, columns):
        total = partials[tp, g].astype(F32)
        for d in range(1, n_tp):
            total = total + arrived[other("tp", d), g].astype(F32)
        out[:, columns] = (
            total * down_scale[:, columns] + middle[:, columns].astype(F32)
        ).astype(BF16)

    if shard_width == channels and local % 128 == 0:
        def share(shard):
            made = jnp.dot(hidden[...], down_full[shard], preferred_element_type=F32)
            for t in range(n_tp):
                partials[t, shard] = made[:, t * local : (t + 1) * local].astype(BF16)
            for d in range(1, n_tp):
                peer = other("tp", d)
                remote(
                    partials.at[peer, shard],
                    arrived.at[tp, shard],
                    part_send.at[shard, d - 1],
                    part_recv.at[shard, d - 1],
                    "tp",
                    d,
                ).start()

        share(fs)
        for step in range(n_fs - 1):
            if step >= 1:
                for sub in range(SUBS):
                    serve(2, sub, step)
            for way in range(2):
                settle(2, step, (way,))
                shard, valid = shard_sent(step + 1, way)
                pl.when(valid)(functools.partial(share, shard))
        for shard in range(n_fs):
            from_peers(shard, lambda t: arrived.at[t, shard])
            conclude(shard, slice(shard * local, (shard + 1) * local))
            for d in range(1, n_tp):
                mine = partials.at[other("tp", d), shard]
                remote(
                    mine, mine, part_send.at[shard, d - 1], part_recv.at[shard, d - 1], "tp", d
                ).wait_send()
    else:
        for step in range(n_fs - 1):
            if step >= 1:
                for sub in range(SUBS):
                    serve(2, sub, step)
            settle(2, step)
        for f in range(n_fs):
            made = jnp.dot(hidden[...], down_full[f], preferred_element_type=F32).astype(BF16)
            span = min(local, shard_width)
            for at in range(0, shard_width, span):
                g, channel = divmod(f * shard_width + at, channels)
                t, low = divmod(channel, local)
                partials[t, g, :, low : low + span] = made[:, at : at + span]
        to_peers(0, lambda t: partials.at[t], lambda t: arrived.at[t])
        from_peers(0, lambda t: arrived.at[t])
        for g in range(groups):
            conclude(g, slice(g * local, (g + 1) * local))

    for copy, valid in sent:
        if valid is None:
            copy.wait_send()
        else:
            pl.when(valid)(copy.wait_send)


BAND = 256
PIECES = 4
TOKEN_PARTS = 2


def pair_kernel(
    residual,
    mixer_gain,
    pool_scale,
    channel_gain,
    down_scale,
    gate_scale,
    up_scale,
    gate_taps,
    up_taps,
    pool_own,
    gate_own,
    up_own,
    down_own,
    out,
    stage_own,
    stage_other,
    stage_down,
    stage_down_other,
    stage_pool,
    tokens,
    small_all,
    scales_all,
    pool_near,
    pool_full,
    weights,
    other,
    down_full,
    down_other,
    normed,
    pooled,
    inputs,
    middle,
    hidden,
    keep,
    give,
    got,
    y_out,
    y_in,
    z_out,
    z_in,
    small_send,
    small_recv,
    scale_send,
    scale_recv,
    pz_send,
    pz_recv,
    px_send,
    px_recv,
    pt_send,
    pt_recv,
    rz_send,
    rz_recv,
    ry_send,
    ry_recv,
    rs_send,
    rs_recv,
    gz_send,
    gz_recv,
    gx_send,
    gx_recv,
    dz_send,
    dz_recv,
    dx_send,
    dx_recv,
    core_send,
    core_recv,
    y_send,
    y_recv,
    z_send,
    z_recv,
    local_sem,
):
    rep, fs, tp = (lax.axis_index(name) for name in ("rep", "fs", "tp"))
    length = residual.shape[0]
    groups, pool_rows, local = pool_own.shape
    channels = pool_full.shape[1]
    width = groups * channels
    rows = gate_own.shape[0]
    half_rows = rows // 2
    half_hidden = gate_own.shape[1] // 2
    chunks = half_hidden // 128
    half_columns = down_own.shape[1] // 2
    member = lax.rem(fs, 2)
    side = tp // 2
    core = lax.rem(tp, 2)
    sibling = {"tp": tp + 1 - 2 * core}
    across = {"tp": lax.rem(tp + 2, 4)}
    diagonal = {"tp": 3 - tp}
    mirror = {"rep": 1 - rep}
    same, far, partner = lax.rem(fs + 2, 4), 3 - fs, fs + 1 - 2 * member
    sources = (same, far, partner)
    outer = (fs == 0) | (fs == 3)
    inner = jnp.logical_not(outer)

    sent = []

    def remote(src, dst, send, recv, device):
        return pltpu.make_async_remote_copy(
            src_ref=src,
            dst_ref=dst,
            send_sem=send,
            recv_sem=recv,
            device_id=device,
            device_id_type=pl.DeviceIdType.MESH,
        )

    def start(*parts):
        copy = remote(*parts)
        sent.append(copy)
        copy.start()

    def aligned(at, size):
        return pl.ds(pl.multiple_of(at, size), size)

    def local_copy(src, dst, idx):
        copy = pltpu.make_async_copy(src, dst, local_sem.at[idx])
        copy.start()
        return copy

    mine = aligned(member * half_hidden, half_hidden)
    theirs = aligned((1 - member) * half_hidden, half_hidden)
    rep_rows = aligned(rep * half_rows, half_rows)
    rep_columns = aligned(rep * half_columns, half_columns)
    load_tokens = local_copy(residual, tokens.at[0, tp], 0)
    load_pool = local_copy(pool_own, stage_pool, 1)
    loads = [
        local_copy(gate_own.at[:, mine], stage_own.at[0], 2),
        local_copy(up_own.at[:, mine], stage_own.at[1], 3),
        local_copy(gate_own.at[rep_rows, theirs], stage_other.at[0], 4),
        local_copy(up_own.at[rep_rows, theirs], stage_other.at[1], 5),
    ]
    load_down = [
        local_copy(down_own.at[mine], stage_down, 6),
        local_copy(down_own.at[theirs, rep_columns], stage_down_other, 7),
    ]

    barrier = pltpu.get_barrier_semaphore()
    peers = (mirror, sibling, across, diagonal) + tuple({"fs": f} for f in sources)
    for device in peers:
        pl.semaphore_signal(
            barrier, inc=1, device_id=device, device_id_type=pl.DeviceIdType.MESH
        )
    small_all[tp, 0] = mixer_gain[...]
    small_all[tp, 1] = pool_scale[...]
    small_all[tp, 2] = channel_gain[...]
    scales_all[fs, 0] = gate_scale[...]
    scales_all[fs, 1] = up_scale[...]
    load_pool.wait()
    pool_near[...] = stage_pool[...].astype(BF16)
    load_tokens.wait()
    pl.semaphore_wait(barrier, len(peers))

    def token_part(slot, t, part):
        span = length // TOKEN_PARTS
        return tokens.at[slot, t, pl.ds(part * span, span)]

    def pool_part(shard, half):
        span = groups // 2
        return pool_full.at[
            pl.ds(half * span, span),
            aligned(shard * pool_rows, pool_rows),
            aligned(tp * local, local),
        ]

    def pool_copy_to(q):
        return remote(
            pool_near.at[pl.ds(rep * (groups // 2), groups // 2)],
            pool_part(fs, rep),
            pz_send.at[q],
            pz_recv.at[q],
            {"fs": sources[q]},
        )

    for q in (2, 1, 0):
        pool_copy_to(q).start()
    for part in range(TOKEN_PARTS):
        piece = token_part(0, tp, part)
        start(piece, piece, ry_send.at[0, part], ry_recv.at[0, part], across)
        start(piece, piece, rs_send.at[0, part], rs_recv.at[0, part], sibling)
    for at, values in enumerate((mixer_gain, pool_scale, channel_gain)):
        for q, device in enumerate((sibling, across, diagonal)):
            start(values, small_all.at[tp, at], small_send.at[at, q], small_recv.at[at, q], device)
    for at, values in enumerate((gate_scale, up_scale)):
        for q, f in enumerate(sources):
            start(
                values, scales_all.at[fs, at], scale_send.at[at, q], scale_recv.at[at, q], {"fs": f}
            )
    pool_copy = local_copy(
        pool_near,
        pool_full.at[:, aligned(fs * pool_rows, pool_rows), aligned(tp * local, local)],
        8,
    )

    late, late_kind = jnp.where(outer, far, same), jnp.where(outer, 1, 0)

    def chunk_target(j, shard, half):
        return weights.at[j, shard, aligned(half * half_rows, half_rows)]

    def chunk_copy(j, q):
        target = chunk_target(j, fs, rep)
        source = target if q == 0 else other.at[j]
        return remote(source, target, gz_send.at[j, q], gz_recv.at[j, q], {"fs": sources[q]})

    def down_part(shard, half, sub):
        span = half_hidden // PIECES
        return down_full.at[shard, half, pl.ds(sub * span, span)]

    def down_copy(q, sub):
        span = half_hidden // PIECES
        target = down_part(fs, rep, sub)
        source = target if q == 0 else down_other.at[pl.ds(sub * span, span)]
        return remote(source, target, dz_send.at[q, sub], dz_recv.at[q, sub], {"fs": sources[q]})

    def token_copy(part):
        return remote(
            token_part(0, tp, part),
            token_part(1, tp, part),
            rz_send.at[part],
            rz_recv.at[part],
            {"fs": partner},
        )

    for part in range(TOKEN_PARTS):
        token_copy(part).start()
    for load in loads:
        load.wait()

    @pl.loop(0, chunks)
    def _(j):
        columns = aligned(j * 128, 128)
        for at in range(2):
            lanes = slice(at * 128, (at + 1) * 128)
            weights[j, fs, :, lanes] = stage_own[at, :, columns].astype(BF16)
            other[j, :, lanes] = stage_other[at, :, columns].astype(BF16)
        chunk_copy(j, 2).start()
        pl.when(inner)(chunk_copy(j, 1).start)

    @pl.when(inner)
    def _():
        @pl.loop(0, chunks)
        def _(j):
            chunk_copy(j, 0).start()

    for load in load_down:
        load.wait()
    for half in range(2):
        down_full[fs, half] = stage_down[
            :, half * half_columns : (half + 1) * half_columns
        ].astype(BF16)
    down_other[...] = stage_down_other[...].astype(BF16)

    @pl.when(inner)
    def _():
        for q in (2, 0, 1):
            for sub in range(PIECES):
                down_copy(q, sub).start()

    def landed(ref, send, recv):
        remote(ref, ref, send, recv, mirror).wait_recv()

    def chunk_onward(j, q, shard):
        piece = chunk_target(j, shard, rep)
        return remote(piece, piece, gx_send.at[j, q], gx_recv.at[j, q], mirror)

    def forward_chunk(j, q, shard):
        piece = chunk_target(j, shard, rep)
        landed(piece, gz_send.at[j, q], gz_recv.at[j, q])
        chunk_onward(j, q, shard).start()

    def down_onward(q, shard, sub):
        piece = down_part(shard, rep, sub)
        return remote(piece, piece, dx_send.at[q, sub], dx_recv.at[q, sub], mirror)

    def forward_down(q, shard, subs=range(PIECES)):
        for sub in subs:
            landed(down_part(shard, rep, sub), dz_send.at[q, sub], dz_recv.at[q, sub])
            down_onward(q, shard, sub).start()

    for q, f in ((2, partner), (1, far), (0, same)):
        piece = pool_part(f, rep)
        landed(piece, pz_send.at[q], pz_recv.at[q])
        start(piece, piece, px_send.at[q], px_recv.at[q], mirror)
    for q, f in enumerate(sources):
        landed(pool_part(f, 1 - rep), px_send.at[q], px_recv.at[q])
    pool_copy.wait()

    def pool_slab(t):
        return pool_full.at[:, :, aligned(t * local, local)]

    slab = pool_slab(tp)
    start(slab, slab, pt_send.at[1], pt_recv.at[1], across)
    start(slab, slab, pt_send.at[0], pt_recv.at[0], sibling)

    t_sibling, t_across, t_diagonal = sibling["tp"], across["tp"], diagonal["tp"]

    def own_onward(part):
        piece = token_part(0, t_across, part)
        landed(piece, ry_send.at[0, part], ry_recv.at[0, part])
        start(piece, piece, rs_send.at[1, part], rs_recv.at[1, part], sibling)

    def partner_onward(part):
        piece = token_part(1, tp, part)
        landed(piece, rz_send.at[part], rz_recv.at[part])
        start(piece, piece, ry_send.at[1, part], ry_recv.at[1, part], across)
        start(piece, piece, rs_send.at[2, part], rs_recv.at[2, part], sibling)

    def forward_chunks(kind, shard, low, high):
        for j in range(low, high):
            forward_chunk(j, kind, shard)

    third = chunks // 3
    own_onward(0)
    pl.when(inner)(functools.partial(forward_chunks, 1, far, 0, third))
    partner_onward(0)
    own_onward(1)
    pl.when(inner)(functools.partial(forward_chunks, 1, far, third, chunks - 1))
    partner_onward(1)
    pl.when(inner)(functools.partial(forward_chunks, 1, far, chunks - 1, chunks))
    second_kind, second = jnp.where(outer, 0, 2), jnp.where(outer, same, partner)
    forward_chunks(second_kind, second, 0, 2)
    slab = pool_slab(t_across)
    landed(slab, pt_send.at[1], pt_recv.at[1])
    start(slab, slab, pt_send.at[2], pt_recv.at[2], sibling)
    forward_chunks(second_kind, second, 2, chunks // 2)

    for part in range(TOKEN_PARTS):
        landed(token_part(0, t_sibling, part), rs_send.at[0, part], rs_recv.at[0, part])
        landed(token_part(0, t_diagonal, part), rs_send.at[1, part], rs_recv.at[1, part])
    for at in range(3):
        for q, t in enumerate((t_sibling, t_across, t_diagonal)):
            landed(small_all.at[t, at], small_send.at[at, q], small_recv.at[at, q])
    landed(pool_slab(t_sibling), pt_send.at[0], pt_recv.at[0])
    landed(pool_slab(t_diagonal), pt_send.at[2], pt_recv.at[2])

    positions = lax.broadcasted_iota(jnp.int32, (BAND, 1), 0).astype(F32) + 1.0
    distance = (
        lax.broadcasted_iota(jnp.int32, (BAND, 2 * BAND), 0)
        + BAND
        - lax.broadcasted_iota(jnp.int32, (BAND, 2 * BAND), 1)
    )

    def mix(slot, between):
        span = slice(slot * length, (slot + 1) * length)
        square = jnp.zeros((length, local), F32)
        for t in range(4):
            for g in range(groups):
                values = tokens[slot, t, :, g * local : (g + 1) * local].astype(F32)
                square = square + values * values
        factor = lax.rsqrt(jnp.sum(square, axis=1, keepdims=True) / width + EPSILON)
        square = jnp.zeros((length, local), F32)
        for g in range(groups):
            if g == groups // 2:
                between()
            part = slice(g * local, (g + 1) * local)
            for t in range(4):
                values = tokens[slot, t, :, part].astype(F32)
                normed[:, t * local : (t + 1) * local] = (
                    values * factor * small_all[t, 0, g : g + 1]
                ).astype(BF16)
            band = jnp.where((distance >= 0) & (distance < WINDOWS[g]), 1.0, 0.0).astype(BF16)
            for b in range(length // BAND):
                here = slice(b * BAND, (b + 1) * BAND)
                if b == 0:
                    totals = jnp.dot(band[:, BAND:], normed[here], preferred_element_type=F32)
                    totals = totals / jnp.minimum(positions, float(WINDOWS[g]))
                else:
                    totals = jnp.dot(
                        band,
                        normed[(b - 1) * BAND : (b + 1) * BAND],
                        preferred_element_type=F32,
                    ) * (1.0 / WINDOWS[g])
                pooled[here] = (totals - normed[here].astype(F32)).astype(BF16)
            mixed = jnp.dot(pooled[...], pool_full[g], preferred_element_type=F32)
            for t in range(4):
                made = (
                    mixed[:, t * local : (t + 1) * local] * small_all[t, 1, g : g + 1]
                    + tokens[slot, t, :, part].astype(F32)
                ).astype(BF16)
                inputs[span, g * channels + t * local : g * channels + (t + 1) * local] = made
                values = made.astype(F32)
                square = square + values * values
        factor = lax.rsqrt(jnp.sum(square, axis=1, keepdims=True) / width + EPSILON)
        if slot == 0:
            for g in range(groups):
                middle[:, g * local : (g + 1) * local] = inputs[
                    span, aligned(g * channels + tp * local, local)
                ]
        for g in range(groups):
            for t in range(4):
                columns = slice(g * channels + t * local, g * channels + (t + 1) * local)
                inputs[span, columns] = (
                    inputs[span, columns].astype(F32) * factor * small_all[t, 2, g : g + 1]
                ).astype(BF16)

    mix(0, functools.partial(forward_chunks, second_kind, second, chunks // 2, chunks // 2 + 1))
    forward_chunks(second_kind, second, chunks // 2 + 1, chunks)

    @pl.when(outer)
    def _():
        @pl.loop(0, chunks)
        def _(j):
            chunk_copy(j, 1).start()
            chunk_copy(j, 0).start()

        for sub in range(PIECES):
            down_copy(2, sub).start()

    for part in range(TOKEN_PARTS):
        piece = token_part(1, t_across, part)
        landed(piece, ry_send.at[1, part], ry_recv.at[1, part])
        start(piece, piece, rs_send.at[3, part], rs_recv.at[3, part], sibling)
    pl.when(outer)(functools.partial(forward_chunk, 0, 1, far))
    for part in range(TOKEN_PARTS):
        landed(token_part(1, t_sibling, part), rs_send.at[2, part], rs_recv.at[2, part])
        landed(token_part(1, t_diagonal, part), rs_send.at[3, part], rs_recv.at[3, part])

    def forward_late(j):
        forward_chunk(j, late_kind, late)
        pl.when(outer)(functools.partial(forward_chunk, j, 2, partner))

    forward_chunk(0, jnp.where(outer, 2, 0), jnp.where(outer, partner, same))
    mix(1, functools.partial(forward_late, 1))
    for at in range(2):
        for q, f in enumerate(sources):
            landed(scales_all.at[f, at], scale_send.at[at, q], scale_recv.at[at, q])

    thirds = scales_all.shape[3] // 128

    def expand(j):
        for q, f in enumerate(sources):
            landed(chunk_target(j, f, 1 - rep), gx_send.at[j, q], gx_recv.at[j, q])
        here = aligned(member * half_hidden + j * 128, 128)
        unit = member * chunks + j
        scale_at = aligned(lax.rem(unit, thirds) * 128, 128)
        taps = [
            table[:, here] * scales_all[unit // thirds, at, :, scale_at]
            for at, table in enumerate((gate_taps, up_taps))
        ]
        block = weights[j].reshape(width, 256)
        for slot in range(2):
            span = slice(slot * length, (slot + 1) * length)
            made = jnp.dot(inputs[span], block, preferred_element_type=F32)
            conv_gate = causal_taps(made[:, :128], taps[0])
            conv_up = causal_taps(made[:, 128:], taps[1])
            silu = conv_gate / (1.0 + jnp.exp(-conv_gate))
            hidden[span, aligned(j * 128, 128)] = (silu * conv_up).astype(BF16)

    @pl.loop(0, chunks)
    def _(j):
        expand(j)

        @pl.when(j < chunks - 2)
        def _():
            forward_late(j + 2)

        @pl.when(outer & (j == chunks - 2))
        def _():
            forward_down(0, same)
            for sub in range(PIECES):
                down_copy(1, sub).start()
                down_copy(0, sub).start()

    def core_copy(shard, half, slot):
        return remote(
            give.at[shard, half, slot],
            got.at[shard, half, slot],
            core_send.at[shard, half, slot],
            core_recv.at[shard, half, slot],
            sibling,
        )

    def product(shard, half):
        for slot in (1, 0):
            span = slice(slot * length, (slot + 1) * length)
            made = jnp.dot(hidden[span], down_full[shard, half], preferred_element_type=F32)
            low, high = made[:, :local], made[:, local:]
            keep[shard, half, slot] = jnp.where(core == 0, low, high)
            give[shard, half, slot] = jnp.where(core == 0, high, low).astype(BF16)
            core_copy(shard, half, slot).start()

    def y_copy(shard, slot):
        return remote(
            y_out.at[shard, slot],
            y_in.at[shard, slot],
            y_send.at[shard, slot],
            y_recv.at[shard, slot],
            across,
        )

    def arrived_x(q, shard):
        for sub in range(PIECES):
            landed(down_part(shard, 1 - rep, sub), dx_send.at[q, sub], dx_recv.at[q, sub])

    def join_cores(shard, half):
        for slot in (1, 0):
            core_copy(shard, half, slot).wait_recv()
            total = keep[shard, half, slot] + got[shard, half, slot].astype(F32)

            @pl.when(half == side)
            def _():
                keep[shard, half, slot] = total

            @pl.when(half != side)
            def _():
                y_out[shard, slot] = total.astype(BF16)
                y_copy(shard, slot).start()

    def join_sides(shard):
        y_copy(shard, 1).wait_recv()
        total = keep[shard, side, 1] + y_in[shard, 1].astype(F32)
        z_out[shard] = total.astype(BF16)
        start(
            z_out.at[shard],
            z_in.at[shard],
            z_send.at[shard],
            z_recv.at[shard],
            {"fs": partner},
        )

    def conclude(shard):
        y_copy(shard, 0).wait_recv()
        total = keep[shard, side, 0] + y_in[shard, 0].astype(F32)
        landed(z_in.at[shard], z_send.at[shard], z_recv.at[shard])
        columns = aligned(shard * local, local)
        total = total + z_in[shard].astype(F32)
        out[:, columns] = (
            total * down_scale[pl.ds(shard, 1), :] + middle[:, columns].astype(F32)
        ).astype(BF16)

    early, early_kind = jnp.where(outer, same, partner), jnp.where(outer, 0, 2)
    later, later_kind = jnp.where(outer, partner, same), jnp.where(outer, 2, 0)

    def pass_on(sub):
        pl.when(outer)(functools.partial(forward_down, 2, partner, (sub,)))
        forward_down(late_kind, late, (sub,))

    product(fs, rep)
    product(fs, 1 - rep)
    join_cores(fs, rep)
    pl.when(inner)(functools.partial(forward_down, 2, partner))
    join_cores(fs, 1 - rep)
    product(early, rep)
    pass_on(0)
    arrived_x(early_kind, early)
    product(early, 1 - rep)
    join_cores(early, rep)
    pass_on(1)
    join_cores(early, 1 - rep)
    pass_on(2)
    join_sides(fs)
    pass_on(3)
    product(later, rep)
    pl.when(inner)(functools.partial(forward_down, 1, far, (0, 1)))
    arrived_x(later_kind, later)
    product(later, 1 - rep)
    join_cores(later, rep)
    pl.when(inner)(functools.partial(forward_down, 1, far, (2, 3)))
    join_cores(later, 1 - rep)
    join_sides(early)
    product(far, rep)
    arrived_x(1, far)
    product(far, 1 - rep)
    join_cores(far, rep)
    join_cores(far, 1 - rep)
    join_sides(later)
    join_sides(far)
    conclude(partner)
    conclude(jnp.where(outer, fs, far))
    conclude(jnp.where(outer, far, fs))
    conclude(same)

    for copy in sent:
        copy.wait_send()
    for q in range(3):
        pool_copy_to(q).wait_send()
    for part in range(TOKEN_PARTS):
        token_copy(part).wait_send()
    for shard in range(4):
        for slot in range(2):
            y_copy(shard, slot).wait_send()
            for half in range(2):
                core_copy(shard, half, slot).wait_send()
    for q, f in enumerate(sources):
        for sub in range(PIECES):
            down_copy(q, sub).wait_send()
            down_onward(q, f, sub).wait_send()

    @pl.loop(0, chunks)
    def _(j):
        for q, f in enumerate(sources):
            chunk_copy(j, q).wait_send()
            chunk_onward(j, q, f).wait_send()


def pair_shards(
    residual,
    mixer_gain,
    pool_weight,
    pool_scale,
    channel_gain,
    gate_weight,
    up_weight,
    gate_scale,
    up_scale,
    gate_taps,
    up_taps,
    down_weight,
    down_scale,
):
    _, length, groups, local = residual.shape
    channels = local * 4
    width = groups * channels
    rows, hidden_width = gate_weight.shape
    half = hidden_width // 2
    chunks = half // 128
    half_columns = down_weight.shape[1] // 2
    vmem = pl.BlockSpec(memory_space=pltpu.VMEM)
    anywhere = pl.BlockSpec(memory_space=pl.ANY)
    dma = pltpu.SemaphoreType.DMA
    pairs = [
        (3, 3),
        (2, 3),
        (3,),
        (3,),
        (3,),
        (TOKEN_PARTS,),
        (2, TOKEN_PARTS),
        (4, TOKEN_PARTS),
        (chunks, 3),
        (chunks, 3),
        (3, PIECES),
        (3, PIECES),
        (4, 2, 2),
        (4, 2),
        (4,),
    ]
    out = pl.pallas_call(
        pair_kernel,
        out_shape=jax.ShapeDtypeStruct((length, groups * local), BF16),
        in_specs=[anywhere] + [vmem] * 8 + [anywhere] * 4,
        out_specs=vmem,
        scratch_shapes=[
            pltpu.VMEM((2, rows, half), F32),
            pltpu.VMEM((2, rows // 2, half), F32),
            pltpu.VMEM((half, 2 * half_columns), F32),
            pltpu.VMEM((half, half_columns), F32),
            pltpu.VMEM(pool_weight.shape, F32),
            pltpu.VMEM((2, 4, length, groups * local), BF16),
            pltpu.VMEM((4, 3, groups, local), F32),
            pltpu.VMEM((4, 2) + gate_scale.shape, F32),
            pltpu.VMEM(pool_weight.shape, BF16),
            pltpu.VMEM((groups, channels, channels), BF16),
            pltpu.VMEM((chunks, 4, rows, 256), BF16),
            pltpu.VMEM((chunks, rows // 2, 256), BF16),
            pltpu.VMEM((4, 2, half, half_columns), BF16),
            pltpu.VMEM((half, half_columns), BF16),
            pltpu.VMEM((length, channels), BF16),
            pltpu.VMEM((length, channels), BF16),
            pltpu.VMEM((2 * length, width), BF16),
            pltpu.VMEM((length, groups * local), BF16),
            pltpu.VMEM((2 * length, half), BF16),
            pltpu.VMEM((4, 2, 2, length, local), F32),
            pltpu.VMEM((4, 2, 2, length, local), BF16),
            pltpu.VMEM((4, 2, 2, length, local), BF16),
            pltpu.VMEM((4, 2, length, local), BF16),
            pltpu.VMEM((4, 2, length, local), BF16),
            pltpu.VMEM((4, length, local), BF16),
            pltpu.VMEM((4, length, local), BF16),
        ]
        + [dma(shape) for shape in pairs for _ in range(2)]
        + [dma((9,))],
        compiler_params=pltpu.CompilerParams(
            collective_id=0, has_side_effects=True, vmem_limit_bytes=VMEM_BYTES
        ),
    )(
        residual.reshape(length, groups * local),
        mixer_gain,
        pool_scale,
        channel_gain,
        down_scale,
        gate_scale,
        up_scale,
        gate_taps,
        up_taps,
        pool_weight,
        gate_weight,
        up_weight,
        down_weight,
    )
    return out.reshape(1, length, groups, local)


def paired(sizes, residual, gate_weight, down_weight):
    _, length, groups, local = residual
    return (
        sizes == (2, 4, 4)
        and residual[0] == 1
        and local == 128
        and length % BAND == 0
        and groups == len(WINDOWS)
        and down_weight[1] == 4 * local
        and gate_weight[0] * 4 == groups * local * 4
        and gate_weight[1] % 512 == 0
    )


def shards(
    sizes,
    residual,
    mixer_gain,
    pool_weight,
    pool_scale,
    channel_gain,
    gate_weight,
    up_weight,
    gate_scale,
    up_scale,
    gate_taps,
    up_taps,
    down_weight,
    down_scale,
):
    if paired(sizes, residual.shape, gate_weight.shape, down_weight.shape):
        return pair_shards(
            residual,
            mixer_gain,
            pool_weight,
            pool_scale,
            channel_gain,
            gate_weight,
            up_weight,
            gate_scale,
            up_scale,
            gate_taps,
            up_taps,
            down_weight,
            down_scale,
        )
    n_rep, n_fs, n_tp = sizes
    _, length, groups, local = residual.shape
    channels = local * n_tp
    width = groups * channels
    own_width = groups * local
    hidden_width = gate_weight.shape[1]
    vmem = pl.BlockSpec(memory_space=pltpu.VMEM)
    anywhere = pl.BlockSpec(memory_space=pl.ANY)
    dma = pltpu.SemaphoreType.DMA
    hops = max(n_fs - 1, 1)
    reps = max(n_rep - 1, 1)
    peers = max(n_tp - 1, 1)
    out = pl.pallas_call(
        functools.partial(block_kernel, sizes),
        out_shape=jax.ShapeDtypeStruct((length, own_width), BF16),
        in_specs=[vmem] * 8 + [anywhere] * 3,
        out_specs=vmem,
        scratch_shapes=[
            pltpu.VMEM((groups, channels, local), BF16),
            pltpu.VMEM((n_fs,) + gate_weight.shape, BF16),
            pltpu.VMEM((n_fs,) + up_weight.shape, BF16),
            pltpu.VMEM((n_fs,) + down_weight.shape, BF16),
            pltpu.VMEM((n_tp, length, own_width), BF16),
            pltpu.VMEM((n_tp, length, own_width), BF16),
            pltpu.VMEM((n_tp, 2, own_width), F32),
            pltpu.VMEM((n_fs, 2, gate_scale.shape[1]), F32),
            pltpu.VMEM((2, hidden_width), F32),
            pltpu.VMEM((length, channels), BF16),
            pltpu.VMEM((length, own_width), BF16),
            pltpu.VMEM((length, width), BF16),
            pltpu.VMEM((length, hidden_width), BF16),
            pltpu.VMEM((length, hidden_width), BF16),
            pltpu.VMEM((n_tp, groups, length, local), BF16),
            pltpu.VMEM((n_tp, groups, length, local), BF16),
            dma((3, SUBS, 2 * hops)),
            dma((3, SUBS, 2 * hops)),
            dma((3, SUBS, 2 * hops, reps)),
            dma((3, SUBS, 2 * hops, reps)),
            dma((hops,)),
            dma((hops,)),
            dma((hops, reps)),
            dma((hops, reps)),
            dma((hops,)),
            dma((hops,)),
            dma((3, peers)),
            dma((3, peers)),
            dma((n_fs, peers)),
            dma((n_fs, peers)),
            dma((7,)),
        ],
        compiler_params=pltpu.CompilerParams(
            collective_id=0, has_side_effects=True, vmem_limit_bytes=60 * 1024 * 1024
        ),
    )(
        residual.reshape(length, own_width),
        jnp.stack([mixer_gain.reshape(-1), channel_gain.reshape(-1)]),
        pool_scale.reshape(1, -1),
        down_scale.reshape(1, -1),
        jnp.concatenate([gate_scale, up_scale], axis=0),
        gate_taps,
        up_taps,
        pool_weight.astype(BF16),
        gate_weight.astype(BF16),
        up_weight.astype(BF16),
        down_weight.astype(BF16),
    )
    return out.reshape(1, length, groups, local)


def solution(mesh):
    placed = (
        P(("rep", "fs"), None, None, "tp"),
        P(None, "tp"),
        P(None, "fs", "tp"),
        P(None, "tp"),
        P(None, "tp"),
        P("fs", "tp"),
        P("fs", "tp"),
        P("fs", "tp"),
        P("fs", "tp"),
        P(None, "tp"),
        P(None, "tp"),
        P("tp", "fs"),
        P(None, "tp"),
    )
    sizes = tuple(mesh.shape[name] for name in ("rep", "fs", "tp"))
    return jax.shard_map(
        functools.partial(shards, sizes),
        mesh=mesh,
        in_specs=placed,
        out_specs=P(("rep", "fs"), None, None, "tp"),
        check_vma=False,
    )
```

```python
import functools

import jax
import jax.numpy as jnp
from jax import lax
from jax.experimental import pallas as pl
from jax.experimental.pallas import tpu as pltpu
from jax.sharding import PartitionSpec as P

WINDOWS = (2, 4, 8, 16)
EPSILON = 1e-05
SUBS = 2
COLUMNS = 256
VMEM_BYTES = 63 * 1024 * 1024 + 896 * 1024
F32 = jnp.float32
BF16 = jnp.bfloat16


def delayed(values, steps):
    rows = lax.broadcasted_iota(jnp.int32, values.shape, 0)
    return jnp.where(rows >= steps, pltpu.roll(values, steps, 0), 0.0)


def causal_taps(values, taps):
    return taps[2:3] * values + taps[1:2] * delayed(values, 1) + taps[0:1] * delayed(values, 2)


def block_kernel(
    sizes,
    residual,
    gains,
    pool_scale,
    down_scale,
    scale_pair,
    gate_taps,
    up_taps,
    pool_own,
    gate_own,
    up_own,
    down_own,
    out,
    pool_full,
    gate_full,
    up_full,
    down_full,
    gathered,
    middle_all,
    gains_all,
    scales_all,
    scale_row,
    pooled,
    middle,
    inputs,
    gate_pre,
    hidden,
    partials,
    arrived,
    ring_send,
    ring_recv,
    rep_send,
    rep_recv,
    pool_send,
    pool_recv,
    pool_rep_send,
    pool_rep_recv,
    scale_send,
    scale_recv,
    tp_send,
    tp_recv,
    part_send,
    part_recv,
    local_sem,
):
    n_rep, n_fs, n_tp = sizes
    rep, fs, tp = (lax.axis_index(name) for name in ("rep", "fs", "tp"))
    length = residual.shape[0]
    groups = pool_full.shape[0]
    channels = pool_full.shape[1]
    local = residual.shape[1] // groups
    width = groups * channels

    def other(axis, offset):
        me, count = {"rep": (rep, n_rep), "fs": (fs, n_fs), "tp": (tp, n_tp)}[axis]
        return lax.rem(me + offset, count)

    def remote(src, dst, send, recv, axis, offset):
        return pltpu.make_async_remote_copy(
            src_ref=src,
            dst_ref=dst,
            send_sem=send,
            recv_sem=recv,
            device_id={axis: other(axis, offset)},
            device_id_type=pl.DeviceIdType.MESH,
        )

    barrier = pltpu.get_barrier_semaphore()
    for axis, count in (("rep", n_rep), ("fs", n_fs), ("tp", n_tp)):
        for offset in range(1, count):
            pl.semaphore_signal(
                barrier,
                inc=1,
                device_id={axis: other(axis, offset)},
                device_id_type=pl.DeviceIdType.MESH,
            )
    pl.semaphore_wait(barrier, n_rep + n_fs + n_tp - 3)

    sent = []

    def start(copy, valid=None):
        sent.append((copy, valid))
        if valid is None:
            copy.start()
        else:
            pl.when(valid)(copy.start)

    weights = ((gate_own, gate_full), (up_own, up_full), (down_own, down_full))

    def piece(w, shard, half, sub, own=False):
        rows = weights[w][0].shape[0] // (n_rep * SUBS)
        part = pl.ds(pl.multiple_of((half * SUBS + sub) * rows, rows), rows)
        return weights[w][0].at[part] if own else weights[w][1].at[shard, part]

    def shard_sent(step, way):
        shard = fs + step if way else fs - step
        return jnp.clip(shard, 0, n_fs - 1), (shard <= n_fs - 1 if way else shard >= 0)

    def line(w, sub, step):
        for way in range(2):
            shard, valid = shard_sent(step, way)
            start(
                remote(
                    piece(w, shard, rep, sub, own=step == 0),
                    piece(w, shard, rep, sub),
                    ring_send.at[w, sub, 2 * step + way],
                    ring_recv.at[w, sub, 2 * step + way],
                    "fs",
                    n_fs - 1 if way else 1,
                ),
                valid & (fs > 0 if way else fs < n_fs - 1),
            )

    def serve(w, sub, step):
        for way in range(2):
            shard, valid = shard_sent(step + 1, way)
            mine = piece(w, shard, rep, sub)
            sems = (w, sub, 2 * step + way)
            pl.when(valid)(
                remote(
                    mine, mine, ring_send.at[sems], ring_recv.at[sems], "fs", 1
                ).wait_recv
            )
            if step < n_fs - 2:
                onward = (w, sub, 2 * step + 2 + way)
                start(
                    remote(
                        mine,
                        mine,
                        ring_send.at[onward],
                        ring_recv.at[onward],
                        "fs",
                        n_fs - 1 if way else 1,
                    ),
                    valid & (fs > 0 if way else fs < n_fs - 1),
                )
            for d in range(1, n_rep):
                start(
                    remote(
                        mine,
                        mine,
                        rep_send.at[sems + (d - 1,)],
                        rep_recv.at[sems + (d - 1,)],
                        "rep",
                        d,
                    ),
                    valid,
                )

    def settle(w, step, ways=(0, 1)):
        for way in ways:
            shard, valid = shard_sent(step + 1, way)

            @pl.when(valid)
            def _():
                for sub in range(SUBS):
                    for d in range(1, n_rep):
                        got = piece(w, shard, other("rep", n_rep - d), sub)
                        sems = (w, sub, 2 * step + way, d - 1)
                        remote(
                            got, got, rep_send.at[sems], rep_recv.at[sems], "rep", d
                        ).wait_recv()

    def local_copy(src, dst, idx):
        copy = pltpu.make_async_copy(src, dst, local_sem.at[idx])
        copy.start()
        return copy

    own_copies = [
        local_copy(residual, gathered.at[tp], 0),
        local_copy(gains, gains_all.at[tp], 1),
        local_copy(scale_pair, scales_all.at[fs], 2),
        local_copy(gate_own, gate_full.at[fs], 3),
        local_copy(up_own, up_full.at[fs], 4),
        local_copy(down_own, down_full.at[fs], 5),
    ]

    pool_rows = pool_own.shape[1]
    rep_groups = groups // n_rep

    def pool_part(shard, half):
        return pool_full.at[
            pl.ds(half * rep_groups, rep_groups),
            pl.ds(pl.multiple_of(shard * pool_rows, pool_rows), pool_rows),
        ]

    pool_copy = local_copy(
        pool_own, pool_full.at[:, pl.ds(pl.multiple_of(fs * pool_rows, pool_rows), pool_rows)], 6
    )

    for d in range(1, n_fs):
        start(
            remote(
                pool_own.at[pl.ds(rep * rep_groups, rep_groups)],
                pool_part(fs, rep),
                pool_send.at[d - 1],
                pool_recv.at[d - 1],
                "fs",
                d,
            )
        )
    for w in (0, 1):
        for sub in range(SUBS):
            if n_fs > 1:
                line(w, sub, 0)
    for d in range(1, n_tp):
        start(remote(gains, gains_all.at[tp], tp_send.at[0, d - 1], tp_recv.at[0, d - 1], "tp", d))
    for d in range(1, n_tp):
        start(
            remote(residual, gathered.at[tp], tp_send.at[1, d - 1], tp_recv.at[1, d - 1], "tp", d)
        )
    for d in range(1, n_fs):
        start(
            remote(
                scale_pair, scales_all.at[fs], scale_send.at[d - 1], scale_recv.at[d - 1], "fs", d
            )
        )

    for d in range(1, n_fs):
        shard = other("fs", n_fs - d)
        mine = pool_part(shard, rep)
        remote(mine, mine, pool_send.at[d - 1], pool_recv.at[d - 1], "fs", d).wait_recv()
        for e in range(1, n_rep):
            start(
                remote(
                    mine,
                    mine,
                    pool_rep_send.at[d - 1, e - 1],
                    pool_rep_recv.at[d - 1, e - 1],
                    "rep",
                    e,
                )
            )
    for d in range(1, n_fs):
        shard = other("fs", n_fs - d)
        for e in range(1, n_rep):
            got = pool_part(shard, other("rep", n_rep - e))
            remote(
                got,
                got,
                pool_rep_send.at[d - 1, e - 1],
                pool_rep_recv.at[d - 1, e - 1],
                "rep",
                e,
            ).wait_recv()
    pool_copy.wait()
    for copy in own_copies:
        copy.wait()

    def tp_arrivals(idx, buffer):
        for d in range(1, n_tp):
            got = buffer.at[other("tp", n_tp - d)]
            remote(got, got, tp_send.at[idx, d - 1], tp_recv.at[idx, d - 1], "tp", d).wait_recv()

    for sub in range(SUBS):
        serve(0, sub, 0)
    tp_arrivals(0, gains_all)
    tp_arrivals(1, gathered)
    for sub in range(SUBS):
        serve(1, sub, 0)

    def mean_square_root(buffer):
        total = jnp.zeros((length, 1), F32)
        for t in range(n_tp):
            values = buffer[t].astype(F32)
            total = total + jnp.sum(values * values, axis=1, keepdims=True)
        return lax.rsqrt(total / width + EPSILON)

    factor = mean_square_root(gathered)
    positions = lax.broadcasted_iota(jnp.int32, (length, 1), 0).astype(F32) + 1.0
    for g in range(groups):
        part = slice(g * local, (g + 1) * local)
        share = 1.0 / jnp.minimum(positions, float(WINDOWS[g]))
        for t in range(n_tp):
            values = gathered[t, :, part].astype(F32)
            normed = (values * factor * gains_all[t, 0:1, part]).astype(BF16).astype(F32)
            totals = normed
            reach = 1
            while reach < WINDOWS[g]:
                totals = totals + delayed(totals, reach)
                reach = reach * 2
            pooled[:, t * local : (t + 1) * local] = (totals * share - normed).astype(BF16)
        mixed = jnp.dot(pooled[...], pool_full[g], preferred_element_type=F32)
        middle[:, part] = (
            mixed * pool_scale[:, part] + residual[:, part].astype(F32)
        ).astype(BF16)

    middle_copy = local_copy(middle, middle_all.at[tp], 0)
    for d in range(1, n_tp):
        start(
            remote(middle, middle_all.at[tp], tp_send.at[2, d - 1], tp_recv.at[2, d - 1], "tp", d)
        )
    for step in range(1, n_fs - 1):
        for w in (0, 1):
            if step == n_fs - 2 and n_fs > 2:
                break
            for sub in range(SUBS):
                serve(w, sub, step)
    for sub in range(SUBS):
        if n_fs > 1:
            line(2, sub, 0)
    for d in range(1, n_fs):
        got = scales_all.at[other("fs", n_fs - d)]
        remote(got, got, scale_send.at[d - 1], scale_recv.at[d - 1], "fs", d).wait_recv()
    shard_columns = scale_pair.shape[1]
    for f in range(n_fs):
        scale_row[:, f * shard_columns : (f + 1) * shard_columns] = scales_all[f]

    middle_copy.wait()
    tp_arrivals(2, middle_all)
    factor = mean_square_root(middle_all)
    for t in range(n_tp):
        for g in range(groups):
            part = slice(g * local, (g + 1) * local)
            start_column = g * channels + t * local
            inputs[:, start_column : start_column + local] = (
                middle_all[t, :, part].astype(F32) * factor * gains_all[t, 1:2, part]
            ).astype(BF16)

    def finish(w):
        if n_fs > 2:
            for sub in range(SUBS):
                serve(w, sub, n_fs - 2)
        for step in range(n_fs - 1):
            settle(w, step)

    def product(full, columns, row):
        block = full[:, :, columns].reshape(width, COLUMNS)
        made = jnp.dot(inputs[...], block, preferred_element_type=F32)
        return (made * scale_row[row : row + 1, columns]).astype(BF16)

    chunks = gate_full.shape[2] // COLUMNS

    finish(0)

    @pl.loop(0, chunks)
    def _(j):
        columns = pl.ds(pl.multiple_of(j * COLUMNS, COLUMNS), COLUMNS)
        gate_pre[:, columns] = product(gate_full, columns, 0)

    finish(1)
    for sub in range(SUBS):
        if n_fs > 1:
            serve(2, sub, 0)

    @pl.loop(0, chunks)
    def _(j):
        columns = pl.ds(pl.multiple_of(j * COLUMNS, COLUMNS), COLUMNS)
        up_values = product(up_full, columns, 1).astype(F32)
        conv_gate = causal_taps(gate_pre[:, columns].astype(F32), gate_taps[:, columns])
        conv_up = causal_taps(up_values, up_taps[:, columns])
        silu = conv_gate / (1.0 + jnp.exp(-conv_gate))
        hidden[:, columns] = (silu * conv_up).astype(BF16)

    shard_width = down_own.shape[1]

    def to_peers(idx, src, dst):
        for d in range(1, n_tp):
            start(
                remote(
                    src(other("tp", d)),
                    dst(tp),
                    part_send.at[idx, d - 1],
                    part_recv.at[idx, d - 1],
                    "tp",
                    d,
                )
            )

    def from_peers(idx, dst):
        for d in range(1, n_tp):
            got = dst(other("tp", n_tp - d))
            remote(
                got, got, part_send.at[idx, d - 1], part_recv.at[idx, d - 1], "tp", d
            ).wait_recv()

    def conclude(g, columns):
        total = partials[tp, g].astype(F32)
        for d in range(1, n_tp):
            total = total + arrived[other("tp", d), g].astype(F32)
        out[:, columns] = (
            total * down_scale[:, columns] + middle[:, columns].astype(F32)
        ).astype(BF16)

    if shard_width == channels and local % 128 == 0:
        def share(shard):
            made = jnp.dot(hidden[...], down_full[shard], preferred_element_type=F32)
            for t in range(n_tp):
                partials[t, shard] = made[:, t * local : (t + 1) * local].astype(BF16)
            for d in range(1, n_tp):
                peer = other("tp", d)
                remote(
                    partials.at[peer, shard],
                    arrived.at[tp, shard],
                    part_send.at[shard, d - 1],
                    part_recv.at[shard, d - 1],
                    "tp",
                    d,
                ).start()

        share(fs)
        for step in range(n_fs - 1):
            if step >= 1:
                for sub in range(SUBS):
                    serve(2, sub, step)
            for way in range(2):
                settle(2, step, (way,))
                shard, valid = shard_sent(step + 1, way)
                pl.when(valid)(functools.partial(share, shard))
        for shard in range(n_fs):
            from_peers(shard, lambda t: arrived.at[t, shard])
            conclude(shard, slice(shard * local, (shard + 1) * local))
            for d in range(1, n_tp):
                mine = partials.at[other("tp", d), shard]
                remote(
                    mine, mine, part_send.at[shard, d - 1], part_recv.at[shard, d - 1], "tp", d
                ).wait_send()
    else:
        for step in range(n_fs - 1):
            if step >= 1:
                for sub in range(SUBS):
                    serve(2, sub, step)
            settle(2, step)
        for f in range(n_fs):
            made = jnp.dot(hidden[...], down_full[f], preferred_element_type=F32).astype(BF16)
            span = min(local, shard_width)
            for at in range(0, shard_width, span):
                g, channel = divmod(f * shard_width + at, channels)
                t, low = divmod(channel, local)
                partials[t, g, :, low : low + span] = made[:, at : at + span]
        to_peers(0, lambda t: partials.at[t], lambda t: arrived.at[t])
        from_peers(0, lambda t: arrived.at[t])
        for g in range(groups):
            conclude(g, slice(g * local, (g + 1) * local))

    for copy, valid in sent:
        if valid is None:
            copy.wait_send()
        else:
            pl.when(valid)(copy.wait_send)


BAND = 256
TOKEN_PARTS = 2


def pair_kernel(
    residual,
    mixer_gain,
    pool_scale,
    channel_gain,
    down_scale_own,
    gate_scale,
    up_scale,
    gate_taps_own,
    up_taps_own,
    pool_own,
    gate_own,
    up_own,
    down_own,
    out,
    down_scale,
    gate_taps,
    up_taps,
    stage_own,
    stage_other,
    stage_down,
    stage_down_other,
    stage_pool,
    tokens,
    small_all,
    scales_all,
    pool_near,
    pool_full,
    weights,
    other,
    down_full,
    down_other,
    normed,
    pooled,
    inputs,
    middle,
    hidden,
    keep,
    give,
    got,
    y_out,
    y_in,
    z_out,
    z_in,
    small_send,
    small_recv,
    scale_send,
    scale_recv,
    pz_send,
    pz_recv,
    px_send,
    px_recv,
    pt_send,
    pt_recv,
    rz_send,
    rz_recv,
    ry_send,
    ry_recv,
    rs_send,
    rs_recv,
    gz_send,
    gz_recv,
    gx_send,
    gx_recv,
    dz_send,
    dz_recv,
    dx_send,
    dx_recv,
    core_send,
    core_recv,
    y_send,
    y_recv,
    z_send,
    z_recv,
    local_sem,
):
    rep, fs, tp = (lax.axis_index(name) for name in ("rep", "fs", "tp"))
    length = residual.shape[0]
    groups, pool_rows, local = pool_own.shape
    channels = pool_full.shape[1]
    width = groups * channels
    rows = gate_own.shape[0]
    half_rows = rows // 2
    chunks = gate_own.shape[1] // 128
    few = chunks * 5 // 12
    many = chunks - few
    half_columns = down_own.shape[1] // 2
    member = lax.rem(fs, 2)
    side = tp // 2
    core = lax.rem(tp, 2)
    sibling = {"tp": tp + 1 - 2 * core}
    across = {"tp": lax.rem(tp + 2, 4)}
    diagonal = {"tp": 3 - tp}
    mirror = {"rep": 1 - rep}
    same, far, partner = lax.rem(fs + 2, 4), 3 - fs, fs + 1 - 2 * member
    sources = (same, far, partner)
    outer = (fs == 0) | (fs == 3)
    inner = jnp.logical_not(outer)
    count = jnp.where(outer, few, many)
    other_count = chunks - count
    begin = jnp.where(outer, many, 0)
    skip = jnp.where(outer, many - few, 0)
    other_skip = many - few - skip

    sent = []

    def remote(src, dst, send, recv, device):
        return pltpu.make_async_remote_copy(
            src_ref=src,
            dst_ref=dst,
            send_sem=send,
            recv_sem=recv,
            device_id=device,
            device_id_type=pl.DeviceIdType.MESH,
        )

    def start(*parts):
        copy = remote(*parts)
        sent.append(copy)
        copy.start()

    def aligned(at, size):
        return pl.ds(pl.multiple_of(at, size), size)

    def local_copy(src, dst, idx):
        copy = pltpu.make_async_copy(src, dst, local_sem.at[idx])
        copy.start()
        return copy

    barrier = pltpu.get_barrier_semaphore()
    peers = (mirror, sibling, across, diagonal) + tuple({"fs": f} for f in sources)
    for device in peers:
        pl.semaphore_signal(
            barrier, inc=1, device_id=device, device_id_type=pl.DeviceIdType.MESH
        )
    mine = pl.ds(pl.multiple_of(jnp.where(outer, few, 0) * 128, 128), many * 128)
    theirs = pl.ds(pl.multiple_of(jnp.where(outer, 0, few) * 128, 128), many * 128)
    rep_rows = aligned(rep * half_rows, half_rows)
    rep_columns = aligned(rep * half_columns, half_columns)
    load_pool = local_copy(pool_own, stage_pool, 1)
    load_tokens = local_copy(residual, tokens.at[0, tp], 0)
    loads = [
        local_copy(gate_own.at[:, mine], stage_own.at[0], 2),
        local_copy(up_own.at[:, mine], stage_own.at[1], 3),
        local_copy(gate_own.at[rep_rows, theirs], stage_other.at[0], 4),
        local_copy(up_own.at[rep_rows, theirs], stage_other.at[1], 5),
    ]
    load_down = [
        local_copy(down_own.at[mine], stage_down, 6),
        local_copy(down_own.at[theirs, rep_columns], stage_down_other, 7),
    ]

    small_loads = [
        local_copy(src, dst, 9 + at)
        for at, (src, dst) in enumerate(
            (
                (mixer_gain, small_all.at[tp, 0]),
                (pool_scale, small_all.at[tp, 1]),
                (channel_gain, small_all.at[tp, 2]),
                (gate_scale, scales_all.at[fs, 0]),
                (up_scale, scales_all.at[fs, 1]),
                (down_scale_own, down_scale),
                (gate_taps_own, gate_taps),
                (up_taps_own, up_taps),
            )
        )
    ]
    load_pool.wait()
    pool_near[...] = stage_pool[...].astype(BF16)
    load_tokens.wait()
    pl.semaphore_wait(barrier, len(peers))

    def token_part(slot, t, part):
        span = length // TOKEN_PARTS
        return tokens.at[slot, t, pl.ds(part * span, span)]

    def pool_part(shard, half):
        span = groups // 2
        return pool_full.at[
            pl.ds(half * span, span),
            aligned(shard * pool_rows, pool_rows),
            aligned(tp * local, local),
        ]

    def pool_copy_to(q):
        return remote(
            pool_near.at[pl.ds(rep * (groups // 2), groups // 2)],
            pool_part(fs, rep),
            pz_send.at[q],
            pz_recv.at[q],
            {"fs": sources[q]},
        )

    for q in (2, 1, 0):
        pool_copy_to(q).start()
    for part in range(TOKEN_PARTS):
        piece = token_part(0, tp, part)
        start(piece, piece, ry_send.at[0, part], ry_recv.at[0, part], across)
        start(piece, piece, rs_send.at[0, part], rs_recv.at[0, part], sibling)
    for at, values in enumerate((mixer_gain, pool_scale, channel_gain)):
        for q, device in enumerate((sibling, across, diagonal)):
            start(values, small_all.at[tp, at], small_send.at[at, q], small_recv.at[at, q], device)
    for at, values in enumerate((gate_scale, up_scale)):
        for q, f in enumerate(sources):
            start(
                values, scales_all.at[fs, at], scale_send.at[at, q], scale_recv.at[at, q], {"fs": f}
            )
    pool_copy = local_copy(
        pool_near,
        pool_full.at[:, aligned(fs * pool_rows, pool_rows), aligned(tp * local, local)],
        8,
    )

    late, late_kind = jnp.where(outer, far, same), jnp.where(outer, 1, 0)

    def chunk_target(j, shard, half):
        return weights.at[j, shard, aligned(half * half_rows, half_rows)]

    def chunk_copy(j, q):
        target = chunk_target(j, fs, rep)
        source = target if q == 1 else other.at[j]
        return remote(source, target, gz_send.at[j, q], gz_recv.at[j, q], {"fs": sources[q]})

    def down_part(shard, half, unit):
        return down_full.at[shard, half, aligned(unit * 128, 128)]

    def down_copy(q, unit):
        target = down_part(fs, rep, unit)
        source = down_other.at[aligned(unit * 128, 128)]
        return remote(source, target, dz_send.at[q, unit], dz_recv.at[q, unit], {"fs": sources[q]})

    def slice_part(shard, half, unit, lane):
        return down_full.at[
            shard, half, aligned(unit * 128, 128), pl.ds(lane * local, local)
        ]

    def slice_copy(unit, lane):
        piece = slice_part(fs, rep, unit, lane)
        return remote(
            piece, piece, dz_send.at[1 + 2 * lane, unit], dz_recv.at[1 + 2 * lane, unit], {"fs": far}
        )

    def token_copy(part):
        return remote(
            token_part(0, tp, part),
            token_part(1, tp, part),
            rz_send.at[part],
            rz_recv.at[part],
            {"fs": partner},
        )

    for part in range(TOKEN_PARTS):
        token_copy(part).start()
    for load in loads + small_loads:
        load.wait()

    @pl.loop(0, many)
    def _(j):
        @pl.when(j < other_count)
        def _():
            columns = aligned((other_skip + j) * 128, 128)
            for at in range(2):
                lanes = slice(at * 128, (at + 1) * 128)
                other[j, :, lanes] = stage_other[at, :, columns].astype(BF16)
            chunk_copy(j, 2).start()

        @pl.when(j < count)
        def _():
            columns = aligned((skip + j) * 128, 128)
            for at in range(2):
                lanes = slice(at * 128, (at + 1) * 128)
                weights[j, fs, :, lanes] = stage_own[at, :, columns].astype(BF16)
            pl.when(inner)(chunk_copy(j, 1).start)

    @pl.when(inner)
    def _():
        @pl.loop(0, other_count)
        def _(j):
            chunk_copy(j, 0).start()

    for load in load_down:
        load.wait()
    hidden[:, few * 128 :] = jnp.zeros((2 * length, (many - few) * 128), BF16)

    @pl.when(outer)
    def _():
        down_full[:, :, few * 128 :] = jnp.zeros(
            (4, 2, (many - few) * 128, half_columns), BF16
        )

    @pl.loop(0, count)
    def _(j):
        here = aligned(j * 128, 128)
        there = aligned((skip + j) * 128, 128)
        for half in range(2):
            down_full[fs, half, here] = stage_down[
                there, half * half_columns : (half + 1) * half_columns
            ].astype(BF16)

    @pl.loop(0, other_count)
    def _(j):
        there = aligned((other_skip + j) * 128, 128)
        down_other[aligned(j * 128, 128)] = stage_down_other[there].astype(BF16)

    @pl.when(inner)
    def _():
        @pl.loop(0, other_count)
        def _(unit):
            down_copy(2, unit).start()

        @pl.loop(0, other_count)
        def _(unit):
            down_copy(0, unit).start()

        for lane in range(2):

            @pl.loop(0, count)
            def _(unit):
                slice_copy(unit, lane).start()

    def landed(ref, send, recv):
        remote(ref, ref, send, recv, mirror).wait_recv()

    def chunk_onward(j, q, shard):
        piece = chunk_target(j, shard, rep)
        return remote(piece, piece, gx_send.at[j, q], gx_recv.at[j, q], mirror)

    def forward_chunk(j, q, shard):
        piece = chunk_target(j, shard, rep)
        landed(piece, gz_send.at[j, q], gz_recv.at[j, q])
        chunk_onward(j, q, shard).start()

    def down_onward(q, shard, unit):
        piece = down_part(shard, rep, unit)
        return remote(piece, piece, dx_send.at[q, unit], dx_recv.at[q, unit], mirror)

    def slice_onward(unit, lane):
        piece = slice_part(far, rep, unit, lane)
        sem = (1 + 2 * lane, unit)
        return remote(piece, piece, dx_send.at[sem], dx_recv.at[sem], mirror)

    def forward_slice(lane, low=0, high=many):
        @pl.loop(low, jnp.minimum(count, high))
        def _(unit):
            sem = (1 + 2 * lane, unit)
            landed(slice_part(far, rep, unit, lane), dz_send.at[sem], dz_recv.at[sem])
            slice_onward(unit, lane).start()

    def forward_down(q, shard, low=0, high=many):
        @pl.loop(low, jnp.minimum(count, high))
        def _(unit):
            landed(down_part(shard, rep, unit), dz_send.at[q, unit], dz_recv.at[q, unit])
            down_onward(q, shard, unit).start()

    for q, f in ((2, partner), (1, far), (0, same)):
        piece = pool_part(f, rep)
        landed(piece, pz_send.at[q], pz_recv.at[q])
        start(piece, piece, px_send.at[q], px_recv.at[q], mirror)
    for q, f in enumerate(sources):
        landed(pool_part(f, 1 - rep), px_send.at[q], px_recv.at[q])
    pool_copy.wait()

    def pool_slab(t):
        return pool_full.at[:, :, aligned(t * local, local)]

    slab = pool_slab(tp)
    start(slab, slab, pt_send.at[1], pt_recv.at[1], across)
    start(slab, slab, pt_send.at[0], pt_recv.at[0], sibling)

    t_sibling, t_across, t_diagonal = sibling["tp"], across["tp"], diagonal["tp"]

    def own_onward(part):
        piece = token_part(0, t_across, part)
        landed(piece, ry_send.at[0, part], ry_recv.at[0, part])
        start(piece, piece, rs_send.at[1, part], rs_recv.at[1, part], sibling)

    def partner_onward(part):
        piece = token_part(1, tp, part)
        landed(piece, rz_send.at[part], rz_recv.at[part])
        start(piece, piece, ry_send.at[1, part], ry_recv.at[1, part], across)
        start(piece, piece, rs_send.at[2, part], rs_recv.at[2, part], sibling)

    def forward_chunks(kind, shard, low, high):
        for j in range(low, high):
            forward_chunk(j, kind, shard)

    third = many // 3
    own_onward(0)
    pl.when(inner)(functools.partial(forward_chunks, 1, far, 0, third))
    partner_onward(0)
    own_onward(1)
    pl.when(inner)(functools.partial(forward_chunks, 1, far, third, many - third))
    partner_onward(1)
    pl.when(inner)(functools.partial(forward_chunks, 1, far, many - third, many))
    second_kind, second = jnp.where(outer, 0, 2), jnp.where(outer, same, partner)
    forward_chunks(second_kind, second, 0, few - 3)
    slab = pool_slab(t_across)
    landed(slab, pt_send.at[1], pt_recv.at[1])
    start(slab, slab, pt_send.at[2], pt_recv.at[2], sibling)
    forward_chunks(second_kind, second, few - 3, few - 2)

    for part in range(TOKEN_PARTS):
        landed(token_part(0, t_sibling, part), rs_send.at[0, part], rs_recv.at[0, part])
        landed(token_part(0, t_diagonal, part), rs_send.at[1, part], rs_recv.at[1, part])
    for at in range(3):
        for q, t in enumerate((t_sibling, t_across, t_diagonal)):
            landed(small_all.at[t, at], small_send.at[at, q], small_recv.at[at, q])
    landed(pool_slab(t_sibling), pt_send.at[0], pt_recv.at[0])
    landed(pool_slab(t_diagonal), pt_send.at[2], pt_recv.at[2])

    positions = lax.broadcasted_iota(jnp.int32, (BAND, 1), 0).astype(F32) + 1.0
    distance = (
        lax.broadcasted_iota(jnp.int32, (BAND, 2 * BAND), 0)
        + BAND
        - lax.broadcasted_iota(jnp.int32, (BAND, 2 * BAND), 1)
    )

    def mix(slot, between):
        span = slice(slot * length, (slot + 1) * length)
        square = jnp.zeros((length, local), F32)
        for t in range(4):
            for g in range(groups):
                values = tokens[slot, t, :, g * local : (g + 1) * local].astype(F32)
                square = square + values * values
        factor = lax.rsqrt(jnp.sum(square, axis=1, keepdims=True) / width + EPSILON)
        square = jnp.zeros((length, local), F32)
        for g in range(groups):
            if g == groups // 2:
                between()
            part = slice(g * local, (g + 1) * local)
            for t in range(4):
                values = tokens[slot, t, :, part].astype(F32)
                normed[:, t * local : (t + 1) * local] = (
                    values * factor * small_all[t, 0, g : g + 1]
                ).astype(BF16)
            band = jnp.where((distance >= 0) & (distance < WINDOWS[g]), 1.0, 0.0).astype(BF16)
            for b in range(length // BAND):
                here = slice(b * BAND, (b + 1) * BAND)
                if b == 0:
                    totals = jnp.dot(band[:, BAND:], normed[here], preferred_element_type=F32)
                    totals = totals / jnp.minimum(positions, float(WINDOWS[g]))
                else:
                    totals = jnp.dot(
                        band,
                        normed[(b - 1) * BAND : (b + 1) * BAND],
                        preferred_element_type=F32,
                    ) * (1.0 / WINDOWS[g])
                pooled[here] = (totals - normed[here].astype(F32)).astype(BF16)
            mixed = jnp.dot(pooled[...], pool_full[g], preferred_element_type=F32)
            for t in range(4):
                made = (
                    mixed[:, t * local : (t + 1) * local] * small_all[t, 1, g : g + 1]
                    + tokens[slot, t, :, part].astype(F32)
                ).astype(BF16)
                inputs[span, g * channels + t * local : g * channels + (t + 1) * local] = made
                values = made.astype(F32)
                square = square + values * values
        factor = lax.rsqrt(jnp.sum(square, axis=1, keepdims=True) / width + EPSILON)
        if slot == 0:
            for g in range(groups):
                middle[:, g * local : (g + 1) * local] = inputs[
                    span, aligned(g * channels + tp * local, local)
                ]
        for g in range(groups):
            for t in range(4):
                columns = slice(g * channels + t * local, g * channels + (t + 1) * local)
                inputs[span, columns] = (
                    inputs[span, columns].astype(F32) * factor * small_all[t, 2, g : g + 1]
                ).astype(BF16)

    def cross():
        forward_chunks(second_kind, second, few - 2, few)

        @pl.when(outer)
        def _():
            @pl.loop(0, many)
            def _(j):
                pl.when(j < few)(chunk_copy(j, 1).start)
                chunk_copy(j, 0).start()

            @pl.loop(0, many)
            def _(unit):
                down_copy(2, unit).start()

    mix(0, cross)
    pl.when(inner)(functools.partial(forward_chunks, 2, partner, few, many))
    for part in range(TOKEN_PARTS):
        piece = token_part(1, t_across, part)
        landed(piece, ry_send.at[1, part], ry_recv.at[1, part])
        start(piece, piece, rs_send.at[3, part], rs_recv.at[3, part], sibling)
    pl.when(outer)(functools.partial(forward_chunk, 0, 1, far))
    for part in range(TOKEN_PARTS):
        landed(token_part(1, t_sibling, part), rs_send.at[2, part], rs_recv.at[2, part])
        landed(token_part(1, t_diagonal, part), rs_send.at[3, part], rs_recv.at[3, part])

    def forward_late(j):
        forward_chunk(j, late_kind, late)
        pl.when(outer)(functools.partial(forward_chunk, j, 2, partner))

    forward_chunk(0, jnp.where(outer, 2, 0), jnp.where(outer, partner, same))
    mix(1, functools.partial(forward_late, 1))
    for at in range(2):
        for q, f in enumerate(sources):
            landed(scales_all.at[f, at], scale_send.at[at, q], scale_recv.at[at, q])

    thirds = scales_all.shape[3] // 128

    def expand(j):
        for q, f in enumerate(sources):
            landed(chunk_target(j, f, 1 - rep), gx_send.at[j, q], gx_recv.at[j, q])
        unit = begin + j
        here = aligned(unit * 128, 128)
        scale_at = aligned(lax.rem(unit, thirds) * 128, 128)
        taps = [
            table[:, here] * scales_all[unit // thirds, at, :, scale_at]
            for at, table in enumerate((gate_taps, up_taps))
        ]
        block = weights[j].reshape(width, 256)
        for slot in range(2):
            span = slice(slot * length, (slot + 1) * length)
            made = jnp.dot(inputs[span], block, preferred_element_type=F32)
            conv_gate = causal_taps(made[:, :128], taps[0])
            conv_up = causal_taps(made[:, 128:], taps[1])
            silu = conv_gate / (1.0 + jnp.exp(-conv_gate))
            hidden[span, aligned(j * 128, 128)] = (silu * conv_up).astype(BF16)

    @pl.loop(0, count)
    def _(j):
        expand(j)

        @pl.when(j < count - 2)
        def _():
            forward_late(j + 2)

        @pl.when(outer & (j == few - 2))
        def _():
            forward_down(0, same)

            @pl.loop(0, many)
            def _(unit):
                @pl.when(unit < few)
                def _():
                    for lane in range(2):
                        slice_copy(unit, lane).start()

                down_copy(0, unit).start()

    def core_copy(shard, half, slot):
        return remote(
            give.at[shard, half, slot],
            got.at[shard, half, slot],
            core_send.at[shard, half, slot],
            core_recv.at[shard, half, slot],
            sibling,
        )

    def product(shard, half):
        for slot in (1, 0):
            span = slice(slot * length, (slot + 1) * length)
            made = jnp.dot(hidden[span], down_full[shard, half], preferred_element_type=F32)
            low, high = made[:, :local], made[:, local:]
            keep[shard, half, slot] = jnp.where(core == 0, low, high)
            give[shard, half, slot] = jnp.where(core == 0, high, low).astype(BF16)
            core_copy(shard, half, slot).start()

    def far_product(half, lane):
        for slot in (1, 0):
            span = slice(slot * length, (slot + 1) * length)
            made = jnp.dot(
                hidden[span],
                down_full[far, half, :, lane * local : (lane + 1) * local],
                preferred_element_type=F32,
            )

            @pl.when(core == lane)
            def _():
                keep[far, half, slot] = made

            @pl.when(core != lane)
            def _():
                give[far, half, slot] = made.astype(BF16)
                core_copy(far, half, slot).start()

    def y_copy(shard, slot):
        return remote(
            y_out.at[shard, slot],
            y_in.at[shard, slot],
            y_send.at[shard, slot],
            y_recv.at[shard, slot],
            across,
        )

    def arrived_x(q, shard):
        @pl.loop(0, count)
        def _(unit):
            landed(down_part(shard, 1 - rep, unit), dx_send.at[q, unit], dx_recv.at[q, unit])

    def join_cores(shard, half):
        for slot in (1, 0):
            core_copy(shard, half, slot).wait_recv()
            total = keep[shard, half, slot] + got[shard, half, slot].astype(F32)

            @pl.when(half == side)
            def _():
                keep[shard, half, slot] = total

            @pl.when(half != side)
            def _():
                y_out[shard, slot] = total.astype(BF16)
                y_copy(shard, slot).start()

    def join_sides(shard):
        y_copy(shard, 1).wait_recv()
        total = keep[shard, side, 1] + y_in[shard, 1].astype(F32)
        z_out[shard] = total.astype(BF16)
        start(
            z_out.at[shard],
            z_in.at[shard],
            z_send.at[shard],
            z_recv.at[shard],
            {"fs": partner},
        )

    def conclude(shard):
        y_copy(shard, 0).wait_recv()
        total = keep[shard, side, 0] + y_in[shard, 0].astype(F32)
        landed(z_in.at[shard], z_send.at[shard], z_recv.at[shard])
        columns = aligned(shard * local, local)
        total = total + z_in[shard].astype(F32)
        out[:, columns] = (
            total * down_scale[pl.ds(shard, 1), :] + middle[:, columns].astype(F32)
        ).astype(BF16)

    early, early_kind = jnp.where(outer, same, partner), jnp.where(outer, 0, 2)
    later, later_kind = jnp.where(outer, partner, same), jnp.where(outer, 2, 0)

    def pass_on(step):
        low, high = 2 * step, min(2 * step + 2, many)

        @pl.when(outer)
        def _():
            forward_down(2, partner, low, high)
            for lane in range(2):
                forward_slice(lane, low, high)

        pl.when(inner)(functools.partial(forward_down, 0, same, low, high))

    pl.when(inner)(functools.partial(forward_down, 2, partner))
    product(fs, rep)
    product(fs, 1 - rep)
    join_cores(fs, rep)
    pass_on(0)
    join_cores(fs, 1 - rep)
    product(early, rep)
    pass_on(1)
    arrived_x(early_kind, early)
    product(early, 1 - rep)
    join_cores(early, rep)
    pass_on(2)
    join_cores(early, 1 - rep)
    pass_on(3)
    join_sides(fs)
    product(later, rep)
    pl.when(inner)(functools.partial(forward_slice, 0))
    arrived_x(later_kind, later)
    product(later, 1 - rep)
    pl.when(inner)(functools.partial(forward_slice, 1, 0, many // 2))
    join_cores(later, rep)
    join_cores(later, 1 - rep)
    far_product(rep, 0)
    pl.when(inner)(functools.partial(forward_slice, 1, many // 2, many))
    for lane in range(2):
        if lane:
            far_product(rep, lane)

        @pl.loop(0, count)
        def _(unit):
            sem = (1 + 2 * lane, unit)
            landed(slice_part(far, 1 - rep, unit, lane), dx_send.at[sem], dx_recv.at[sem])

        far_product(1 - rep, lane)

        @pl.when(core == lane)
        def _():
            join_cores(far, rep)
            join_cores(far, 1 - rep)

        if lane == 0:
            join_sides(early)
    join_sides(later)
    join_sides(far)
    conclude(partner)
    conclude(jnp.where(outer, fs, far))
    conclude(jnp.where(outer, far, fs))
    conclude(same)

    for copy in sent:
        copy.wait_send()
    for q in range(3):
        pool_copy_to(q).wait_send()
    for part in range(TOKEN_PARTS):
        token_copy(part).wait_send()
    for shard in range(4):
        for slot in range(2):
            y_copy(shard, slot).wait_send()
            for half in range(2):
                core_copy(shard, half, slot).wait_send()

    @pl.loop(0, many)
    def _(j):
        for q, f in enumerate(sources):

            @pl.when(j < (count if q == 1 else other_count))
            def _():
                chunk_copy(j, q).wait_send()
                if q == 1:
                    for lane in range(2):
                        slice_copy(j, lane).wait_send()
                else:
                    down_copy(q, j).wait_send()

            @pl.when(j < count)
            def _():
                chunk_onward(j, q, f).wait_send()
                if q == 1:
                    for lane in range(2):
                        slice_onward(j, lane).wait_send()
                else:
                    down_onward(q, f, j).wait_send()


def pair_shards(
    residual,
    mixer_gain,
    pool_weight,
    pool_scale,
    channel_gain,
    gate_weight,
    up_weight,
    gate_scale,
    up_scale,
    gate_taps,
    up_taps,
    down_weight,
    down_scale,
):
    _, length, groups, local = residual.shape
    channels = local * 4
    width = groups * channels
    rows, hidden_width = gate_weight.shape
    chunks = hidden_width // 128
    chunks = chunks - chunks * 5 // 12
    half = chunks * 128
    half_columns = down_weight.shape[1] // 2
    vmem = pl.BlockSpec(memory_space=pltpu.VMEM)
    anywhere = pl.BlockSpec(memory_space=pl.ANY)
    dma = pltpu.SemaphoreType.DMA
    pairs = [
        (3, 3),
        (2, 3),
        (3,),
        (3,),
        (3,),
        (TOKEN_PARTS,),
        (2, TOKEN_PARTS),
        (4, TOKEN_PARTS),
        (chunks, 3),
        (chunks, 3),
        (4, chunks),
        (4, chunks),
        (4, 2, 2),
        (4, 2),
        (4,),
    ]
    out = pl.pallas_call(
        pair_kernel,
        out_shape=jax.ShapeDtypeStruct((length, groups * local), BF16),
        in_specs=[anywhere] * 13,
        out_specs=vmem,
        scratch_shapes=[
            pltpu.VMEM(down_scale.shape, F32),
            pltpu.VMEM(gate_taps.shape, F32),
            pltpu.VMEM(up_taps.shape, F32),
            pltpu.VMEM((2, rows, half), F32),
            pltpu.VMEM((2, rows // 2, half), F32),
            pltpu.VMEM((half, 2 * half_columns), F32),
            pltpu.VMEM((half, half_columns), F32),
            pltpu.VMEM(pool_weight.shape, F32),
            pltpu.VMEM((2, 4, length, groups * local), BF16),
            pltpu.VMEM((4, 3, groups, local), F32),
            pltpu.VMEM((4, 2) + gate_scale.shape, F32),
            pltpu.VMEM(pool_weight.shape, BF16),
            pltpu.VMEM((groups, channels, channels), BF16),
            pltpu.VMEM((chunks, 4, rows, 256), BF16),
            pltpu.VMEM((chunks, rows // 2, 256), BF16),
            pltpu.VMEM((4, 2, half, half_columns), BF16),
            pltpu.VMEM((half, half_columns), BF16),
            pltpu.VMEM((length, channels), BF16),
            pltpu.VMEM((length, channels), BF16),
            pltpu.VMEM((2 * length, width), BF16),
            pltpu.VMEM((length, groups * local), BF16),
            pltpu.VMEM((2 * length, half), BF16),
            pltpu.VMEM((4, 2, 2, length, local), F32),
            pltpu.VMEM((4, 2, 2, length, local), BF16),
            pltpu.VMEM((4, 2, 2, length, local), BF16),
            pltpu.VMEM((4, 2, length, local), BF16),
            pltpu.VMEM((4, 2, length, local), BF16),
            pltpu.VMEM((4, length, local), BF16),
            pltpu.VMEM((4, length, local), BF16),
        ]
        + [dma(shape) for shape in pairs for _ in range(2)]
        + [dma((17,))],
        compiler_params=pltpu.CompilerParams(
            collective_id=0, has_side_effects=True, vmem_limit_bytes=VMEM_BYTES
        ),
    )(
        residual.reshape(length, groups * local),
        mixer_gain,
        pool_scale,
        channel_gain,
        down_scale,
        gate_scale,
        up_scale,
        gate_taps,
        up_taps,
        pool_weight,
        gate_weight,
        up_weight,
        down_weight,
    )
    return out.reshape(1, length, groups, local)


def paired(sizes, residual, gate_weight, down_weight):
    _, length, groups, local = residual
    return (
        sizes == (2, 4, 4)
        and residual[0] == 1
        and local == 128
        and length % BAND == 0
        and groups == len(WINDOWS)
        and down_weight[1] == 4 * local
        and gate_weight[0] * 4 == groups * local * 4
        and gate_weight[1] % 1536 == 0
    )


def shards(
    sizes,
    residual,
    mixer_gain,
    pool_weight,
    pool_scale,
    channel_gain,
    gate_weight,
    up_weight,
    gate_scale,
    up_scale,
    gate_taps,
    up_taps,
    down_weight,
    down_scale,
):
    if paired(sizes, residual.shape, gate_weight.shape, down_weight.shape):
        return pair_shards(
            residual,
            mixer_gain,
            pool_weight,
            pool_scale,
            channel_gain,
            gate_weight,
            up_weight,
            gate_scale,
            up_scale,
            gate_taps,
            up_taps,
            down_weight,
            down_scale,
        )
    n_rep, n_fs, n_tp = sizes
    _, length, groups, local = residual.shape
    channels = local * n_tp
    width = groups * channels
    own_width = groups * local
    hidden_width = gate_weight.shape[1]
    vmem = pl.BlockSpec(memory_space=pltpu.VMEM)
    anywhere = pl.BlockSpec(memory_space=pl.ANY)
    dma = pltpu.SemaphoreType.DMA
    hops = max(n_fs - 1, 1)
    reps = max(n_rep - 1, 1)
    peers = max(n_tp - 1, 1)
    out = pl.pallas_call(
        functools.partial(block_kernel, sizes),
        out_shape=jax.ShapeDtypeStruct((length, own_width), BF16),
        in_specs=[vmem] * 8 + [anywhere] * 3,
        out_specs=vmem,
        scratch_shapes=[
            pltpu.VMEM((groups, channels, local), BF16),
            pltpu.VMEM((n_fs,) + gate_weight.shape, BF16),
            pltpu.VMEM((n_fs,) + up_weight.shape, BF16),
            pltpu.VMEM((n_fs,) + down_weight.shape, BF16),
            pltpu.VMEM((n_tp, length, own_width), BF16),
            pltpu.VMEM((n_tp, length, own_width), BF16),
            pltpu.VMEM((n_tp, 2, own_width), F32),
            pltpu.VMEM((n_fs, 2, gate_scale.shape[1]), F32),
            pltpu.VMEM((2, hidden_width), F32),
            pltpu.VMEM((length, channels), BF16),
            pltpu.VMEM((length, own_width), BF16),
            pltpu.VMEM((length, width), BF16),
            pltpu.VMEM((length, hidden_width), BF16),
            pltpu.VMEM((length, hidden_width), BF16),
            pltpu.VMEM((n_tp, groups, length, local), BF16),
            pltpu.VMEM((n_tp, groups, length, local), BF16),
            dma((3, SUBS, 2 * hops)),
            dma((3, SUBS, 2 * hops)),
            dma((3, SUBS, 2 * hops, reps)),
            dma((3, SUBS, 2 * hops, reps)),
            dma((hops,)),
            dma((hops,)),
            dma((hops, reps)),
            dma((hops, reps)),
            dma((hops,)),
            dma((hops,)),
            dma((3, peers)),
            dma((3, peers)),
            dma((n_fs, peers)),
            dma((n_fs, peers)),
            dma((7,)),
        ],
        compiler_params=pltpu.CompilerParams(
            collective_id=0, has_side_effects=True, vmem_limit_bytes=60 * 1024 * 1024
        ),
    )(
        residual.reshape(length, own_width),
        jnp.stack([mixer_gain.reshape(-1), channel_gain.reshape(-1)]),
        pool_scale.reshape(1, -1),
        down_scale.reshape(1, -1),
        jnp.concatenate([gate_scale, up_scale], axis=0),
        gate_taps,
        up_taps,
        pool_weight.astype(BF16),
        gate_weight.astype(BF16),
        up_weight.astype(BF16),
        down_weight.astype(BF16),
    )
    return out.reshape(1, length, groups, local)


def solution(mesh):
    placed = (
        P(("rep", "fs"), None, None, "tp"),
        P(None, "tp"),
        P(None, "fs", "tp"),
        P(None, "tp"),
        P(None, "tp"),
        P("fs", "tp"),
        P("fs", "tp"),
        P("fs", "tp"),
        P("fs", "tp"),
        P(None, "tp"),
        P(None, "tp"),
        P("tp", "fs"),
        P(None, "tp"),
    )
    sizes = tuple(mesh.shape[name] for name in ("rep", "fs", "tp"))
    return jax.shard_map(
        functools.partial(shards, sizes),
        mesh=mesh,
        in_specs=placed,
        out_specs=P(("rep", "fs"), None, None, "tp"),
        check_vma=False,
    )
```

```python
import functools

import jax
import jax.numpy as jnp
from jax import lax
from jax.experimental import pallas as pl
from jax.experimental.pallas import tpu as pltpu
from jax.sharding import PartitionSpec as P

WINDOWS = (2, 4, 8, 16)
EPSILON = 1e-05
SUBS = 2
COLUMNS = 256
VMEM_BYTES = 63 * 1024 * 1024 + 896 * 1024
F32 = jnp.float32
BF16 = jnp.bfloat16


def delayed(values, steps):
    rows = lax.broadcasted_iota(jnp.int32, values.shape, 0)
    return jnp.where(rows >= steps, pltpu.roll(values, steps, 0), 0.0)


def causal_taps(values, taps):
    return taps[2:3] * values + taps[1:2] * delayed(values, 1) + taps[0:1] * delayed(values, 2)


def block_kernel(
    sizes,
    residual,
    gains,
    pool_scale,
    down_scale,
    scale_pair,
    gate_taps,
    up_taps,
    pool_own,
    gate_own,
    up_own,
    down_own,
    out,
    pool_full,
    gate_full,
    up_full,
    down_full,
    gathered,
    middle_all,
    gains_all,
    scales_all,
    scale_row,
    pooled,
    middle,
    inputs,
    gate_pre,
    hidden,
    partials,
    arrived,
    ring_send,
    ring_recv,
    rep_send,
    rep_recv,
    pool_send,
    pool_recv,
    pool_rep_send,
    pool_rep_recv,
    scale_send,
    scale_recv,
    tp_send,
    tp_recv,
    part_send,
    part_recv,
    local_sem,
):
    n_rep, n_fs, n_tp = sizes
    rep, fs, tp = (lax.axis_index(name) for name in ("rep", "fs", "tp"))
    length = residual.shape[0]
    groups = pool_full.shape[0]
    channels = pool_full.shape[1]
    local = residual.shape[1] // groups
    width = groups * channels

    def other(axis, offset):
        me, count = {"rep": (rep, n_rep), "fs": (fs, n_fs), "tp": (tp, n_tp)}[axis]
        return lax.rem(me + offset, count)

    def remote(src, dst, send, recv, axis, offset):
        return pltpu.make_async_remote_copy(
            src_ref=src,
            dst_ref=dst,
            send_sem=send,
            recv_sem=recv,
            device_id={axis: other(axis, offset)},
            device_id_type=pl.DeviceIdType.MESH,
        )

    barrier = pltpu.get_barrier_semaphore()
    for axis, count in (("rep", n_rep), ("fs", n_fs), ("tp", n_tp)):
        for offset in range(1, count):
            pl.semaphore_signal(
                barrier,
                inc=1,
                device_id={axis: other(axis, offset)},
                device_id_type=pl.DeviceIdType.MESH,
            )
    pl.semaphore_wait(barrier, n_rep + n_fs + n_tp - 3)

    sent = []

    def start(copy, valid=None):
        sent.append((copy, valid))
        if valid is None:
            copy.start()
        else:
            pl.when(valid)(copy.start)

    weights = ((gate_own, gate_full), (up_own, up_full), (down_own, down_full))

    def piece(w, shard, half, sub, own=False):
        rows = weights[w][0].shape[0] // (n_rep * SUBS)
        part = pl.ds(pl.multiple_of((half * SUBS + sub) * rows, rows), rows)
        return weights[w][0].at[part] if own else weights[w][1].at[shard, part]

    def shard_sent(step, way):
        shard = fs + step if way else fs - step
        return jnp.clip(shard, 0, n_fs - 1), (shard <= n_fs - 1 if way else shard >= 0)

    def line(w, sub, step):
        for way in range(2):
            shard, valid = shard_sent(step, way)
            start(
                remote(
                    piece(w, shard, rep, sub, own=step == 0),
                    piece(w, shard, rep, sub),
                    ring_send.at[w, sub, 2 * step + way],
                    ring_recv.at[w, sub, 2 * step + way],
                    "fs",
                    n_fs - 1 if way else 1,
                ),
                valid & (fs > 0 if way else fs < n_fs - 1),
            )

    def serve(w, sub, step):
        for way in range(2):
            shard, valid = shard_sent(step + 1, way)
            mine = piece(w, shard, rep, sub)
            sems = (w, sub, 2 * step + way)
            pl.when(valid)(
                remote(
                    mine, mine, ring_send.at[sems], ring_recv.at[sems], "fs", 1
                ).wait_recv
            )
            if step < n_fs - 2:
                onward = (w, sub, 2 * step + 2 + way)
                start(
                    remote(
                        mine,
                        mine,
                        ring_send.at[onward],
                        ring_recv.at[onward],
                        "fs",
                        n_fs - 1 if way else 1,
                    ),
                    valid & (fs > 0 if way else fs < n_fs - 1),
                )
            for d in range(1, n_rep):
                start(
                    remote(
                        mine,
                        mine,
                        rep_send.at[sems + (d - 1,)],
                        rep_recv.at[sems + (d - 1,)],
                        "rep",
                        d,
                    ),
                    valid,
                )

    def settle(w, step, ways=(0, 1)):
        for way in ways:
            shard, valid = shard_sent(step + 1, way)

            @pl.when(valid)
            def _():
                for sub in range(SUBS):
                    for d in range(1, n_rep):
                        got = piece(w, shard, other("rep", n_rep - d), sub)
                        sems = (w, sub, 2 * step + way, d - 1)
                        remote(
                            got, got, rep_send.at[sems], rep_recv.at[sems], "rep", d
                        ).wait_recv()

    def local_copy(src, dst, idx):
        copy = pltpu.make_async_copy(src, dst, local_sem.at[idx])
        copy.start()
        return copy

    own_copies = [
        local_copy(residual, gathered.at[tp], 0),
        local_copy(gains, gains_all.at[tp], 1),
        local_copy(scale_pair, scales_all.at[fs], 2),
        local_copy(gate_own, gate_full.at[fs], 3),
        local_copy(up_own, up_full.at[fs], 4),
        local_copy(down_own, down_full.at[fs], 5),
    ]

    pool_rows = pool_own.shape[1]
    rep_groups = groups // n_rep

    def pool_part(shard, half):
        return pool_full.at[
            pl.ds(half * rep_groups, rep_groups),
            pl.ds(pl.multiple_of(shard * pool_rows, pool_rows), pool_rows),
        ]

    pool_copy = local_copy(
        pool_own, pool_full.at[:, pl.ds(pl.multiple_of(fs * pool_rows, pool_rows), pool_rows)], 6
    )

    for d in range(1, n_fs):
        start(
            remote(
                pool_own.at[pl.ds(rep * rep_groups, rep_groups)],
                pool_part(fs, rep),
                pool_send.at[d - 1],
                pool_recv.at[d - 1],
                "fs",
                d,
            )
        )
    for w in (0, 1):
        for sub in range(SUBS):
            if n_fs > 1:
                line(w, sub, 0)
    for d in range(1, n_tp):
        start(remote(gains, gains_all.at[tp], tp_send.at[0, d - 1], tp_recv.at[0, d - 1], "tp", d))
    for d in range(1, n_tp):
        start(
            remote(residual, gathered.at[tp], tp_send.at[1, d - 1], tp_recv.at[1, d - 1], "tp", d)
        )
    for d in range(1, n_fs):
        start(
            remote(
                scale_pair, scales_all.at[fs], scale_send.at[d - 1], scale_recv.at[d - 1], "fs", d
            )
        )

    for d in range(1, n_fs):
        shard = other("fs", n_fs - d)
        mine = pool_part(shard, rep)
        remote(mine, mine, pool_send.at[d - 1], pool_recv.at[d - 1], "fs", d).wait_recv()
        for e in range(1, n_rep):
            start(
                remote(
                    mine,
                    mine,
                    pool_rep_send.at[d - 1, e - 1],
                    pool_rep_recv.at[d - 1, e - 1],
                    "rep",
                    e,
                )
            )
    for d in range(1, n_fs):
        shard = other("fs", n_fs - d)
        for e in range(1, n_rep):
            got = pool_part(shard, other("rep", n_rep - e))
            remote(
                got,
                got,
                pool_rep_send.at[d - 1, e - 1],
                pool_rep_recv.at[d - 1, e - 1],
                "rep",
                e,
            ).wait_recv()
    pool_copy.wait()
    for copy in own_copies:
        copy.wait()

    def tp_arrivals(idx, buffer):
        for d in range(1, n_tp):
            got = buffer.at[other("tp", n_tp - d)]
            remote(got, got, tp_send.at[idx, d - 1], tp_recv.at[idx, d - 1], "tp", d).wait_recv()

    for sub in range(SUBS):
        serve(0, sub, 0)
    tp_arrivals(0, gains_all)
    tp_arrivals(1, gathered)
    for sub in range(SUBS):
        serve(1, sub, 0)

    def mean_square_root(buffer):
        total = jnp.zeros((length, 1), F32)
        for t in range(n_tp):
            values = buffer[t].astype(F32)
            total = total + jnp.sum(values * values, axis=1, keepdims=True)
        return lax.rsqrt(total / width + EPSILON)

    factor = mean_square_root(gathered)
    positions = lax.broadcasted_iota(jnp.int32, (length, 1), 0).astype(F32) + 1.0
    for g in range(groups):
        part = slice(g * local, (g + 1) * local)
        share = 1.0 / jnp.minimum(positions, float(WINDOWS[g]))
        for t in range(n_tp):
            values = gathered[t, :, part].astype(F32)
            normed = (values * factor * gains_all[t, 0:1, part]).astype(BF16).astype(F32)
            totals = normed
            reach = 1
            while reach < WINDOWS[g]:
                totals = totals + delayed(totals, reach)
                reach = reach * 2
            pooled[:, t * local : (t + 1) * local] = (totals * share - normed).astype(BF16)
        mixed = jnp.dot(pooled[...], pool_full[g], preferred_element_type=F32)
        middle[:, part] = (
            mixed * pool_scale[:, part] + residual[:, part].astype(F32)
        ).astype(BF16)

    middle_copy = local_copy(middle, middle_all.at[tp], 0)
    for d in range(1, n_tp):
        start(
            remote(middle, middle_all.at[tp], tp_send.at[2, d - 1], tp_recv.at[2, d - 1], "tp", d)
        )
    for step in range(1, n_fs - 1):
        for w in (0, 1):
            if step == n_fs - 2 and n_fs > 2:
                break
            for sub in range(SUBS):
                serve(w, sub, step)
    for sub in range(SUBS):
        if n_fs > 1:
            line(2, sub, 0)
    for d in range(1, n_fs):
        got = scales_all.at[other("fs", n_fs - d)]
        remote(got, got, scale_send.at[d - 1], scale_recv.at[d - 1], "fs", d).wait_recv()
    shard_columns = scale_pair.shape[1]
    for f in range(n_fs):
        scale_row[:, f * shard_columns : (f + 1) * shard_columns] = scales_all[f]

    middle_copy.wait()
    tp_arrivals(2, middle_all)
    factor = mean_square_root(middle_all)
    for t in range(n_tp):
        for g in range(groups):
            part = slice(g * local, (g + 1) * local)
            start_column = g * channels + t * local
            inputs[:, start_column : start_column + local] = (
                middle_all[t, :, part].astype(F32) * factor * gains_all[t, 1:2, part]
            ).astype(BF16)

    def finish(w):
        if n_fs > 2:
            for sub in range(SUBS):
                serve(w, sub, n_fs - 2)
        for step in range(n_fs - 1):
            settle(w, step)

    def product(full, columns, row):
        block = full[:, :, columns].reshape(width, COLUMNS)
        made = jnp.dot(inputs[...], block, preferred_element_type=F32)
        return (made * scale_row[row : row + 1, columns]).astype(BF16)

    chunks = gate_full.shape[2] // COLUMNS

    finish(0)

    @pl.loop(0, chunks)
    def _(j):
        columns = pl.ds(pl.multiple_of(j * COLUMNS, COLUMNS), COLUMNS)
        gate_pre[:, columns] = product(gate_full, columns, 0)

    finish(1)
    for sub in range(SUBS):
        if n_fs > 1:
            serve(2, sub, 0)

    @pl.loop(0, chunks)
    def _(j):
        columns = pl.ds(pl.multiple_of(j * COLUMNS, COLUMNS), COLUMNS)
        up_values = product(up_full, columns, 1).astype(F32)
        conv_gate = causal_taps(gate_pre[:, columns].astype(F32), gate_taps[:, columns])
        conv_up = causal_taps(up_values, up_taps[:, columns])
        silu = conv_gate / (1.0 + jnp.exp(-conv_gate))
        hidden[:, columns] = (silu * conv_up).astype(BF16)

    shard_width = down_own.shape[1]

    def to_peers(idx, src, dst):
        for d in range(1, n_tp):
            start(
                remote(
                    src(other("tp", d)),
                    dst(tp),
                    part_send.at[idx, d - 1],
                    part_recv.at[idx, d - 1],
                    "tp",
                    d,
                )
            )

    def from_peers(idx, dst):
        for d in range(1, n_tp):
            got = dst(other("tp", n_tp - d))
            remote(
                got, got, part_send.at[idx, d - 1], part_recv.at[idx, d - 1], "tp", d
            ).wait_recv()

    def conclude(g, columns):
        total = partials[tp, g].astype(F32)
        for d in range(1, n_tp):
            total = total + arrived[other("tp", d), g].astype(F32)
        out[:, columns] = (
            total * down_scale[:, columns] + middle[:, columns].astype(F32)
        ).astype(BF16)

    if shard_width == channels and local % 128 == 0:
        def share(shard):
            made = jnp.dot(hidden[...], down_full[shard], preferred_element_type=F32)
            for t in range(n_tp):
                partials[t, shard] = made[:, t * local : (t + 1) * local].astype(BF16)
            for d in range(1, n_tp):
                peer = other("tp", d)
                remote(
                    partials.at[peer, shard],
                    arrived.at[tp, shard],
                    part_send.at[shard, d - 1],
                    part_recv.at[shard, d - 1],
                    "tp",
                    d,
                ).start()

        share(fs)
        for step in range(n_fs - 1):
            if step >= 1:
                for sub in range(SUBS):
                    serve(2, sub, step)
            for way in range(2):
                settle(2, step, (way,))
                shard, valid = shard_sent(step + 1, way)
                pl.when(valid)(functools.partial(share, shard))
        for shard in range(n_fs):
            from_peers(shard, lambda t: arrived.at[t, shard])
            conclude(shard, slice(shard * local, (shard + 1) * local))
            for d in range(1, n_tp):
                mine = partials.at[other("tp", d), shard]
                remote(
                    mine, mine, part_send.at[shard, d - 1], part_recv.at[shard, d - 1], "tp", d
                ).wait_send()
    else:
        for step in range(n_fs - 1):
            if step >= 1:
                for sub in range(SUBS):
                    serve(2, sub, step)
            settle(2, step)
        for f in range(n_fs):
            made = jnp.dot(hidden[...], down_full[f], preferred_element_type=F32).astype(BF16)
            span = min(local, shard_width)
            for at in range(0, shard_width, span):
                g, channel = divmod(f * shard_width + at, channels)
                t, low = divmod(channel, local)
                partials[t, g, :, low : low + span] = made[:, at : at + span]
        to_peers(0, lambda t: partials.at[t], lambda t: arrived.at[t])
        from_peers(0, lambda t: arrived.at[t])
        for g in range(groups):
            conclude(g, slice(g * local, (g + 1) * local))

    for copy, valid in sent:
        if valid is None:
            copy.wait_send()
        else:
            pl.when(valid)(copy.wait_send)


BAND = 256
FEW = 5
TOKEN_PARTS = 2


def pair_kernel(
    residual,
    mixer_gain,
    pool_scale,
    channel_gain,
    down_scale_own,
    gate_scale,
    up_scale,
    gate_taps_own,
    up_taps_own,
    pool_own,
    gate_own,
    up_own,
    down_own,
    out,
    down_scale,
    gate_taps,
    up_taps,
    stage_own,
    stage_other,
    stage_down,
    stage_down_other,
    stage_pool,
    tokens,
    small_all,
    scales_all,
    pool_near,
    pool_full,
    weights,
    other,
    down_full,
    down_other,
    normed,
    pooled,
    inputs,
    middle,
    hidden,
    keep,
    give,
    got,
    y_out,
    y_in,
    z_out,
    z_in,
    small_send,
    small_recv,
    scale_send,
    scale_recv,
    pz_send,
    pz_recv,
    px_send,
    px_recv,
    pt_send,
    pt_recv,
    rz_send,
    rz_recv,
    ry_send,
    ry_recv,
    rs_send,
    rs_recv,
    gz_send,
    gz_recv,
    gx_send,
    gx_recv,
    dz_send,
    dz_recv,
    dx_send,
    dx_recv,
    core_send,
    core_recv,
    y_send,
    y_recv,
    z_send,
    z_recv,
    local_sem,
):
    rep, fs, tp = (lax.axis_index(name) for name in ("rep", "fs", "tp"))
    length = residual.shape[0]
    groups, pool_rows, local = pool_own.shape
    channels = pool_full.shape[1]
    width = groups * channels
    rows = gate_own.shape[0]
    half_rows = rows // 2
    chunks = gate_own.shape[1] // 128
    few = chunks * FEW // 12
    many = chunks - few
    half_columns = down_own.shape[1] // 2
    member = lax.rem(fs, 2)
    side = tp // 2
    core = lax.rem(tp, 2)
    sibling = {"tp": tp + 1 - 2 * core}
    across = {"tp": lax.rem(tp + 2, 4)}
    diagonal = {"tp": 3 - tp}
    mirror = {"rep": 1 - rep}
    same, far, partner = lax.rem(fs + 2, 4), 3 - fs, fs + 1 - 2 * member
    sources = (same, far, partner)
    outer = (fs == 0) | (fs == 3)
    inner = jnp.logical_not(outer)
    count = jnp.where(outer, few, many)
    other_count = chunks - count
    begin = jnp.where(outer, many, 0)
    skip = jnp.where(outer, many - few, 0)
    other_skip = many - few - skip

    sent = []

    def remote(src, dst, send, recv, device):
        return pltpu.make_async_remote_copy(
            src_ref=src,
            dst_ref=dst,
            send_sem=send,
            recv_sem=recv,
            device_id=device,
            device_id_type=pl.DeviceIdType.MESH,
        )

    def start(*parts):
        copy = remote(*parts)
        sent.append(copy)
        copy.start()

    def aligned(at, size):
        return pl.ds(pl.multiple_of(at, size), size)

    def local_copy(src, dst, idx):
        copy = pltpu.make_async_copy(src, dst, local_sem.at[idx])
        copy.start()
        return copy

    barrier = pltpu.get_barrier_semaphore()
    peers = (mirror, sibling, across, diagonal) + tuple({"fs": f} for f in sources)
    for device in peers:
        pl.semaphore_signal(
            barrier, inc=1, device_id=device, device_id_type=pl.DeviceIdType.MESH
        )
    mine = pl.ds(pl.multiple_of(jnp.where(outer, few, 0) * 128, 128), many * 128)
    theirs = pl.ds(pl.multiple_of(jnp.where(outer, 0, few) * 128, 128), many * 128)
    rep_rows = aligned(rep * half_rows, half_rows)
    rep_columns = aligned(rep * half_columns, half_columns)
    load_pool = local_copy(pool_own, stage_pool, 1)
    load_tokens = local_copy(residual, tokens.at[0, tp], 0)
    loads = [
        local_copy(gate_own.at[:, mine], stage_own.at[0], 2),
        local_copy(up_own.at[:, mine], stage_own.at[1], 3),
        local_copy(gate_own.at[rep_rows, theirs], stage_other.at[0], 4),
        local_copy(up_own.at[rep_rows, theirs], stage_other.at[1], 5),
    ]
    load_down = [
        local_copy(down_own.at[mine], stage_down, 6),
        local_copy(down_own.at[theirs, rep_columns], stage_down_other, 7),
    ]

    small_loads = [
        local_copy(src, dst, 9 + at)
        for at, (src, dst) in enumerate(
            (
                (mixer_gain, small_all.at[tp, 0]),
                (pool_scale, small_all.at[tp, 1]),
                (channel_gain, small_all.at[tp, 2]),
                (gate_scale, scales_all.at[fs, 0]),
                (up_scale, scales_all.at[fs, 1]),
                (down_scale_own, down_scale),
                (gate_taps_own, gate_taps),
                (up_taps_own, up_taps),
            )
        )
    ]
    load_pool.wait()
    pool_near[...] = stage_pool[...].astype(BF16)
    load_tokens.wait()
    pl.semaphore_wait(barrier, len(peers))

    def token_part(slot, t, part):
        span = length // TOKEN_PARTS
        return tokens.at[slot, t, pl.ds(part * span, span)]

    def pool_part(shard, half):
        span = groups // 2
        return pool_full.at[
            pl.ds(half * span, span),
            aligned(shard * pool_rows, pool_rows),
            aligned(tp * local, local),
        ]

    def pool_copy_to(q):
        return remote(
            pool_near.at[pl.ds(rep * (groups // 2), groups // 2)],
            pool_part(fs, rep),
            pz_send.at[q],
            pz_recv.at[q],
            {"fs": sources[q]},
        )

    for q in (2, 1, 0):
        pool_copy_to(q).start()
    for part in range(TOKEN_PARTS):
        piece = token_part(0, tp, part)
        start(piece, piece, ry_send.at[0, part], ry_recv.at[0, part], across)
        start(piece, piece, rs_send.at[0, part], rs_recv.at[0, part], sibling)
    for at, values in enumerate((mixer_gain, pool_scale, channel_gain)):
        for q, device in enumerate((sibling, across, diagonal)):
            start(values, small_all.at[tp, at], small_send.at[at, q], small_recv.at[at, q], device)
    for at, values in enumerate((gate_scale, up_scale)):
        for q, f in enumerate(sources):
            start(
                values, scales_all.at[fs, at], scale_send.at[at, q], scale_recv.at[at, q], {"fs": f}
            )
    pool_copy = local_copy(
        pool_near,
        pool_full.at[:, aligned(fs * pool_rows, pool_rows), aligned(tp * local, local)],
        8,
    )

    late, late_kind = jnp.where(outer, far, same), jnp.where(outer, 1, 0)

    def chunk_target(j, shard, half):
        return weights.at[j, shard, aligned(half * half_rows, half_rows)]

    def chunk_copy(j, q):
        target = chunk_target(j, fs, rep)
        source = target if q == 1 else other.at[j]
        return remote(source, target, gz_send.at[j, q], gz_recv.at[j, q], {"fs": sources[q]})

    def down_part(shard, half, unit):
        return down_full.at[shard, half, aligned(unit * 128, 128)]

    def down_copy(q, unit):
        target = down_part(fs, rep, unit)
        source = down_other.at[aligned(unit * 128, 128)]
        return remote(source, target, dz_send.at[q, unit], dz_recv.at[q, unit], {"fs": sources[q]})

    def slice_part(shard, half, unit, lane):
        return down_full.at[
            shard, half, aligned(unit * 128, 128), pl.ds(lane * local, local)
        ]

    def slice_copy(unit, lane):
        piece = slice_part(fs, rep, unit, lane)
        return remote(
            piece, piece, dz_send.at[1 + 2 * lane, unit], dz_recv.at[1 + 2 * lane, unit], {"fs": far}
        )

    def token_copy(part):
        return remote(
            token_part(0, tp, part),
            token_part(1, tp, part),
            rz_send.at[part],
            rz_recv.at[part],
            {"fs": partner},
        )

    for part in range(TOKEN_PARTS):
        token_copy(part).start()
    for load in loads + small_loads:
        load.wait()

    @pl.loop(0, many)
    def _(j):
        @pl.when(j < other_count)
        def _():
            columns = aligned((other_skip + j) * 128, 128)
            for at in range(2):
                lanes = slice(at * 128, (at + 1) * 128)
                other[j, :, lanes] = stage_other[at, :, columns].astype(BF16)
            chunk_copy(j, 2).start()

        @pl.when(j < count)
        def _():
            columns = aligned((skip + j) * 128, 128)
            for at in range(2):
                lanes = slice(at * 128, (at + 1) * 128)
                weights[j, fs, :, lanes] = stage_own[at, :, columns].astype(BF16)
            pl.when(inner)(chunk_copy(j, 1).start)

    @pl.when(inner)
    def _():
        @pl.loop(0, other_count)
        def _(j):
            chunk_copy(j, 0).start()

    for load in load_down:
        load.wait()
    if many > few:
        hidden[:, few * 128 :] = jnp.zeros((2 * length, (many - few) * 128), BF16)

        @pl.when(outer)
        def _():
            down_full[:, :, few * 128 :] = jnp.zeros(
                (4, 2, (many - few) * 128, half_columns), BF16
            )

    @pl.loop(0, count)
    def _(j):
        here = aligned(j * 128, 128)
        there = aligned((skip + j) * 128, 128)
        for half in range(2):
            down_full[fs, half, here] = stage_down[
                there, half * half_columns : (half + 1) * half_columns
            ].astype(BF16)

    @pl.loop(0, other_count)
    def _(j):
        there = aligned((other_skip + j) * 128, 128)
        down_other[aligned(j * 128, 128)] = stage_down_other[there].astype(BF16)

    @pl.when(outer)
    def _():
        for unit in range(2):
            down_copy(2, unit).start()

    @pl.when(inner)
    def _():
        @pl.loop(0, other_count)
        def _(unit):
            down_copy(2, unit).start()

        @pl.loop(0, other_count)
        def _(unit):
            down_copy(0, unit).start()

        for lane in range(2):

            @pl.loop(0, count)
            def _(unit):
                slice_copy(unit, lane).start()

    def landed(ref, send, recv):
        remote(ref, ref, send, recv, mirror).wait_recv()

    def chunk_onward(j, q, shard):
        piece = chunk_target(j, shard, rep)
        return remote(piece, piece, gx_send.at[j, q], gx_recv.at[j, q], mirror)

    def forward_chunk(j, q, shard):
        piece = chunk_target(j, shard, rep)
        landed(piece, gz_send.at[j, q], gz_recv.at[j, q])
        chunk_onward(j, q, shard).start()

    def down_onward(q, shard, unit):
        piece = down_part(shard, rep, unit)
        return remote(piece, piece, dx_send.at[q, unit], dx_recv.at[q, unit], mirror)

    def slice_onward(unit, lane):
        piece = slice_part(far, rep, unit, lane)
        sem = (1 + 2 * lane, unit)
        return remote(piece, piece, dx_send.at[sem], dx_recv.at[sem], mirror)

    def forward_slice(lane, low=0, high=many):
        @pl.loop(low, jnp.minimum(count, high))
        def _(unit):
            sem = (1 + 2 * lane, unit)
            landed(slice_part(far, rep, unit, lane), dz_send.at[sem], dz_recv.at[sem])
            slice_onward(unit, lane).start()

    def forward_down(q, shard, low=0, high=many):
        @pl.loop(low, jnp.minimum(count, high))
        def _(unit):
            landed(down_part(shard, rep, unit), dz_send.at[q, unit], dz_recv.at[q, unit])
            down_onward(q, shard, unit).start()

    for q, f in ((2, partner), (1, far), (0, same)):
        piece = pool_part(f, rep)
        landed(piece, pz_send.at[q], pz_recv.at[q])
        start(piece, piece, px_send.at[q], px_recv.at[q], mirror)
    for q, f in enumerate(sources):
        landed(pool_part(f, 1 - rep), px_send.at[q], px_recv.at[q])
    pool_copy.wait()

    def pool_slab(t):
        return pool_full.at[:, :, aligned(t * local, local)]

    slab = pool_slab(tp)
    start(slab, slab, pt_send.at[1], pt_recv.at[1], across)
    start(slab, slab, pt_send.at[0], pt_recv.at[0], sibling)

    t_sibling, t_across, t_diagonal = sibling["tp"], across["tp"], diagonal["tp"]

    def own_onward(part):
        piece = token_part(0, t_across, part)
        landed(piece, ry_send.at[0, part], ry_recv.at[0, part])
        start(piece, piece, rs_send.at[1, part], rs_recv.at[1, part], sibling)

    def partner_onward(part):
        piece = token_part(1, tp, part)
        landed(piece, rz_send.at[part], rz_recv.at[part])
        start(piece, piece, ry_send.at[1, part], ry_recv.at[1, part], across)
        start(piece, piece, rs_send.at[2, part], rs_recv.at[2, part], sibling)

    def forward_chunks(kind, shard, low, high):
        for j in range(low, high):
            forward_chunk(j, kind, shard)

    third = many // 3
    own_onward(0)
    pl.when(inner)(functools.partial(forward_chunks, 1, far, 0, third))
    partner_onward(0)
    own_onward(1)
    pl.when(inner)(functools.partial(forward_chunks, 1, far, third, many - third))
    partner_onward(1)
    pl.when(inner)(functools.partial(forward_chunks, 1, far, many - third, many))
    second_kind, second = jnp.where(outer, 0, 2), jnp.where(outer, same, partner)
    forward_chunks(second_kind, second, 0, few - 3)
    slab = pool_slab(t_across)
    landed(slab, pt_send.at[1], pt_recv.at[1])
    start(slab, slab, pt_send.at[2], pt_recv.at[2], sibling)
    forward_chunks(second_kind, second, few - 3, few - 2)

    for part in range(TOKEN_PARTS):
        landed(token_part(0, t_sibling, part), rs_send.at[0, part], rs_recv.at[0, part])
        landed(token_part(0, t_diagonal, part), rs_send.at[1, part], rs_recv.at[1, part])
    for at in range(3):
        for q, t in enumerate((t_sibling, t_across, t_diagonal)):
            landed(small_all.at[t, at], small_send.at[at, q], small_recv.at[at, q])
    landed(pool_slab(t_sibling), pt_send.at[0], pt_recv.at[0])
    landed(pool_slab(t_diagonal), pt_send.at[2], pt_recv.at[2])

    positions = lax.broadcasted_iota(jnp.int32, (BAND, 1), 0).astype(F32) + 1.0
    distance = (
        lax.broadcasted_iota(jnp.int32, (BAND, 2 * BAND), 0)
        + BAND
        - lax.broadcasted_iota(jnp.int32, (BAND, 2 * BAND), 1)
    )

    def mix(slot, between):
        span = slice(slot * length, (slot + 1) * length)
        square = jnp.zeros((length, local), F32)
        for t in range(4):
            for g in range(groups):
                values = tokens[slot, t, :, g * local : (g + 1) * local].astype(F32)
                square = square + values * values
        factor = lax.rsqrt(jnp.sum(square, axis=1, keepdims=True) / width + EPSILON)
        square = jnp.zeros((length, local), F32)
        for g in range(groups):
            if g == groups // 2:
                between()
            part = slice(g * local, (g + 1) * local)
            for t in range(4):
                values = tokens[slot, t, :, part].astype(F32)
                normed[:, t * local : (t + 1) * local] = (
                    values * factor * small_all[t, 0, g : g + 1]
                ).astype(BF16)
            band = jnp.where((distance >= 0) & (distance < WINDOWS[g]), 1.0, 0.0).astype(BF16)
            for b in range(length // BAND):
                here = slice(b * BAND, (b + 1) * BAND)
                if b == 0:
                    totals = jnp.dot(band[:, BAND:], normed[here], preferred_element_type=F32)
                    totals = totals / jnp.minimum(positions, float(WINDOWS[g]))
                else:
                    totals = jnp.dot(
                        band,
                        normed[(b - 1) * BAND : (b + 1) * BAND],
                        preferred_element_type=F32,
                    ) * (1.0 / WINDOWS[g])
                pooled[here] = (totals - normed[here].astype(F32)).astype(BF16)
            mixed = jnp.dot(pooled[...], pool_full[g], preferred_element_type=F32)
            for t in range(4):
                made = (
                    mixed[:, t * local : (t + 1) * local] * small_all[t, 1, g : g + 1]
                    + tokens[slot, t, :, part].astype(F32)
                ).astype(BF16)
                inputs[span, g * channels + t * local : g * channels + (t + 1) * local] = made
                values = made.astype(F32)
                square = square + values * values
        factor = lax.rsqrt(jnp.sum(square, axis=1, keepdims=True) / width + EPSILON)
        if slot == 0:
            for g in range(groups):
                middle[:, g * local : (g + 1) * local] = inputs[
                    span, aligned(g * channels + tp * local, local)
                ]
        for g in range(groups):
            for t in range(4):
                columns = slice(g * channels + t * local, g * channels + (t + 1) * local)
                inputs[span, columns] = (
                    inputs[span, columns].astype(F32) * factor * small_all[t, 2, g : g + 1]
                ).astype(BF16)

    def cross():
        forward_chunks(second_kind, second, few - 2, few)

        @pl.when(outer)
        def _():
            @pl.loop(0, many)
            def _(j):
                pl.when(j < few)(chunk_copy(j, 1).start)
                chunk_copy(j, 0).start()

            @pl.loop(2, many)
            def _(unit):
                down_copy(2, unit).start()

    mix(0, cross)

    @pl.when(inner)
    def _():
        forward_chunks(2, partner, few, many)
        forward_down(2, partner, 0, 2)

    for part in range(TOKEN_PARTS):
        piece = token_part(1, t_across, part)
        landed(piece, ry_send.at[1, part], ry_recv.at[1, part])
        start(piece, piece, rs_send.at[3, part], rs_recv.at[3, part], sibling)
    pl.when(outer)(functools.partial(forward_chunk, 0, 1, far))
    for part in range(TOKEN_PARTS):
        landed(token_part(1, t_sibling, part), rs_send.at[2, part], rs_recv.at[2, part])
        landed(token_part(1, t_diagonal, part), rs_send.at[3, part], rs_recv.at[3, part])

    def forward_late(j):
        forward_chunk(j, late_kind, late)
        pl.when(outer)(functools.partial(forward_chunk, j, 2, partner))

    forward_chunk(0, jnp.where(outer, 2, 0), jnp.where(outer, partner, same))
    mix(1, functools.partial(forward_late, 1))
    for at in range(2):
        for q, f in enumerate(sources):
            landed(scales_all.at[f, at], scale_send.at[at, q], scale_recv.at[at, q])

    thirds = scales_all.shape[3] // 128

    def expand(j):
        for q, f in enumerate(sources):
            landed(chunk_target(j, f, 1 - rep), gx_send.at[j, q], gx_recv.at[j, q])
        unit = begin + j
        here = aligned(unit * 128, 128)
        scale_at = aligned(lax.rem(unit, thirds) * 128, 128)
        taps = [
            table[:, here] * scales_all[unit // thirds, at, :, scale_at]
            for at, table in enumerate((gate_taps, up_taps))
        ]
        block = weights[j].reshape(width, 256)
        for slot in range(2):
            span = slice(slot * length, (slot + 1) * length)
            made = jnp.dot(inputs[span], block, preferred_element_type=F32)
            conv_gate = causal_taps(made[:, :128], taps[0])
            conv_up = causal_taps(made[:, 128:], taps[1])
            silu = conv_gate / (1.0 + jnp.exp(-conv_gate))
            hidden[span, aligned(j * 128, 128)] = (silu * conv_up).astype(BF16)

    @pl.loop(0, count)
    def _(j):
        expand(j)

        @pl.when(j < count - 2)
        def _():
            forward_late(j + 2)

        @pl.when(inner & (j == many - 3))
        def _():
            forward_down(2, partner, 2, 4)

        @pl.when(inner & (j == many - 2))
        def _():
            forward_down(2, partner, 4, 6)

        @pl.when(outer & (j == few - 2))
        def _():
            forward_down(0, same)

            @pl.loop(0, many)
            def _(unit):
                down_copy(0, unit).start()

            for lane in range(2):

                @pl.loop(0, few)
                def _(unit):
                    slice_copy(unit, lane).start()

    def core_copy(shard, half, slot):
        return remote(
            give.at[shard, half, slot],
            got.at[shard, half, slot],
            core_send.at[shard, half, slot],
            core_recv.at[shard, half, slot],
            sibling,
        )

    def product(shard, half):
        made = jnp.dot(hidden[...], down_full[shard, half], preferred_element_type=F32)
        for slot in (1, 0):
            span = slice(slot * length, (slot + 1) * length)
            low, high = made[span, :local], made[span, local:]
            keep[shard, half, slot] = jnp.where(core == 0, low, high)
            give[shard, half, slot] = jnp.where(core == 0, high, low).astype(BF16)
        for slot in (1, 0):
            core_copy(shard, half, slot).start()

    def product_by_slot(shard, half):
        for slot in (1, 0):
            span = slice(slot * length, (slot + 1) * length)
            made = jnp.dot(hidden[span], down_full[shard, half], preferred_element_type=F32)
            low, high = made[:, :local], made[:, local:]
            keep[shard, half, slot] = jnp.where(core == 0, low, high)
            give[shard, half, slot] = jnp.where(core == 0, high, low).astype(BF16)
            core_copy(shard, half, slot).start()

    def y_part(buffer, shard, which):
        if which == 0:
            return buffer.at[shard, 0]
        return buffer.at[shard, 1, pl.ds((which - 1) * (length // 2), length // 2)]

    def y_copy(shard, which):
        return remote(
            y_part(y_out, shard, which),
            y_part(y_in, shard, which),
            y_send.at[shard, which],
            y_recv.at[shard, which],
            across,
        )

    def z_copy(shard, part):
        rows = pl.ds(part * (length // 2), length // 2)
        return remote(
            z_out.at[shard, rows],
            z_in.at[shard, rows],
            z_send.at[shard, part],
            z_recv.at[shard, part],
            {"fs": partner},
        )

    def arrived_x(q, shard):
        @pl.loop(0, count)
        def _(unit):
            landed(down_part(shard, 1 - rep, unit), dx_send.at[q, unit], dx_recv.at[q, unit])

    def join_cores(shard, half):
        for slot in (1, 0):
            core_copy(shard, half, slot).wait_recv()
            total = keep[shard, half, slot] + got[shard, half, slot].astype(F32)

            @pl.when(half == side)
            def _():
                keep[shard, half, slot] = total

            @pl.when(half != side)
            def _():
                y_out[shard, slot] = total.astype(BF16)
                for which in (1, 2) if slot else (0,):
                    y_copy(shard, which).start()

    def join_sides(shard):
        for part in range(2):
            rows = slice(part * (length // 2), (part + 1) * (length // 2))
            y_copy(shard, 1 + part).wait_recv()
            total = keep[shard, side, 1, rows] + y_in[shard, 1, rows].astype(F32)
            z_out[shard, rows] = total.astype(BF16)
            z_copy(shard, part).start()

    def conclude(shard):
        y_copy(shard, 0).wait_recv()
        total = keep[shard, side, 0] + y_in[shard, 0].astype(F32)
        for part in range(2):
            z_copy(shard, part).wait_recv()
        columns = aligned(shard * local, local)
        total = total + z_in[shard].astype(F32)
        out[:, columns] = (
            total * down_scale[pl.ds(shard, 1), :] + middle[:, columns].astype(F32)
        ).astype(BF16)

    early, early_kind = jnp.where(outer, same, partner), jnp.where(outer, 0, 2)
    later, later_kind = jnp.where(outer, partner, same), jnp.where(outer, 2, 0)

    def pass_on(step):
        low, high = 2 * step, min(2 * step + 2, many)
        forward_down(later_kind, later, low, high)

    pl.when(inner)(functools.partial(forward_down, 2, partner, 6, many))
    product(fs, rep)
    product(fs, 1 - rep)
    pl.when(inner)(functools.partial(pass_on, 0))
    join_cores(fs, rep)
    join_cores(fs, 1 - rep)
    pl.when(outer)(functools.partial(pass_on, 0))
    product(early, rep)
    pass_on(1)
    arrived_x(early_kind, early)
    product(early, 1 - rep)
    pass_on(2)
    pl.when(inner)(functools.partial(pass_on, 3))
    join_cores(early, rep)
    join_cores(early, 1 - rep)
    pl.when(inner)(functools.partial(forward_slice, 0, 0, 3))
    product(later, rep)
    join_sides(fs)
    pl.when(outer)(functools.partial(forward_slice, 0, 0, 3))
    forward_slice(0, 3)
    arrived_x(later_kind, later)
    product(later, 1 - rep)
    join_cores(later, rep)
    forward_slice(1, 0, many // 2)
    join_cores(later, 1 - rep)
    forward_slice(1, many // 2)
    product(far, rep)
    join_sides(early)
    for lane in range(2):

        @pl.loop(0, count)
        def _(unit):
            sem = (1 + 2 * lane, unit)
            landed(slice_part(far, 1 - rep, unit, lane), dx_send.at[sem], dx_recv.at[sem])

    product_by_slot(far, 1 - rep)
    join_cores(far, rep)
    join_cores(far, 1 - rep)
    join_sides(later)
    join_sides(far)
    conclude(partner)
    conclude(jnp.where(outer, fs, far))
    conclude(jnp.where(outer, far, fs))
    conclude(same)

    for copy in sent:
        copy.wait_send()
    for q in range(3):
        pool_copy_to(q).wait_send()
    for part in range(TOKEN_PARTS):
        token_copy(part).wait_send()
    for shard in range(4):
        for which in range(3):
            y_copy(shard, which).wait_send()
        for slot in range(2):
            z_copy(shard, slot).wait_send()
            for half in range(2):
                core_copy(shard, half, slot).wait_send()

    @pl.loop(0, many)
    def _(j):
        for q, f in enumerate(sources):

            @pl.when(j < (count if q == 1 else other_count))
            def _():
                chunk_copy(j, q).wait_send()
                if q == 1:
                    for lane in range(2):
                        slice_copy(j, lane).wait_send()
                else:
                    down_copy(q, j).wait_send()

            @pl.when(j < count)
            def _():
                chunk_onward(j, q, f).wait_send()
                if q == 1:
                    for lane in range(2):
                        slice_onward(j, lane).wait_send()
                else:
                    down_onward(q, f, j).wait_send()


def pair_shards(
    residual,
    mixer_gain,
    pool_weight,
    pool_scale,
    channel_gain,
    gate_weight,
    up_weight,
    gate_scale,
    up_scale,
    gate_taps,
    up_taps,
    down_weight,
    down_scale,
):
    _, length, groups, local = residual.shape
    channels = local * 4
    width = groups * channels
    rows, hidden_width = gate_weight.shape
    chunks = hidden_width // 128
    chunks = chunks - chunks * FEW // 12
    half = chunks * 128
    half_columns = down_weight.shape[1] // 2
    vmem = pl.BlockSpec(memory_space=pltpu.VMEM)
    anywhere = pl.BlockSpec(memory_space=pl.ANY)
    dma = pltpu.SemaphoreType.DMA
    pairs = [
        (3, 3),
        (2, 3),
        (3,),
        (3,),
        (3,),
        (TOKEN_PARTS,),
        (2, TOKEN_PARTS),
        (4, TOKEN_PARTS),
        (chunks, 3),
        (chunks, 3),
        (4, chunks),
        (4, chunks),
        (4, 2, 2),
        (4, 3),
        (4, 2),
    ]
    out = pl.pallas_call(
        pair_kernel,
        out_shape=jax.ShapeDtypeStruct((length, groups * local), BF16),
        in_specs=[anywhere] * 13,
        out_specs=vmem,
        scratch_shapes=[
            pltpu.VMEM(down_scale.shape, F32),
            pltpu.VMEM(gate_taps.shape, F32),
            pltpu.VMEM(up_taps.shape, F32),
            pltpu.VMEM((2, rows, half), F32),
            pltpu.VMEM((2, rows // 2, half), F32),
            pltpu.VMEM((half, 2 * half_columns), F32),
            pltpu.VMEM((half, half_columns), F32),
            pltpu.VMEM(pool_weight.shape, F32),
            pltpu.VMEM((2, 4, length, groups * local), BF16),
            pltpu.VMEM((4, 3, groups, local), F32),
            pltpu.VMEM((4, 2) + gate_scale.shape, F32),
            pltpu.VMEM(pool_weight.shape, BF16),
            pltpu.VMEM((groups, channels, channels), BF16),
            pltpu.VMEM((chunks, 4, rows, 256), BF16),
            pltpu.VMEM((chunks, rows // 2, 256), BF16),
            pltpu.VMEM((4, 2, half, half_columns), BF16),
            pltpu.VMEM((half, half_columns), BF16),
            pltpu.VMEM((length, channels), BF16),
            pltpu.VMEM((length, channels), BF16),
            pltpu.VMEM((2 * length, width), BF16),
            pltpu.VMEM((length, groups * local), BF16),
            pltpu.VMEM((2 * length, half), BF16),
            pltpu.VMEM((4, 2, 2, length, local), F32),
            pltpu.VMEM((4, 2, 2, length, local), BF16),
            pltpu.VMEM((4, 2, 2, length, local), BF16),
            pltpu.VMEM((4, 2, length, local), BF16),
            pltpu.VMEM((4, 2, length, local), BF16),
            pltpu.VMEM((4, length, local), BF16),
            pltpu.VMEM((4, length, local), BF16),
        ]
        + [dma(shape) for shape in pairs for _ in range(2)]
        + [dma((17,))],
        compiler_params=pltpu.CompilerParams(
            collective_id=0, has_side_effects=True, vmem_limit_bytes=VMEM_BYTES
        ),
    )(
        residual.reshape(length, groups * local),
        mixer_gain,
        pool_scale,
        channel_gain,
        down_scale,
        gate_scale,
        up_scale,
        gate_taps,
        up_taps,
        pool_weight,
        gate_weight,
        up_weight,
        down_weight,
    )
    return out.reshape(1, length, groups, local)


def paired(sizes, residual, gate_weight, down_weight):
    _, length, groups, local = residual
    return (
        sizes == (2, 4, 4)
        and residual[0] == 1
        and local == 128
        and length % BAND == 0
        and groups == len(WINDOWS)
        and down_weight[1] == 4 * local
        and gate_weight[0] * 4 == groups * local * 4
        and gate_weight[1] % 1536 == 0
    )


def shards(
    sizes,
    residual,
    mixer_gain,
    pool_weight,
    pool_scale,
    channel_gain,
    gate_weight,
    up_weight,
    gate_scale,
    up_scale,
    gate_taps,
    up_taps,
    down_weight,
    down_scale,
):
    if paired(sizes, residual.shape, gate_weight.shape, down_weight.shape):
        return pair_shards(
            residual,
            mixer_gain,
            pool_weight,
            pool_scale,
            channel_gain,
            gate_weight,
            up_weight,
            gate_scale,
            up_scale,
            gate_taps,
            up_taps,
            down_weight,
            down_scale,
        )
    n_rep, n_fs, n_tp = sizes
    _, length, groups, local = residual.shape
    channels = local * n_tp
    width = groups * channels
    own_width = groups * local
    hidden_width = gate_weight.shape[1]
    vmem = pl.BlockSpec(memory_space=pltpu.VMEM)
    anywhere = pl.BlockSpec(memory_space=pl.ANY)
    dma = pltpu.SemaphoreType.DMA
    hops = max(n_fs - 1, 1)
    reps = max(n_rep - 1, 1)
    peers = max(n_tp - 1, 1)
    out = pl.pallas_call(
        functools.partial(block_kernel, sizes),
        out_shape=jax.ShapeDtypeStruct((length, own_width), BF16),
        in_specs=[vmem] * 8 + [anywhere] * 3,
        out_specs=vmem,
        scratch_shapes=[
            pltpu.VMEM((groups, channels, local), BF16),
            pltpu.VMEM((n_fs,) + gate_weight.shape, BF16),
            pltpu.VMEM((n_fs,) + up_weight.shape, BF16),
            pltpu.VMEM((n_fs,) + down_weight.shape, BF16),
            pltpu.VMEM((n_tp, length, own_width), BF16),
            pltpu.VMEM((n_tp, length, own_width), BF16),
            pltpu.VMEM((n_tp, 2, own_width), F32),
            pltpu.VMEM((n_fs, 2, gate_scale.shape[1]), F32),
            pltpu.VMEM((2, hidden_width), F32),
            pltpu.VMEM((length, channels), BF16),
            pltpu.VMEM((length, own_width), BF16),
            pltpu.VMEM((length, width), BF16),
            pltpu.VMEM((length, hidden_width), BF16),
            pltpu.VMEM((length, hidden_width), BF16),
            pltpu.VMEM((n_tp, groups, length, local), BF16),
            pltpu.VMEM((n_tp, groups, length, local), BF16),
            dma((3, SUBS, 2 * hops)),
            dma((3, SUBS, 2 * hops)),
            dma((3, SUBS, 2 * hops, reps)),
            dma((3, SUBS, 2 * hops, reps)),
            dma((hops,)),
            dma((hops,)),
            dma((hops, reps)),
            dma((hops, reps)),
            dma((hops,)),
            dma((hops,)),
            dma((3, peers)),
            dma((3, peers)),
            dma((n_fs, peers)),
            dma((n_fs, peers)),
            dma((7,)),
        ],
        compiler_params=pltpu.CompilerParams(
            collective_id=0, has_side_effects=True, vmem_limit_bytes=60 * 1024 * 1024
        ),
    )(
        residual.reshape(length, own_width),
        jnp.stack([mixer_gain.reshape(-1), channel_gain.reshape(-1)]),
        pool_scale.reshape(1, -1),
        down_scale.reshape(1, -1),
        jnp.concatenate([gate_scale, up_scale], axis=0),
        gate_taps,
        up_taps,
        pool_weight.astype(BF16),
        gate_weight.astype(BF16),
        up_weight.astype(BF16),
        down_weight.astype(BF16),
    )
    return out.reshape(1, length, groups, local)


def solution(mesh):
    placed = (
        P(("rep", "fs"), None, None, "tp"),
        P(None, "tp"),
        P(None, "fs", "tp"),
        P(None, "tp"),
        P(None, "tp"),
        P("fs", "tp"),
        P("fs", "tp"),
        P("fs", "tp"),
        P("fs", "tp"),
        P(None, "tp"),
        P(None, "tp"),
        P("tp", "fs"),
        P(None, "tp"),
    )
    sizes = tuple(mesh.shape[name] for name in ("rep", "fs", "tp"))
    return jax.shard_map(
        functools.partial(shards, sizes),
        mesh=mesh,
        in_specs=placed,
        out_specs=P(("rep", "fs"), None, None, "tp"),
        check_vma=False,
    )
```

```python
import functools

import jax
import jax.numpy as jnp
from jax import lax
from jax.experimental import pallas as pl
from jax.experimental.pallas import tpu as pltpu
from jax.sharding import PartitionSpec as P

WINDOWS = (2, 4, 8, 16)
EPSILON = 1e-05
SUBS = 2
COLUMNS = 256
VMEM_BYTES = 63 * 1024 * 1024 + 896 * 1024
F32 = jnp.float32
BF16 = jnp.bfloat16


def delayed(values, steps):
    rows = lax.broadcasted_iota(jnp.int32, values.shape, 0)
    return jnp.where(rows >= steps, pltpu.roll(values, steps, 0), 0.0)


def causal_taps(values, taps):
    return taps[2:3] * values + taps[1:2] * delayed(values, 1) + taps[0:1] * delayed(values, 2)


def block_kernel(
    sizes,
    residual,
    gains,
    pool_scale,
    down_scale,
    scale_pair,
    gate_taps,
    up_taps,
    pool_own,
    gate_own,
    up_own,
    down_own,
    out,
    pool_full,
    gate_full,
    up_full,
    down_full,
    gathered,
    middle_all,
    gains_all,
    scales_all,
    scale_row,
    pooled,
    middle,
    inputs,
    gate_pre,
    hidden,
    partials,
    arrived,
    ring_send,
    ring_recv,
    rep_send,
    rep_recv,
    pool_send,
    pool_recv,
    pool_rep_send,
    pool_rep_recv,
    scale_send,
    scale_recv,
    tp_send,
    tp_recv,
    part_send,
    part_recv,
    local_sem,
):
    n_rep, n_fs, n_tp = sizes
    rep, fs, tp = (lax.axis_index(name) for name in ("rep", "fs", "tp"))
    length = residual.shape[0]
    groups = pool_full.shape[0]
    channels = pool_full.shape[1]
    local = residual.shape[1] // groups
    width = groups * channels

    def other(axis, offset):
        me, count = {"rep": (rep, n_rep), "fs": (fs, n_fs), "tp": (tp, n_tp)}[axis]
        return lax.rem(me + offset, count)

    def remote(src, dst, send, recv, axis, offset):
        return pltpu.make_async_remote_copy(
            src_ref=src,
            dst_ref=dst,
            send_sem=send,
            recv_sem=recv,
            device_id={axis: other(axis, offset)},
            device_id_type=pl.DeviceIdType.MESH,
        )

    barrier = pltpu.get_barrier_semaphore()
    for axis, count in (("rep", n_rep), ("fs", n_fs), ("tp", n_tp)):
        for offset in range(1, count):
            pl.semaphore_signal(
                barrier,
                inc=1,
                device_id={axis: other(axis, offset)},
                device_id_type=pl.DeviceIdType.MESH,
            )
    pl.semaphore_wait(barrier, n_rep + n_fs + n_tp - 3)

    sent = []

    def start(copy, valid=None):
        sent.append((copy, valid))
        if valid is None:
            copy.start()
        else:
            pl.when(valid)(copy.start)

    weights = ((gate_own, gate_full), (up_own, up_full), (down_own, down_full))

    def piece(w, shard, half, sub, own=False):
        rows = weights[w][0].shape[0] // (n_rep * SUBS)
        part = pl.ds(pl.multiple_of((half * SUBS + sub) * rows, rows), rows)
        return weights[w][0].at[part] if own else weights[w][1].at[shard, part]

    def shard_sent(step, way):
        shard = fs + step if way else fs - step
        return jnp.clip(shard, 0, n_fs - 1), (shard <= n_fs - 1 if way else shard >= 0)

    def line(w, sub, step):
        for way in range(2):
            shard, valid = shard_sent(step, way)
            start(
                remote(
                    piece(w, shard, rep, sub, own=step == 0),
                    piece(w, shard, rep, sub),
                    ring_send.at[w, sub, 2 * step + way],
                    ring_recv.at[w, sub, 2 * step + way],
                    "fs",
                    n_fs - 1 if way else 1,
                ),
                valid & (fs > 0 if way else fs < n_fs - 1),
            )

    def serve(w, sub, step):
        for way in range(2):
            shard, valid = shard_sent(step + 1, way)
            mine = piece(w, shard, rep, sub)
            sems = (w, sub, 2 * step + way)
            pl.when(valid)(
                remote(
                    mine, mine, ring_send.at[sems], ring_recv.at[sems], "fs", 1
                ).wait_recv
            )
            if step < n_fs - 2:
                onward = (w, sub, 2 * step + 2 + way)
                start(
                    remote(
                        mine,
                        mine,
                        ring_send.at[onward],
                        ring_recv.at[onward],
                        "fs",
                        n_fs - 1 if way else 1,
                    ),
                    valid & (fs > 0 if way else fs < n_fs - 1),
                )
            for d in range(1, n_rep):
                start(
                    remote(
                        mine,
                        mine,
                        rep_send.at[sems + (d - 1,)],
                        rep_recv.at[sems + (d - 1,)],
                        "rep",
                        d,
                    ),
                    valid,
                )

    def settle(w, step, ways=(0, 1)):
        for way in ways:
            shard, valid = shard_sent(step + 1, way)

            @pl.when(valid)
            def _():
                for sub in range(SUBS):
                    for d in range(1, n_rep):
                        got = piece(w, shard, other("rep", n_rep - d), sub)
                        sems = (w, sub, 2 * step + way, d - 1)
                        remote(
                            got, got, rep_send.at[sems], rep_recv.at[sems], "rep", d
                        ).wait_recv()

    def local_copy(src, dst, idx):
        copy = pltpu.make_async_copy(src, dst, local_sem.at[idx])
        copy.start()
        return copy

    own_copies = [
        local_copy(residual, gathered.at[tp], 0),
        local_copy(gains, gains_all.at[tp], 1),
        local_copy(scale_pair, scales_all.at[fs], 2),
        local_copy(gate_own, gate_full.at[fs], 3),
        local_copy(up_own, up_full.at[fs], 4),
        local_copy(down_own, down_full.at[fs], 5),
    ]

    pool_rows = pool_own.shape[1]
    rep_groups = groups // n_rep

    def pool_part(shard, half):
        return pool_full.at[
            pl.ds(half * rep_groups, rep_groups),
            pl.ds(pl.multiple_of(shard * pool_rows, pool_rows), pool_rows),
        ]

    pool_copy = local_copy(
        pool_own, pool_full.at[:, pl.ds(pl.multiple_of(fs * pool_rows, pool_rows), pool_rows)], 6
    )

    for d in range(1, n_fs):
        start(
            remote(
                pool_own.at[pl.ds(rep * rep_groups, rep_groups)],
                pool_part(fs, rep),
                pool_send.at[d - 1],
                pool_recv.at[d - 1],
                "fs",
                d,
            )
        )
    for w in (0, 1):
        for sub in range(SUBS):
            if n_fs > 1:
                line(w, sub, 0)
    for d in range(1, n_tp):
        start(remote(gains, gains_all.at[tp], tp_send.at[0, d - 1], tp_recv.at[0, d - 1], "tp", d))
    for d in range(1, n_tp):
        start(
            remote(residual, gathered.at[tp], tp_send.at[1, d - 1], tp_recv.at[1, d - 1], "tp", d)
        )
    for d in range(1, n_fs):
        start(
            remote(
                scale_pair, scales_all.at[fs], scale_send.at[d - 1], scale_recv.at[d - 1], "fs", d
            )
        )

    for d in range(1, n_fs):
        shard = other("fs", n_fs - d)
        mine = pool_part(shard, rep)
        remote(mine, mine, pool_send.at[d - 1], pool_recv.at[d - 1], "fs", d).wait_recv()
        for e in range(1, n_rep):
            start(
                remote(
                    mine,
                    mine,
                    pool_rep_send.at[d - 1, e - 1],
                    pool_rep_recv.at[d - 1, e - 1],
                    "rep",
                    e,
                )
            )
    for d in range(1, n_fs):
        shard = other("fs", n_fs - d)
        for e in range(1, n_rep):
            got = pool_part(shard, other("rep", n_rep - e))
            remote(
                got,
                got,
                pool_rep_send.at[d - 1, e - 1],
                pool_rep_recv.at[d - 1, e - 1],
                "rep",
                e,
            ).wait_recv()
    pool_copy.wait()
    for copy in own_copies:
        copy.wait()

    def tp_arrivals(idx, buffer):
        for d in range(1, n_tp):
            got = buffer.at[other("tp", n_tp - d)]
            remote(got, got, tp_send.at[idx, d - 1], tp_recv.at[idx, d - 1], "tp", d).wait_recv()

    for sub in range(SUBS):
        serve(0, sub, 0)
    tp_arrivals(0, gains_all)
    tp_arrivals(1, gathered)
    for sub in range(SUBS):
        serve(1, sub, 0)

    def mean_square_root(buffer):
        total = jnp.zeros((length, 1), F32)
        for t in range(n_tp):
            values = buffer[t].astype(F32)
            total = total + jnp.sum(values * values, axis=1, keepdims=True)
        return lax.rsqrt(total / width + EPSILON)

    factor = mean_square_root(gathered)
    positions = lax.broadcasted_iota(jnp.int32, (length, 1), 0).astype(F32) + 1.0
    for g in range(groups):
        part = slice(g * local, (g + 1) * local)
        share = 1.0 / jnp.minimum(positions, float(WINDOWS[g]))
        for t in range(n_tp):
            values = gathered[t, :, part].astype(F32)
            normed = (values * factor * gains_all[t, 0:1, part]).astype(BF16).astype(F32)
            totals = normed
            reach = 1
            while reach < WINDOWS[g]:
                totals = totals + delayed(totals, reach)
                reach = reach * 2
            pooled[:, t * local : (t + 1) * local] = (totals * share - normed).astype(BF16)
        mixed = jnp.dot(pooled[...], pool_full[g], preferred_element_type=F32)
        middle[:, part] = (
            mixed * pool_scale[:, part] + residual[:, part].astype(F32)
        ).astype(BF16)

    middle_copy = local_copy(middle, middle_all.at[tp], 0)
    for d in range(1, n_tp):
        start(
            remote(middle, middle_all.at[tp], tp_send.at[2, d - 1], tp_recv.at[2, d - 1], "tp", d)
        )
    for step in range(1, n_fs - 1):
        for w in (0, 1):
            if step == n_fs - 2 and n_fs > 2:
                break
            for sub in range(SUBS):
                serve(w, sub, step)
    for sub in range(SUBS):
        if n_fs > 1:
            line(2, sub, 0)
    for d in range(1, n_fs):
        got = scales_all.at[other("fs", n_fs - d)]
        remote(got, got, scale_send.at[d - 1], scale_recv.at[d - 1], "fs", d).wait_recv()
    shard_columns = scale_pair.shape[1]
    for f in range(n_fs):
        scale_row[:, f * shard_columns : (f + 1) * shard_columns] = scales_all[f]

    middle_copy.wait()
    tp_arrivals(2, middle_all)
    factor = mean_square_root(middle_all)
    for t in range(n_tp):
        for g in range(groups):
            part = slice(g * local, (g + 1) * local)
            start_column = g * channels + t * local
            inputs[:, start_column : start_column + local] = (
                middle_all[t, :, part].astype(F32) * factor * gains_all[t, 1:2, part]
            ).astype(BF16)

    def finish(w):
        if n_fs > 2:
            for sub in range(SUBS):
                serve(w, sub, n_fs - 2)
        for step in range(n_fs - 1):
            settle(w, step)

    def product(full, columns, row):
        block = full[:, :, columns].reshape(width, COLUMNS)
        made = jnp.dot(inputs[...], block, preferred_element_type=F32)
        return (made * scale_row[row : row + 1, columns]).astype(BF16)

    chunks = gate_full.shape[2] // COLUMNS

    finish(0)

    @pl.loop(0, chunks)
    def _(j):
        columns = pl.ds(pl.multiple_of(j * COLUMNS, COLUMNS), COLUMNS)
        gate_pre[:, columns] = product(gate_full, columns, 0)

    finish(1)
    for sub in range(SUBS):
        if n_fs > 1:
            serve(2, sub, 0)

    @pl.loop(0, chunks)
    def _(j):
        columns = pl.ds(pl.multiple_of(j * COLUMNS, COLUMNS), COLUMNS)
        up_values = product(up_full, columns, 1).astype(F32)
        conv_gate = causal_taps(gate_pre[:, columns].astype(F32), gate_taps[:, columns])
        conv_up = causal_taps(up_values, up_taps[:, columns])
        silu = conv_gate / (1.0 + jnp.exp(-conv_gate))
        hidden[:, columns] = (silu * conv_up).astype(BF16)

    shard_width = down_own.shape[1]

    def to_peers(idx, src, dst):
        for d in range(1, n_tp):
            start(
                remote(
                    src(other("tp", d)),
                    dst(tp),
                    part_send.at[idx, d - 1],
                    part_recv.at[idx, d - 1],
                    "tp",
                    d,
                )
            )

    def from_peers(idx, dst):
        for d in range(1, n_tp):
            got = dst(other("tp", n_tp - d))
            remote(
                got, got, part_send.at[idx, d - 1], part_recv.at[idx, d - 1], "tp", d
            ).wait_recv()

    def conclude(g, columns):
        total = partials[tp, g].astype(F32)
        for d in range(1, n_tp):
            total = total + arrived[other("tp", d), g].astype(F32)
        out[:, columns] = (
            total * down_scale[:, columns] + middle[:, columns].astype(F32)
        ).astype(BF16)

    if shard_width == channels and local % 128 == 0:
        def share(shard):
            made = jnp.dot(hidden[...], down_full[shard], preferred_element_type=F32)
            for t in range(n_tp):
                partials[t, shard] = made[:, t * local : (t + 1) * local].astype(BF16)
            for d in range(1, n_tp):
                peer = other("tp", d)
                remote(
                    partials.at[peer, shard],
                    arrived.at[tp, shard],
                    part_send.at[shard, d - 1],
                    part_recv.at[shard, d - 1],
                    "tp",
                    d,
                ).start()

        share(fs)
        for step in range(n_fs - 1):
            if step >= 1:
                for sub in range(SUBS):
                    serve(2, sub, step)
            for way in range(2):
                settle(2, step, (way,))
                shard, valid = shard_sent(step + 1, way)
                pl.when(valid)(functools.partial(share, shard))
        for shard in range(n_fs):
            from_peers(shard, lambda t: arrived.at[t, shard])
            conclude(shard, slice(shard * local, (shard + 1) * local))
            for d in range(1, n_tp):
                mine = partials.at[other("tp", d), shard]
                remote(
                    mine, mine, part_send.at[shard, d - 1], part_recv.at[shard, d - 1], "tp", d
                ).wait_send()
    else:
        for step in range(n_fs - 1):
            if step >= 1:
                for sub in range(SUBS):
                    serve(2, sub, step)
            settle(2, step)
        for f in range(n_fs):
            made = jnp.dot(hidden[...], down_full[f], preferred_element_type=F32).astype(BF16)
            span = min(local, shard_width)
            for at in range(0, shard_width, span):
                g, channel = divmod(f * shard_width + at, channels)
                t, low = divmod(channel, local)
                partials[t, g, :, low : low + span] = made[:, at : at + span]
        to_peers(0, lambda t: partials.at[t], lambda t: arrived.at[t])
        from_peers(0, lambda t: arrived.at[t])
        for g in range(groups):
            conclude(g, slice(g * local, (g + 1) * local))

    for copy, valid in sent:
        if valid is None:
            copy.wait_send()
        else:
            pl.when(valid)(copy.wait_send)


BAND = 256
FEW = 5
TOKEN_PARTS = 2


def pair_kernel(
    residual,
    mixer_gain,
    pool_scale,
    channel_gain,
    down_scale_own,
    gate_scale,
    up_scale,
    gate_taps_own,
    up_taps_own,
    pool_own,
    gate_own,
    up_own,
    down_own,
    out,
    down_scale,
    gate_taps,
    up_taps,
    stage_own,
    stage_other,
    stage_down,
    stage_down_other,
    stage_pool,
    tokens,
    small_all,
    scales_all,
    pool_near,
    pool_full,
    weights,
    other,
    down_full,
    down_other,
    normed,
    pooled,
    inputs,
    middle,
    hidden,
    keep,
    give,
    got,
    y_out,
    y_in,
    z_out,
    z_in,
    small_send,
    small_recv,
    scale_send,
    scale_recv,
    pz_send,
    pz_recv,
    px_send,
    px_recv,
    pt_send,
    pt_recv,
    rz_send,
    rz_recv,
    ry_send,
    ry_recv,
    rs_send,
    rs_recv,
    gz_send,
    gz_recv,
    gx_send,
    gx_recv,
    dz_send,
    dz_recv,
    dx_send,
    dx_recv,
    core_send,
    core_recv,
    y_send,
    y_recv,
    z_send,
    z_recv,
    local_sem,
):
    rep, fs, tp = (lax.axis_index(name) for name in ("rep", "fs", "tp"))
    length = residual.shape[0]
    groups, pool_rows, local = pool_own.shape
    channels = pool_full.shape[1]
    width = groups * channels
    rows = gate_own.shape[0]
    half_rows = rows // 2
    chunks = gate_own.shape[1] // 128
    few = chunks * FEW // 12
    many = chunks - few
    half_columns = down_own.shape[1] // 2
    member = lax.rem(fs, 2)
    side = tp // 2
    core = lax.rem(tp, 2)
    sibling = {"tp": tp + 1 - 2 * core}
    across = {"tp": lax.rem(tp + 2, 4)}
    diagonal = {"tp": 3 - tp}
    mirror = {"rep": 1 - rep}
    same, far, partner = lax.rem(fs + 2, 4), 3 - fs, fs + 1 - 2 * member
    sources = (same, far, partner)
    outer = (fs == 0) | (fs == 3)
    inner = jnp.logical_not(outer)
    count = jnp.where(outer, few, many)
    other_count = chunks - count
    begin = jnp.where(outer, many, 0)
    skip = jnp.where(outer, many - few, 0)
    other_skip = many - few - skip

    sent = []

    def remote(src, dst, send, recv, device):
        return pltpu.make_async_remote_copy(
            src_ref=src,
            dst_ref=dst,
            send_sem=send,
            recv_sem=recv,
            device_id=device,
            device_id_type=pl.DeviceIdType.MESH,
        )

    def start(*parts):
        copy = remote(*parts)
        sent.append(copy)
        copy.start()

    def aligned(at, size):
        return pl.ds(pl.multiple_of(at, size), size)

    def local_copy(src, dst, idx):
        copy = pltpu.make_async_copy(src, dst, local_sem.at[idx])
        copy.start()
        return copy

    barrier = pltpu.get_barrier_semaphore()
    peers = (mirror, sibling, across, diagonal) + tuple({"fs": f} for f in sources)
    for device in peers:
        pl.semaphore_signal(
            barrier, inc=1, device_id=device, device_id_type=pl.DeviceIdType.MESH
        )
    mine = pl.ds(pl.multiple_of(jnp.where(outer, few, 0) * 128, 128), many * 128)
    theirs = pl.ds(pl.multiple_of(jnp.where(outer, 0, few) * 128, 128), many * 128)
    rep_rows = aligned(rep * half_rows, half_rows)
    rep_columns = aligned(rep * half_columns, half_columns)
    load_pool = local_copy(pool_own, stage_pool, 1)
    load_tokens = local_copy(residual, tokens.at[0, tp], 0)
    loads = [
        local_copy(gate_own.at[:, mine], stage_own.at[0], 2),
        local_copy(up_own.at[:, mine], stage_own.at[1], 3),
        local_copy(gate_own.at[rep_rows, theirs], stage_other.at[0], 4),
        local_copy(up_own.at[rep_rows, theirs], stage_other.at[1], 5),
    ]
    load_down = [
        local_copy(down_own.at[mine], stage_down, 6),
        local_copy(down_own.at[theirs, rep_columns], stage_down_other, 7),
    ]

    small_loads = [
        local_copy(src, dst, 9 + at)
        for at, (src, dst) in enumerate(
            (
                (mixer_gain, small_all.at[tp, 0]),
                (pool_scale, small_all.at[tp, 1]),
                (channel_gain, small_all.at[tp, 2]),
                (gate_scale, scales_all.at[fs, 0]),
                (up_scale, scales_all.at[fs, 1]),
                (down_scale_own, down_scale),
                (gate_taps_own, gate_taps),
                (up_taps_own, up_taps),
            )
        )
    ]
    load_pool.wait()
    pool_near[...] = stage_pool[...].astype(BF16)
    load_tokens.wait()
    pl.semaphore_wait(barrier, len(peers))

    def token_part(slot, t, part):
        span = length // TOKEN_PARTS
        return tokens.at[slot, t, pl.ds(part * span, span)]

    def pool_part(shard, half):
        span = groups // 2
        return pool_full.at[
            pl.ds(half * span, span),
            aligned(shard * pool_rows, pool_rows),
            aligned(tp * local, local),
        ]

    def pool_copy_to(q):
        return remote(
            pool_near.at[pl.ds(rep * (groups // 2), groups // 2)],
            pool_part(fs, rep),
            pz_send.at[q],
            pz_recv.at[q],
            {"fs": sources[q]},
        )

    for q in (2, 1, 0):
        pool_copy_to(q).start()
    for part in range(TOKEN_PARTS):
        piece = token_part(0, tp, part)
        start(piece, piece, ry_send.at[0, part], ry_recv.at[0, part], across)
        start(piece, piece, rs_send.at[0, part], rs_recv.at[0, part], sibling)
    for at, values in enumerate((mixer_gain, pool_scale, channel_gain)):
        for q, device in enumerate((sibling, across, diagonal)):
            start(values, small_all.at[tp, at], small_send.at[at, q], small_recv.at[at, q], device)
    for at, values in enumerate((gate_scale, up_scale)):
        for q, f in enumerate(sources):
            start(
                values, scales_all.at[fs, at], scale_send.at[at, q], scale_recv.at[at, q], {"fs": f}
            )
    pool_copy = local_copy(
        pool_near,
        pool_full.at[:, aligned(fs * pool_rows, pool_rows), aligned(tp * local, local)],
        8,
    )

    late, late_kind = jnp.where(outer, far, same), jnp.where(outer, 1, 0)

    def chunk_target(j, shard, half):
        return weights.at[j, shard, aligned(half * half_rows, half_rows)]

    def chunk_copy(j, q):
        target = chunk_target(j, fs, rep)
        source = target if q == 1 else other.at[j]
        return remote(source, target, gz_send.at[0], gz_recv.at[j, q], {"fs": sources[q]})

    def down_part(shard, half, unit):
        return down_full.at[shard, half, aligned(unit * 128, 128)]

    def down_copy(q, unit):
        target = down_part(fs, rep, unit)
        source = down_other.at[aligned(unit * 128, 128)]
        return remote(source, target, dz_send.at[0], dz_recv.at[q, unit], {"fs": sources[q]})

    def slice_part(shard, half, unit, lane):
        return down_full.at[
            shard, half, aligned(unit * 128, 128), pl.ds(lane * local, local)
        ]

    def slice_copy(unit, lane):
        piece = slice_part(fs, rep, unit, lane)
        return remote(
            piece, piece, dz_send.at[0], dz_recv.at[1 + 2 * lane, unit], {"fs": far}
        )

    def token_copy(part):
        return remote(
            token_part(0, tp, part),
            token_part(1, tp, part),
            rz_send.at[part],
            rz_recv.at[part],
            {"fs": partner},
        )

    for part in range(TOKEN_PARTS):
        token_copy(part).start()
    for load in loads + small_loads:
        load.wait()

    @pl.loop(0, many)
    def _(j):
        @pl.when(j < other_count)
        def _():
            columns = aligned((other_skip + j) * 128, 128)
            for at in range(2):
                lanes = slice(at * 128, (at + 1) * 128)
                other[j, :, lanes] = stage_other[at, :, columns].astype(BF16)
            chunk_copy(j, 2).start()

        @pl.when(j < count)
        def _():
            columns = aligned((skip + j) * 128, 128)
            for at in range(2):
                lanes = slice(at * 128, (at + 1) * 128)
                weights[j, fs, :, lanes] = stage_own[at, :, columns].astype(BF16)
            pl.when(inner)(chunk_copy(j, 1).start)

    @pl.when(inner)
    def _():
        @pl.loop(0, other_count)
        def _(j):
            chunk_copy(j, 0).start()

    for load in load_down:
        load.wait()
    if many > few:
        hidden[:, few * 128 :] = jnp.zeros((2 * length, (many - few) * 128), BF16)

        @pl.when(outer)
        def _():
            down_full[:, :, few * 128 :] = jnp.zeros(
                (4, 2, (many - few) * 128, half_columns), BF16
            )

    @pl.loop(0, count)
    def _(j):
        here = aligned(j * 128, 128)
        there = aligned((skip + j) * 128, 128)
        for half in range(2):
            down_full[fs, half, here] = stage_down[
                there, half * half_columns : (half + 1) * half_columns
            ].astype(BF16)

    @pl.loop(0, other_count)
    def _(j):
        there = aligned((other_skip + j) * 128, 128)
        down_other[aligned(j * 128, 128)] = stage_down_other[there].astype(BF16)

    @pl.when(outer)
    def _():
        for unit in range(2):
            down_copy(2, unit).start()

    @pl.when(inner)
    def _():
        @pl.loop(0, other_count)
        def _(unit):
            down_copy(2, unit).start()

        @pl.loop(0, other_count)
        def _(unit):
            down_copy(0, unit).start()

        for lane in range(2):

            @pl.loop(0, count)
            def _(unit):
                slice_copy(unit, lane).start()

    def landed(ref, send, recv):
        remote(ref, ref, send, recv, mirror).wait_recv()

    def chunk_onward(j, q, shard):
        piece = chunk_target(j, shard, rep)
        return remote(piece, piece, gx_send.at[0], gx_recv.at[j, q], mirror)

    def forward_chunk(j, q, shard):
        piece = chunk_target(j, shard, rep)
        landed(piece, gz_send.at[0], gz_recv.at[j, q])
        chunk_onward(j, q, shard).start()

    def down_onward(q, shard, unit):
        piece = down_part(shard, rep, unit)
        return remote(piece, piece, dx_send.at[0], dx_recv.at[q, unit], mirror)

    def slice_onward(unit, lane):
        piece = slice_part(far, rep, unit, lane)
        sem = (1 + 2 * lane, unit)
        return remote(piece, piece, dx_send.at[0], dx_recv.at[sem], mirror)

    def forward_slice(lane, low=0, high=many):
        @pl.loop(low, jnp.minimum(count, high))
        def _(unit):
            sem = (1 + 2 * lane, unit)
            landed(slice_part(far, rep, unit, lane), dz_send.at[0], dz_recv.at[sem])
            slice_onward(unit, lane).start()

    def forward_down(q, shard, low=0, high=many):
        @pl.loop(low, jnp.minimum(count, high))
        def _(unit):
            landed(down_part(shard, rep, unit), dz_send.at[0], dz_recv.at[q, unit])
            down_onward(q, shard, unit).start()

    for q, f in ((2, partner), (1, far), (0, same)):
        piece = pool_part(f, rep)
        landed(piece, pz_send.at[q], pz_recv.at[q])
        start(piece, piece, px_send.at[q], px_recv.at[q], mirror)
    for q, f in enumerate(sources):
        landed(pool_part(f, 1 - rep), px_send.at[q], px_recv.at[q])
    pool_copy.wait()

    def pool_slab(t):
        return pool_full.at[:, :, aligned(t * local, local)]

    slab = pool_slab(tp)
    start(slab, slab, pt_send.at[1], pt_recv.at[1], across)
    start(slab, slab, pt_send.at[0], pt_recv.at[0], sibling)

    t_sibling, t_across, t_diagonal = sibling["tp"], across["tp"], diagonal["tp"]

    def own_onward(part):
        piece = token_part(0, t_across, part)
        landed(piece, ry_send.at[0, part], ry_recv.at[0, part])
        start(piece, piece, rs_send.at[1, part], rs_recv.at[1, part], sibling)

    def partner_onward(part):
        piece = token_part(1, tp, part)
        landed(piece, rz_send.at[part], rz_recv.at[part])
        start(piece, piece, ry_send.at[1, part], ry_recv.at[1, part], across)
        start(piece, piece, rs_send.at[2, part], rs_recv.at[2, part], sibling)

    def forward_chunks(kind, shard, low, high):
        for j in range(low, high):
            forward_chunk(j, kind, shard)

    third = many // 3
    own_onward(0)
    pl.when(inner)(functools.partial(forward_chunks, 1, far, 0, third))
    partner_onward(0)
    own_onward(1)
    pl.when(inner)(functools.partial(forward_chunks, 1, far, third, many - third))
    partner_onward(1)
    pl.when(inner)(functools.partial(forward_chunks, 1, far, many - third, many))
    second_kind, second = jnp.where(outer, 0, 2), jnp.where(outer, same, partner)
    forward_chunks(second_kind, second, 0, few - 3)
    slab = pool_slab(t_across)
    landed(slab, pt_send.at[1], pt_recv.at[1])
    start(slab, slab, pt_send.at[2], pt_recv.at[2], sibling)
    forward_chunks(second_kind, second, few - 3, few - 2)

    for part in range(TOKEN_PARTS):
        landed(token_part(0, t_sibling, part), rs_send.at[0, part], rs_recv.at[0, part])
        landed(token_part(0, t_diagonal, part), rs_send.at[1, part], rs_recv.at[1, part])
    for at in range(3):
        for q, t in enumerate((t_sibling, t_across, t_diagonal)):
            landed(small_all.at[t, at], small_send.at[at, q], small_recv.at[at, q])
    landed(pool_slab(t_sibling), pt_send.at[0], pt_recv.at[0])
    landed(pool_slab(t_diagonal), pt_send.at[2], pt_recv.at[2])

    positions = lax.broadcasted_iota(jnp.int32, (BAND, 1), 0).astype(F32) + 1.0
    distance = (
        lax.broadcasted_iota(jnp.int32, (BAND, 2 * BAND), 0)
        + BAND
        - lax.broadcasted_iota(jnp.int32, (BAND, 2 * BAND), 1)
    )

    def mix(slot, between):
        span = slice(slot * length, (slot + 1) * length)
        square = jnp.zeros((length, local), F32)
        for t in range(4):
            for g in range(groups):
                values = tokens[slot, t, :, g * local : (g + 1) * local].astype(F32)
                square = square + values * values
        factor = lax.rsqrt(jnp.sum(square, axis=1, keepdims=True) / width + EPSILON)
        square = jnp.zeros((length, local), F32)
        for g in range(groups):
            if g == groups // 2:
                between()
            part = slice(g * local, (g + 1) * local)
            for t in range(4):
                values = tokens[slot, t, :, part].astype(F32)
                normed[:, t * local : (t + 1) * local] = (
                    values * factor * small_all[t, 0, g : g + 1]
                ).astype(BF16)
            band = jnp.where((distance >= 0) & (distance < WINDOWS[g]), 1.0, 0.0).astype(BF16)
            for b in range(length // BAND):
                here = slice(b * BAND, (b + 1) * BAND)
                if b == 0:
                    totals = jnp.dot(band[:, BAND:], normed[here], preferred_element_type=F32)
                    totals = totals / jnp.minimum(positions, float(WINDOWS[g]))
                else:
                    totals = jnp.dot(
                        band,
                        normed[(b - 1) * BAND : (b + 1) * BAND],
                        preferred_element_type=F32,
                    ) * (1.0 / WINDOWS[g])
                pooled[here] = (totals - normed[here].astype(F32)).astype(BF16)
            mixed = jnp.dot(pooled[...], pool_full[g], preferred_element_type=F32)
            for t in range(4):
                made = (
                    mixed[:, t * local : (t + 1) * local] * small_all[t, 1, g : g + 1]
                    + tokens[slot, t, :, part].astype(F32)
                ).astype(BF16)
                inputs[span, g * channels + t * local : g * channels + (t + 1) * local] = made
                values = made.astype(F32)
                square = square + values * values
        factor = lax.rsqrt(jnp.sum(square, axis=1, keepdims=True) / width + EPSILON)
        if slot == 0:
            for g in range(groups):
                middle[:, g * local : (g + 1) * local] = inputs[
                    span, aligned(g * channels + tp * local, local)
                ]
        for g in range(groups):
            for t in range(4):
                columns = slice(g * channels + t * local, g * channels + (t + 1) * local)
                inputs[span, columns] = (
                    inputs[span, columns].astype(F32) * factor * small_all[t, 2, g : g + 1]
                ).astype(BF16)

    def cross():
        forward_chunks(second_kind, second, few - 2, few)

        @pl.when(outer)
        def _():
            @pl.loop(0, many)
            def _(j):
                pl.when(j < few)(chunk_copy(j, 1).start)
                chunk_copy(j, 0).start()

            @pl.loop(2, many)
            def _(unit):
                down_copy(2, unit).start()

    mix(0, cross)

    @pl.when(inner)
    def _():
        forward_chunks(2, partner, few, many)
        forward_down(2, partner, 0, 2)

    for part in range(TOKEN_PARTS):
        piece = token_part(1, t_across, part)
        landed(piece, ry_send.at[1, part], ry_recv.at[1, part])
        start(piece, piece, rs_send.at[3, part], rs_recv.at[3, part], sibling)
    pl.when(outer)(functools.partial(forward_chunk, 0, 1, far))
    for part in range(TOKEN_PARTS):
        landed(token_part(1, t_sibling, part), rs_send.at[2, part], rs_recv.at[2, part])
        landed(token_part(1, t_diagonal, part), rs_send.at[3, part], rs_recv.at[3, part])

    def forward_late(j):
        forward_chunk(j, late_kind, late)
        pl.when(outer)(functools.partial(forward_chunk, j, 2, partner))

    forward_chunk(0, jnp.where(outer, 2, 0), jnp.where(outer, partner, same))
    mix(1, functools.partial(forward_late, 1))
    for at in range(2):
        for q, f in enumerate(sources):
            landed(scales_all.at[f, at], scale_send.at[at, q], scale_recv.at[at, q])

    thirds = scales_all.shape[3] // 128

    def expand(j):
        for q, f in enumerate(sources):
            landed(chunk_target(j, f, 1 - rep), gx_send.at[0], gx_recv.at[j, q])
        unit = begin + j
        here = aligned(unit * 128, 128)
        scale_at = aligned(lax.rem(unit, thirds) * 128, 128)
        taps = [
            table[:, here] * scales_all[unit // thirds, at, :, scale_at]
            for at, table in enumerate((gate_taps, up_taps))
        ]
        block = weights[j].reshape(width, 256)
        for slot in range(2):
            span = slice(slot * length, (slot + 1) * length)
            made = jnp.dot(inputs[span], block, preferred_element_type=F32)
            conv_gate = causal_taps(made[:, :128], taps[0])
            conv_up = causal_taps(made[:, 128:], taps[1])
            silu = conv_gate / (1.0 + jnp.exp(-conv_gate))
            hidden[span, aligned(j * 128, 128)] = (silu * conv_up).astype(BF16)

    @pl.loop(0, count)
    def _(j):
        expand(j)

        @pl.when(j < count - 2)
        def _():
            forward_late(j + 2)

        @pl.when(inner & (j == many - 3))
        def _():
            forward_down(2, partner, 2, 4)

        @pl.when(inner & (j == many - 2))
        def _():
            forward_down(2, partner, 4, 6)

        @pl.when(outer & (j == few - 2))
        def _():
            forward_down(0, same)

            @pl.loop(0, many)
            def _(unit):
                down_copy(0, unit).start()

            for lane in range(2):

                @pl.loop(0, few)
                def _(unit):
                    slice_copy(unit, lane).start()

    def core_copy(shard, half, slot):
        return remote(
            give.at[shard, half, slot],
            got.at[shard, half, slot],
            core_send.at[0],
            core_recv.at[shard, half, slot],
            sibling,
        )

    def product(shard, half):
        made = jnp.dot(hidden[...], down_full[shard, half], preferred_element_type=F32)
        for slot in (1, 0):
            span = slice(slot * length, (slot + 1) * length)
            low, high = made[span, :local], made[span, local:]
            keep[shard, half, slot] = jnp.where(core == 0, low, high)
            give[shard, half, slot] = jnp.where(core == 0, high, low).astype(BF16)
        for slot in (1, 0):
            core_copy(shard, half, slot).start()

    def product_by_slot(shard, half):
        for slot in (1, 0):
            span = slice(slot * length, (slot + 1) * length)
            made = jnp.dot(hidden[span], down_full[shard, half], preferred_element_type=F32)
            low, high = made[:, :local], made[:, local:]
            keep[shard, half, slot] = jnp.where(core == 0, low, high)
            give[shard, half, slot] = jnp.where(core == 0, high, low).astype(BF16)
            core_copy(shard, half, slot).start()

    def y_part(buffer, shard, which):
        if which == 0:
            return buffer.at[shard, 0]
        return buffer.at[shard, 1, pl.ds((which - 1) * (length // 2), length // 2)]

    def y_copy(shard, which):
        return remote(
            y_part(y_out, shard, which),
            y_part(y_in, shard, which),
            y_send.at[0],
            y_recv.at[shard, which],
            across,
        )

    def z_copy(shard, part):
        rows = pl.ds(part * (length // 2), length // 2)
        return remote(
            z_out.at[shard, rows],
            z_in.at[shard, rows],
            z_send.at[0],
            z_recv.at[shard, part],
            {"fs": partner},
        )

    def arrived_x(q, shard):
        @pl.loop(0, count)
        def _(unit):
            landed(down_part(shard, 1 - rep, unit), dx_send.at[0], dx_recv.at[q, unit])

    def join_cores(shard, half):
        for slot in (1, 0):
            core_copy(shard, half, slot).wait_recv()
            total = keep[shard, half, slot] + got[shard, half, slot].astype(F32)

            @pl.when(half == side)
            def _():
                keep[shard, half, slot] = total

            @pl.when(half != side)
            def _():
                y_out[shard, slot] = total.astype(BF16)
                for which in (1, 2) if slot else (0,):
                    y_copy(shard, which).start()

    def join_sides(shard):
        for part in range(2):
            rows = slice(part * (length // 2), (part + 1) * (length // 2))
            y_copy(shard, 1 + part).wait_recv()
            total = keep[shard, side, 1, rows] + y_in[shard, 1, rows].astype(F32)
            z_out[shard, rows] = total.astype(BF16)
            z_copy(shard, part).start()

    def conclude(shard):
        y_copy(shard, 0).wait_recv()
        total = keep[shard, side, 0] + y_in[shard, 0].astype(F32)
        for part in range(2):
            z_copy(shard, part).wait_recv()
        columns = aligned(shard * local, local)
        total = total + z_in[shard].astype(F32)
        out[:, columns] = (
            total * down_scale[pl.ds(shard, 1), :] + middle[:, columns].astype(F32)
        ).astype(BF16)

    early, early_kind = jnp.where(outer, same, partner), jnp.where(outer, 0, 2)
    later, later_kind = jnp.where(outer, partner, same), jnp.where(outer, 2, 0)

    def pass_on(step):
        low, high = 2 * step, min(2 * step + 2, many)
        forward_down(later_kind, later, low, high)

    pl.when(inner)(functools.partial(forward_down, 2, partner, 6, many))
    product(fs, rep)
    product(fs, 1 - rep)
    pl.when(inner)(functools.partial(pass_on, 0))
    join_cores(fs, rep)
    join_cores(fs, 1 - rep)
    pl.when(outer)(functools.partial(pass_on, 0))
    product(early, rep)
    pass_on(1)
    arrived_x(early_kind, early)
    product(early, 1 - rep)
    pass_on(2)
    pl.when(inner)(functools.partial(pass_on, 3))
    join_cores(early, rep)
    join_cores(early, 1 - rep)
    pl.when(inner)(functools.partial(forward_slice, 0, 0, 3))
    product(later, rep)
    join_sides(fs)
    pl.when(outer)(functools.partial(forward_slice, 0, 0, 3))
    forward_slice(0, 3)
    arrived_x(later_kind, later)
    product(later, 1 - rep)
    join_cores(later, rep)
    forward_slice(1, 0, many // 2)
    join_cores(later, 1 - rep)
    forward_slice(1, many // 2)
    product(far, rep)
    join_sides(early)
    for lane in range(2):

        @pl.loop(0, count)
        def _(unit):
            sem = (1 + 2 * lane, unit)
            landed(slice_part(far, 1 - rep, unit, lane), dx_send.at[0], dx_recv.at[sem])

    product_by_slot(far, 1 - rep)
    join_cores(far, rep)
    join_cores(far, 1 - rep)
    join_sides(later)
    join_sides(far)
    conclude(partner)
    conclude(jnp.where(outer, fs, far))
    conclude(jnp.where(outer, far, fs))
    conclude(same)

    for copy in sent:
        copy.wait_send()
    for q in range(3):
        pool_copy_to(q).wait_send()
    for part in range(TOKEN_PARTS):
        token_copy(part).wait_send()
    def drained(ref, send, recv):
        remote(ref, ref, send.at[0], recv, mirror).wait_send()

    drained(y_out, y_send, y_recv.at[0, 0])
    drained(z_out, z_send, z_recv.at[0, 0])
    drained(give, core_send, core_recv.at[0, 0, 0])

    def drain(own, others):
        total = own + 2 * others
        drained(weights.at[:4, :, pl.ds(0, total * 16)], gz_send, gz_recv.at[0, 0])
        drained(weights.at[:4, :, pl.ds(0, own * 48)], gx_send, gx_recv.at[0, 0])
        drained(down_full.at[:2, :, pl.ds(0, total * 32)], dz_send, dz_recv.at[0, 0])
        drained(down_full.at[:3, 0, pl.ds(0, own * 128)], dx_send, dx_recv.at[0, 0])

    pl.when(inner)(functools.partial(drain, many, few))
    pl.when(outer)(functools.partial(drain, few, many))


def pair_shards(
    residual,
    mixer_gain,
    pool_weight,
    pool_scale,
    channel_gain,
    gate_weight,
    up_weight,
    gate_scale,
    up_scale,
    gate_taps,
    up_taps,
    down_weight,
    down_scale,
):
    _, length, groups, local = residual.shape
    channels = local * 4
    width = groups * channels
    rows, hidden_width = gate_weight.shape
    chunks = hidden_width // 128
    chunks = chunks - chunks * FEW // 12
    half = chunks * 128
    half_columns = down_weight.shape[1] // 2
    vmem = pl.BlockSpec(memory_space=pltpu.VMEM)
    anywhere = pl.BlockSpec(memory_space=pl.ANY)
    dma = pltpu.SemaphoreType.DMA
    shapes = [
        (3, 3),
        (2, 3),
        (3,),
        (3,),
        (3,),
        (TOKEN_PARTS,),
        (2, TOKEN_PARTS),
        (4, TOKEN_PARTS),
    ]
    shared = [(chunks, 3), (chunks, 3), (4, chunks), (4, chunks), (4, 2, 2), (4, 3), (4, 2)]
    pairs = [(shape, shape) for shape in shapes] + [((1,), shape) for shape in shared]
    out = pl.pallas_call(
        pair_kernel,
        out_shape=jax.ShapeDtypeStruct((length, groups * local), BF16),
        in_specs=[anywhere] * 13,
        out_specs=vmem,
        scratch_shapes=[
            pltpu.VMEM(down_scale.shape, F32),
            pltpu.VMEM(gate_taps.shape, F32),
            pltpu.VMEM(up_taps.shape, F32),
            pltpu.VMEM((2, rows, half), F32),
            pltpu.VMEM((2, rows // 2, half), F32),
            pltpu.VMEM((half, 2 * half_columns), F32),
            pltpu.VMEM((half, half_columns), F32),
            pltpu.VMEM(pool_weight.shape, F32),
            pltpu.VMEM((2, 4, length, groups * local), BF16),
            pltpu.VMEM((4, 3, groups, local), F32),
            pltpu.VMEM((4, 2) + gate_scale.shape, F32),
            pltpu.VMEM(pool_weight.shape, BF16),
            pltpu.VMEM((groups, channels, channels), BF16),
            pltpu.VMEM((chunks, 4, rows, 256), BF16),
            pltpu.VMEM((chunks, rows // 2, 256), BF16),
            pltpu.VMEM((4, 2, half, half_columns), BF16),
            pltpu.VMEM((half, half_columns), BF16),
            pltpu.VMEM((length, channels), BF16),
            pltpu.VMEM((length, channels), BF16),
            pltpu.VMEM((2 * length, width), BF16),
            pltpu.VMEM((length, groups * local), BF16),
            pltpu.VMEM((2 * length, half), BF16),
            pltpu.VMEM((4, 2, 2, length, local), F32),
            pltpu.VMEM((4, 2, 2, length, local), BF16),
            pltpu.VMEM((4, 2, 2, length, local), BF16),
            pltpu.VMEM((4, 2, length, local), BF16),
            pltpu.VMEM((4, 2, length, local), BF16),
            pltpu.VMEM((4, length, local), BF16),
            pltpu.VMEM((4, length, local), BF16),
        ]
        + [dma(shape) for pair in pairs for shape in pair]
        + [dma((17,))],
        compiler_params=pltpu.CompilerParams(
            collective_id=0, has_side_effects=True, vmem_limit_bytes=VMEM_BYTES
        ),
    )(
        residual.reshape(length, groups * local),
        mixer_gain,
        pool_scale,
        channel_gain,
        down_scale,
        gate_scale,
        up_scale,
        gate_taps,
        up_taps,
        pool_weight,
        gate_weight,
        up_weight,
        down_weight,
    )
    return out.reshape(1, length, groups, local)


def paired(sizes, residual, gate_weight, down_weight):
    _, length, groups, local = residual
    return (
        sizes == (2, 4, 4)
        and residual[0] == 1
        and local == 128
        and length % BAND == 0
        and groups == len(WINDOWS)
        and down_weight[1] == 4 * local
        and gate_weight[0] * 4 == groups * local * 4
        and gate_weight[1] % 1536 == 0
    )


def shards(
    sizes,
    residual,
    mixer_gain,
    pool_weight,
    pool_scale,
    channel_gain,
    gate_weight,
    up_weight,
    gate_scale,
    up_scale,
    gate_taps,
    up_taps,
    down_weight,
    down_scale,
):
    if paired(sizes, residual.shape, gate_weight.shape, down_weight.shape):
        return pair_shards(
            residual,
            mixer_gain,
            pool_weight,
            pool_scale,
            channel_gain,
            gate_weight,
            up_weight,
            gate_scale,
            up_scale,
            gate_taps,
            up_taps,
            down_weight,
            down_scale,
        )
    n_rep, n_fs, n_tp = sizes
    _, length, groups, local = residual.shape
    channels = local * n_tp
    width = groups * channels
    own_width = groups * local
    hidden_width = gate_weight.shape[1]
    vmem = pl.BlockSpec(memory_space=pltpu.VMEM)
    anywhere = pl.BlockSpec(memory_space=pl.ANY)
    dma = pltpu.SemaphoreType.DMA
    hops = max(n_fs - 1, 1)
    reps = max(n_rep - 1, 1)
    peers = max(n_tp - 1, 1)
    out = pl.pallas_call(
        functools.partial(block_kernel, sizes),
        out_shape=jax.ShapeDtypeStruct((length, own_width), BF16),
        in_specs=[vmem] * 8 + [anywhere] * 3,
        out_specs=vmem,
        scratch_shapes=[
            pltpu.VMEM((groups, channels, local), BF16),
            pltpu.VMEM((n_fs,) + gate_weight.shape, BF16),
            pltpu.VMEM((n_fs,) + up_weight.shape, BF16),
            pltpu.VMEM((n_fs,) + down_weight.shape, BF16),
            pltpu.VMEM((n_tp, length, own_width), BF16),
            pltpu.VMEM((n_tp, length, own_width), BF16),
            pltpu.VMEM((n_tp, 2, own_width), F32),
            pltpu.VMEM((n_fs, 2, gate_scale.shape[1]), F32),
            pltpu.VMEM((2, hidden_width), F32),
            pltpu.VMEM((length, channels), BF16),
            pltpu.VMEM((length, own_width), BF16),
            pltpu.VMEM((length, width), BF16),
            pltpu.VMEM((length, hidden_width), BF16),
            pltpu.VMEM((length, hidden_width), BF16),
            pltpu.VMEM((n_tp, groups, length, local), BF16),
            pltpu.VMEM((n_tp, groups, length, local), BF16),
            dma((3, SUBS, 2 * hops)),
            dma((3, SUBS, 2 * hops)),
            dma((3, SUBS, 2 * hops, reps)),
            dma((3, SUBS, 2 * hops, reps)),
            dma((hops,)),
            dma((hops,)),
            dma((hops, reps)),
            dma((hops, reps)),
            dma((hops,)),
            dma((hops,)),
            dma((3, peers)),
            dma((3, peers)),
            dma((n_fs, peers)),
            dma((n_fs, peers)),
            dma((7,)),
        ],
        compiler_params=pltpu.CompilerParams(
            collective_id=0, has_side_effects=True, vmem_limit_bytes=60 * 1024 * 1024
        ),
    )(
        residual.reshape(length, own_width),
        jnp.stack([mixer_gain.reshape(-1), channel_gain.reshape(-1)]),
        pool_scale.reshape(1, -1),
        down_scale.reshape(1, -1),
        jnp.concatenate([gate_scale, up_scale], axis=0),
        gate_taps,
        up_taps,
        pool_weight.astype(BF16),
        gate_weight.astype(BF16),
        up_weight.astype(BF16),
        down_weight.astype(BF16),
    )
    return out.reshape(1, length, groups, local)


def solution(mesh):
    placed = (
        P(("rep", "fs"), None, None, "tp"),
        P(None, "tp"),
        P(None, "fs", "tp"),
        P(None, "tp"),
        P(None, "tp"),
        P("fs", "tp"),
        P("fs", "tp"),
        P("fs", "tp"),
        P("fs", "tp"),
        P(None, "tp"),
        P(None, "tp"),
        P("tp", "fs"),
        P(None, "tp"),
    )
    sizes = tuple(mesh.shape[name] for name in ("rep", "fs", "tp"))
    return jax.shard_map(
        functools.partial(shards, sizes),
        mesh=mesh,
        in_specs=placed,
        out_specs=P(("rep", "fs"), None, None, "tp"),
        check_vma=False,
    )
```
